512 devices in a mesh: kv: 32 (over z, x), tp: 16 (over y, core).
Axes of the slice: x: 4, y: 8, z: 8, core: 2. Of those that a mesh axis runs over, the one named last changes fastest.
Arguments:
- tokens: bfloat16 [16, 4096], P(None, ('kv', 'tp')), may hold values from -24 to 24
- live_lengths: int32 [16], replicated, may hold values from 256 to 16384, as said below
- kv_cache: bfloat16 [16, 16384, 2048], P(None, 'kv', 'tp'), may hold values from -128 to 128
- gate_sums: float32 [16, 16, 16384], P(None, 'tp', 'kv'), may hold values from -16384 to 0, as said below
- w_query: bfloat16 [4096, 4096], P('kv', 'tp'), may hold values from -0.09375 to 0.09375
- w_key: bfloat16 [4096, 1024], P('kv', 'tp'), may hold values from -0.09375 to 0.09375
- w_value: bfloat16 [4096, 1024], P('kv', 'tp'), may hold values from -0.09375 to 0.09375
- w_forget: bfloat16 [4096, 16], replicated, may hold values from -0.09375 to 0.09375
- forget_bias: float32 [16], replicated, may hold values from -1 to 2
- w_out: bfloat16 [4096, 4096], P('tp', 'kv'), may hold values from -0.75 to 0.75
- first_gain: float32 [4096], P(('kv', 'tp')), may hold values from 0 to 4
- w_gate: bfloat16 [4096, 11264], P('kv', 'tp'), may hold values from -0.09375 to 0.09375
- w_up: bfloat16 [4096, 11264], P('kv', 'tp'), may hold values from -0.09375 to 0.09375
- w_down: bfloat16 [11264, 4096], P('tp', 'kv'), may hold values from -0.109375 to 0.109375
- second_gain: float32 [4096], P(('kv', 'tp')), may hold values from 0 to 4
Outputs:
- layer_out: bfloat16 [16, 4096], P(None, ('kv', 'tp'))
The draws below stay inside these ranges and needn't reach their ends.
Inputs may be any that keep to these rules, and one draw needn't show every extreme that they name: `live_lengths`: at least one sequence has length exactly 16384. `gate_sums`: entries at positions at or beyond the sequence's length are 0.
All inputs are finite; a program needn't handle non-finite values.
Results may differ from the reference program's by a relative error of at most 0.019.
Values may be sent and summed in bfloat16 or wider, within the bound.
No kernel may reach another device: no remote copies, remote signals or barrier semaphores. Data moves between devices by JAX's collectives and lax.ppermute only.
A program may use at most 64 MiB of HBM per device.

```python
import jax
import jax.numpy as jnp
from jax import lax

D = 4096
DH = 64
KEY_HEAD_COUNT = 16
GROUP = 4
H = 64
FF = 11264
SEQUENCE_COUNT = 16
P_DEV = 512
LEN = 16384


def sequence_lengths(key):
    base_key = jax.random.fold_in(key, 701)
    short_key, long_key, order_key = jax.random.split(base_key, 3)
    short_floor = max(LEN // 64, 2)
    short_lengths = jax.random.randint(short_key, (SEQUENCE_COUNT,), short_floor, max(LEN // 8, short_floor) + 1)
    long_lengths = jax.random.randint(long_key, (SEQUENCE_COUNT,), max(LEN // 2, 2), LEN + 1)
    ranking = jax.random.permutation(order_key, SEQUENCE_COUNT)
    chosen = jnp.where(ranking < max(SEQUENCE_COUNT // 4, 1), long_lengths, short_lengths)
    return jnp.where(ranking == 0, LEN, chosen).astype(jnp.int32)


def column_scales(key, rise_factor):
    jitter_strength = jax.random.uniform(key, (D,), jnp.float32, 0.8, 1.25)
    where_col = jnp.arange(D, dtype=jnp.float32) / max(D - 1, 1)
    return jitter_strength * jnp.exp(jnp.log(rise_factor) * (where_col - 0.5))


def token_rows(key):
    base_key = jax.random.fold_in(key, 702)
    noise_key, scale_key = jax.random.split(base_key, 2)
    noise_draw = jnp.clip(jax.random.normal(noise_key, (SEQUENCE_COUNT, D), jnp.float32), -6.0, 6.0)
    scales = column_scales(scale_key, 3.0)[None, :]
    return noise_draw * scales + scales


def query_weight(key):
    base_key = jax.random.fold_in(key, 703)
    return jnp.clip(jax.random.normal(base_key, (D, H * DH), jnp.float32), -6.0, 6.0) * D ** (-0.5)


def log_uniform(key, array_shape, lower_end, upper_end):
    return jnp.exp(jax.random.uniform(key, array_shape, jnp.float32, jnp.log(lower_end), jnp.log(upper_end)))


def rising_gain(key, salt_value):
    base_key = jax.random.fold_in(key, salt_value)
    return column_scales(base_key, 3.0)


def draw_tokens(key, part):
    return token_rows(key).astype(jnp.bfloat16)


def draw_live_lengths(key, part):
    return sequence_lengths(key)


def draw_w_query(key, part):
    return query_weight(key).astype(jnp.bfloat16)


def draw_first_gain(key, part):
    return rising_gain(key, 706)


def draw_second_gain(key, part):
    return rising_gain(key, 707)


def draw_kv_cache(key, part):
    base_key = jax.random.fold_in(key, 704)
    noise_key, offset_key = jax.random.split(base_key, 2)
    entries = jnp.clip(jax.random.normal(noise_key, (SEQUENCE_COUNT, LEN, KEY_HEAD_COUNT, 2, DH), jnp.float32), -6.0, 6.0)
    block_count = (LEN + 63) // 64
    offsets = jnp.clip(jax.random.normal(offset_key, (SEQUENCE_COUNT, block_count, 1, KEY_HEAD_COUNT, 1, DH), jnp.float32), -3.0, 3.0)
    offsets = jnp.broadcast_to(offsets, (SEQUENCE_COUNT, block_count, 64, KEY_HEAD_COUNT, 1, DH)).reshape(SEQUENCE_COUNT, block_count * 64, KEY_HEAD_COUNT, 1, DH)[:, :LEN]
    slot_pick = jnp.array([0.0, 1.0], jnp.float32).reshape(1, 1, 1, 2, 1)
    entries = entries + offsets * slot_pick
    return entries.reshape(SEQUENCE_COUNT, LEN, KEY_HEAD_COUNT * 2 * DH).astype(jnp.bfloat16)


def draw_gate_sums(key, part):
    base_key = jax.random.fold_in(key, 705)
    head_key, fast_key, slow_key, block_key, rough_key, location_random_key, depth_key = jax.random.split(base_key, 7)
    length_values = sequence_lengths(key)
    head_order = jax.random.permutation(head_key, KEY_HEAD_COUNT)
    quick_decay_heads = head_order < max(KEY_HEAD_COUNT // 2, 1)
    fast_rate = log_uniform(fast_key, (SEQUENCE_COUNT, KEY_HEAD_COUNT, 1), 0.04, 0.12)
    slow_rate = log_uniform(slow_key, (SEQUENCE_COUNT, KEY_HEAD_COUNT, 1), 0.2, 0.8) / LEN
    increment_ratio = jnp.where(quick_decay_heads[None, :, None], fast_rate, slow_rate)
    block_count = (LEN + P_DEV - 1) // P_DEV
    block_multiplier = log_uniform(block_key, (SEQUENCE_COUNT, KEY_HEAD_COUNT, block_count, 1), 0.5, 2.0)
    block_multiplier = jnp.broadcast_to(block_multiplier, (SEQUENCE_COUNT, KEY_HEAD_COUNT, block_count, P_DEV)).reshape(SEQUENCE_COUNT, KEY_HEAD_COUNT, block_count * P_DEV)[:, :, :LEN]
    jitter_strength = jax.random.uniform(rough_key, (SEQUENCE_COUNT, KEY_HEAD_COUNT, LEN), jnp.float32, 0.5, 1.5)
    spike_locations = jax.random.randint(location_random_key, (SEQUENCE_COUNT, KEY_HEAD_COUNT, 3), 0, length_values[:, None, None])
    depth_values = jnp.log(jax.random.uniform(depth_key, (SEQUENCE_COUNT, KEY_HEAD_COUNT, 3), jnp.float32, 0.5, 0.8))
    position_selector = jnp.arange(LEN, dtype=jnp.int32)
    spike_decrease = jnp.sum(jnp.where(position_selector[None, None, None, :] == spike_locations[..., None], depth_values[..., None], 0.0), axis=2)
    spike_decrease = jnp.where(quick_decay_heads[None, :, None], 0.0, spike_decrease)
    logarithm_gate_values = -increment_ratio * block_multiplier * jitter_strength + spike_decrease
    live_mask = position_selector[None, None, :] < length_values[:, None, None]
    masked = jnp.where(live_mask, logarithm_gate_values, 0.0)
    suffix_sum = jnp.flip(jnp.cumsum(jnp.flip(masked, axis=-1), axis=-1), axis=-1) - masked
    return suffix_sum


def spiked(drawn, own_key, source, target, blocks, factor):
    owner, partner = [(jnp.arange(drawn.shape[axis_at]) // (drawn.shape[axis_at] // blocks)).reshape([-1 if axis == axis_at else 1 for axis in range(drawn.ndim)]) for axis_at in (source, target)]
    chosen = jax.random.permutation(own_key, blocks)[partner]
    strong = (owner == chosen) | (owner == (partner + blocks // 2) % blocks)
    return jnp.where(strong, factor * drawn, drawn)


def block_scale(own_key, extent, shards, least, largest):
    def one(dim, parts):
        steps = jax.random.uniform(jax.random.fold_in(jax.random.fold_in(own_key, 6), dim), (parts,), jnp.float32, least / len(shards), largest / len(shards))
        return jnp.repeat(jnp.exp(steps), extent[dim] // parts).reshape((-1,) + (1,) * (len(extent) - dim - 1))

    loudness = one(*shards[0])
    for cut in shards[1:]:
        loudness = loudness * one(*cut)
    return loudness


def scatter_about(rng, extent, width, bound, cuts=(), kind=jnp.bfloat16):
    level = block_scale(rng, extent, cuts, -0.22, 0.18) if cuts else 1.0
    values = jax.random.normal(rng, extent, jnp.float32) * width * level
    return jnp.minimum(jnp.maximum(values, -bound), bound).astype(kind)


def gaussian_with(own_key, extent, deviation, most, cuts, heavy, kind=jnp.bfloat16):
    drawn = deviation * jax.random.normal(own_key, extent, jnp.float32)
    if cuts:
        drawn = drawn * block_scale(own_key, extent, cuts, -0.22, 0.18)
    return jnp.clip(spiked(drawn, jax.random.fold_in(own_key, 3), *heavy), -most, most).astype(kind)


def setup_inputs(seed: int = 0) -> dict:
    arg_keys = jax.random.split(jax.random.key(seed), 16)
    tokens = draw_tokens(jax.random.fold_in(arg_keys[15], 71), 0)
    live_lengths = draw_live_lengths(jax.random.fold_in(arg_keys[15], 71), 0)
    kv_cache = draw_kv_cache(jax.random.fold_in(arg_keys[15], 71), 0)
    gate_sums = draw_gate_sums(jax.random.fold_in(arg_keys[15], 71), 0)
    w_query = draw_w_query(jax.random.fold_in(arg_keys[15], 71), 0)
    w_key = scatter_about(arg_keys[5], (D, KEY_HEAD_COUNT * DH), D ** -0.5, 0.09375, ((0, 32), (1, 16)))
    w_value = scatter_about(arg_keys[6], (D, KEY_HEAD_COUNT * DH), D ** -0.5, 0.09375, ((0, 32), (1, 16)))
    w_forget = scatter_about(arg_keys[7], (D, KEY_HEAD_COUNT), D ** -0.5, 0.09375)
    forget_bias = jnp.clip(jax.random.uniform(arg_keys[8], (KEY_HEAD_COUNT,), jnp.float32, -1.0, 2.0), -1.0, 2.0)
    w_out = gaussian_with(arg_keys[9], (H * DH, D), (H * DH // 16) ** -0.5, 0.75, ((0, 16), (1, 32)), (0, 1, 32, 2.75))
    first_gain = draw_first_gain(jax.random.fold_in(arg_keys[15], 71), 0)
    w_gate = scatter_about(arg_keys[11], (D, FF), D ** -0.5, 0.09375, ((0, 32), (1, 16)))
    w_up = scatter_about(arg_keys[12], (D, FF), D ** -0.5, 0.09375, ((0, 32), (1, 16)))
    w_down = gaussian_with(arg_keys[13], (FF, D), FF ** -0.5, 0.109375, ((0, 16), (1, 32)), (0, 1, 32, 2.75))
    second_gain = draw_second_gain(jax.random.fold_in(arg_keys[15], 71), 0)
    return {"tokens": tokens, "live_lengths": live_lengths, "kv_cache": kv_cache, "gate_sums": gate_sums, "w_query": w_query, "w_key": w_key, "w_value": w_value, "w_forget": w_forget, "forget_bias": forget_bias, "w_out": w_out, "first_gain": first_gain, "w_gate": w_gate, "w_up": w_up, "w_down": w_down, "second_gain": second_gain}


EPSILON = 1e-05

def layer_norm(mixture, norm_gain):
    centre = lax.optimization_barrier(jnp.mean(mixture, axis=-1, keepdims=True))
    spread = lax.optimization_barrier(jnp.mean(jnp.square(mixture - centre), axis=-1, keepdims=True))
    return ((mixture - centre) * lax.rsqrt(spread + EPSILON) * norm_gain).astype(jnp.bfloat16)

def attend_sequence(pieces):
    query_row, new_key, new_value, new_gate, cache_rows, gate_row, length = pieces
    queries = query_row.astype(jnp.float32).reshape(KEY_HEAD_COUNT, GROUP, DH)
    blocks = cache_rows.astype(jnp.float32).reshape(LEN, KEY_HEAD_COUNT, 2, DH)
    score_scale = DH ** (-0.5)
    scores = jnp.einsum('gjd,sgd->gjs', queries, blocks[:, :, 0, :]) * score_scale
    scores = scores + gate_row[:, None, :] + new_gate[:, None, None]
    live_mask = jnp.arange(LEN, dtype=jnp.int32) < length
    own_score = jnp.einsum('gjd,gd->gj', queries, new_key.astype(jnp.float32).reshape(KEY_HEAD_COUNT, DH)) * score_scale
    row_top = jnp.maximum(lax.optimization_barrier(jnp.max(jnp.where(live_mask, scores, -jnp.inf), axis=-1)), own_score)
    weights = jnp.where(live_mask, jnp.exp(scores - row_top[..., None]), 0.0)
    own_weight = jnp.exp(own_score - row_top)
    weight_total = lax.optimization_barrier(jnp.sum(weights, axis=-1)) + own_weight
    rounded = lax.optimization_barrier(weights.astype(jnp.bfloat16)).astype(jnp.float32)
    own_rounded = lax.optimization_barrier(own_weight.astype(jnp.bfloat16)).astype(jnp.float32)
    summed = jnp.einsum('gjs,sgd->gjd', rounded, blocks[:, :, 1, :])
    summed = summed + own_rounded[..., None] * new_value.astype(jnp.float32).reshape(KEY_HEAD_COUNT, 1, DH)
    return (summed / weight_total[..., None]).reshape(KEY_HEAD_COUNT * GROUP * DH).astype(jnp.bfloat16)

def reference(tokens, live_lengths, kv_cache, gate_sums, w_query, w_key, w_value, w_forget, forget_bias, w_out, first_gain, w_gate, w_up, w_down, second_gain):
    queries = jnp.dot(tokens, w_query, preferred_element_type=jnp.float32).astype(jnp.bfloat16)
    new_keys = jnp.dot(tokens, w_key, preferred_element_type=jnp.float32).astype(jnp.bfloat16)
    new_values = jnp.dot(tokens, w_value, preferred_element_type=jnp.float32).astype(jnp.bfloat16)
    new_gates = jax.nn.log_sigmoid(jnp.dot(tokens, w_forget, preferred_element_type=jnp.float32) + forget_bias)
    attended = lax.map(attend_sequence, (queries, new_keys, new_values, new_gates, kv_cache, gate_sums, live_lengths))
    attn_out = jnp.dot(attended, w_out, preferred_element_type=jnp.float32)
    after_mix = layer_norm(tokens.astype(jnp.float32) + attn_out, first_gain)
    gate_units = jnp.dot(after_mix, w_gate, preferred_element_type=jnp.float32)
    up_units = jnp.dot(after_mix, w_up, preferred_element_type=jnp.float32)
    hidden = (jax.nn.silu(gate_units) * up_units).astype(jnp.bfloat16)
    ffn_out = jnp.dot(hidden, w_down, preferred_element_type=jnp.float32)
    return layer_norm(after_mix.astype(jnp.float32) + ffn_out, second_gain)
```

```python
import jax
import jax.numpy as jnp
from jax import lax
from jax.sharding import Mesh
from jax.sharding import PartitionSpec as P

D = 4096
DH = 64
GROUP = 4
HALF = 384
KV = ("kv_0", "kv_1")
KV_TP = ("kv_0", "kv_1", "tp")
EPSILON = 1e-05
EMPTY_SCORE = -1e30
F32 = jnp.float32
BF16 = jnp.bfloat16


def exchanged(pieces, axis):
    return lax.all_to_all(pieces, axis, 0, 0, tiled=True)


def sent_to_all(shard, axis):
    devices = lax.axis_size(axis)
    return exchanged(jnp.broadcast_to(shard[None], (devices, *shard.shape)), axis)


def in_pieces(value, count):
    pieces = []
    for _ in range(count):
        piece = lax.reduce_precision(value, 8, 7)
        pieces.append(piece.astype(BF16))
        value = value - piece
    return pieces


def on_device(
    tokens,
    live_lengths,
    kv_cache,
    gate_sums,
    w_query,
    w_key,
    w_value,
    w_forget,
    forget_bias,
    w_out,
    first_gain,
    w_gate,
    w_up,
    w_down,
    second_gain,
):
    sequences, own_cols = tokens.shape
    kv_index = lax.axis_index(KV)
    tp_index = lax.axis_index("tp")
    kv_size = lax.axis_size(KV)
    positions = kv_cache.shape[1]
    hidden_cols = w_gate.shape[1]

    turned = jnp.concatenate(
        [tokens.astype(F32).T, first_gain[:, None], second_gain[:, None]], axis=1
    )
    block = sent_to_all(turned, "tp").reshape(-1, sequences + 2)
    rows = block[:, :sequences].T
    gains = block[:, sequences:].T
    width = rows.shape[1]

    rows_bf = rows.astype(BF16)
    forget_rows = lax.dynamic_slice(w_forget, (kv_index * width, tp_index), (width, 1))
    query_part = jnp.dot(rows_bf, w_query, preferred_element_type=F32)
    key_part = jnp.dot(rows_bf, w_key, preferred_element_type=F32)
    value_part = jnp.dot(rows_bf, w_value, preferred_element_type=F32)
    forget_part = jnp.dot(rows_bf, forget_rows, preferred_element_type=F32)[:, 0]
    token_part = jnp.sum(rows, axis=1)
    out_part = jnp.sum(w_out.astype(F32), axis=1)
    new_rows = jnp.concatenate([key_part, value_part], axis=1).astype(BF16)
    new_rows = jnp.concatenate([new_rows] * (kv_size // sequences), axis=0)
    small = jnp.concatenate([*in_pieces(forget_part, 2), *in_pieces(token_part, 2)])
    small = jnp.pad(small, (0, 2 * DH - small.size))
    mixed = jnp.concatenate(
        [new_rows, jnp.broadcast_to(small[None], (kv_size, small.size))], axis=1
    )
    common = jnp.concatenate([query_part.astype(BF16), *(p[None] for p in in_pieces(out_part, 2))])
    message = jnp.concatenate(
        [jnp.broadcast_to(common[None], (kv_size, *common.shape)), mixed[:, None]], axis=1
    )
    total = jnp.sum(exchanged(message, KV).astype(F32), axis=0)
    queries = total[:sequences].astype(BF16).reshape(sequences, GROUP, DH)
    out_row_sums = total[sequences] + total[sequences + 1]
    mixed = total[sequences + 2]
    new_key = mixed[:DH].astype(BF16)
    new_value = mixed[DH : 2 * DH].astype(BF16).astype(F32)
    small = mixed[2 * DH : 2 * DH + 4 * sequences].reshape(4, sequences)
    new_gate = jax.nn.log_sigmoid(
        small[0] + small[1] + lax.dynamic_slice_in_dim(forget_bias, tp_index, 1)
    )
    token_sums = small[2] + small[3]

    score_scale = DH**-0.5
    keys, values = kv_cache[:, :, :DH], kv_cache[:, :, DH:]
    scores = (
        jnp.einsum("bjd,bpd->bjp", queries, keys, preferred_element_type=F32) * score_scale
    )
    scores = scores + gate_sums[:, :, :] + new_gate[:, None, None]
    position = kv_index * positions + jnp.arange(positions, dtype=jnp.int32)
    live = (position[None, :] < live_lengths[:, None])[:, None, :]
    own_here = (jnp.arange(sequences) == kv_index)[:, None]
    own_score = jnp.einsum("bjd,d->bj", queries, new_key, preferred_element_type=F32) * score_scale
    own_score = jnp.where(own_here, own_score, EMPTY_SCORE)
    top = jnp.maximum(jnp.max(jnp.where(live, scores, EMPTY_SCORE), axis=-1), own_score)
    weights = jnp.where(live, jnp.exp(scores - top[..., None]), 0.0)
    own_weight = jnp.where(own_here, jnp.exp(own_score - top), 0.0)
    weight_total = jnp.sum(weights, axis=-1) + own_weight
    weighted = jnp.einsum(
        "bjp,bpd->bjd", weights.astype(BF16), values, preferred_element_type=F32
    )
    own_rounded = lax.reduce_precision(own_weight, 8, 7)
    weighted = weighted + own_rounded[..., None] * new_value
    stats = jnp.concatenate([*in_pieces(top, 3), *in_pieces(weight_total, 2)], axis=1)
    stats = jnp.pad(stats, ((0, 0), (0, 2 * DH - stats.shape[1])))
    message = jnp.concatenate([weighted.reshape(sequences, -1).astype(BF16), stats], axis=1)
    parts = sent_to_all(message, KV).astype(F32)
    heads = GROUP * DH
    stats = parts[:, :, heads : heads + 5 * GROUP].reshape(kv_size, sequences, 5, GROUP)
    tops = stats[:, :, 0] + stats[:, :, 1] + stats[:, :, 2]
    totals = stats[:, :, 3] + stats[:, :, 4]
    scales = jnp.exp(tops - jnp.max(tops, axis=0))
    joint_total = jnp.sum(totals * scales, axis=0)
    parts = parts[:, :, :heads].reshape(kv_size, sequences, GROUP, DH)
    joint = jnp.sum(parts * scales[..., None], axis=0)
    attended = (joint / joint_total[..., None]).astype(BF16).reshape(sequences, heads)

    attn_part = jnp.dot(attended, w_out, preferred_element_type=F32)
    mean_part = jnp.sum(attended.astype(F32) * out_row_sums, axis=1)
    means = jnp.concatenate(in_pieces(mean_part, 2))
    means = jnp.pad(means, (0, width - means.size))
    message = jnp.concatenate([attn_part.astype(BF16), means[None]])
    total = jnp.sum(sent_to_all(message, "tp").astype(F32), axis=0)
    mean_sums = total[sequences, :sequences] + total[sequences, sequences : 2 * sequences]
    centre = (token_sums + mean_sums) / D
    centred = rows + total[:sequences] - centre[:, None]
    scaled = centred * gains[0]

    squares = jnp.sum(centred * centred, axis=1)
    scaled_bf = scaled.astype(BF16)
    pad = ((0, 0), (0, 2 * HALF - hidden_cols))
    gate_part = jnp.dot(scaled_bf, w_gate, preferred_element_type=F32).astype(BF16)
    up_part = jnp.dot(scaled_bf, w_up, preferred_element_type=F32).astype(BF16)
    squares = jnp.concatenate(in_pieces(squares, 2))
    squares = jnp.pad(squares, (0, HALF - squares.size))
    message = jnp.stack(
        [
            jnp.pad(gate_part, pad).reshape(kv_size, HALF),
            jnp.pad(up_part, pad).reshape(kv_size, HALF),
            jnp.broadcast_to(squares[None], (kv_size, HALF)),
        ],
        axis=1,
    )
    total = jnp.sum(exchanged(message, KV).astype(F32), axis=0)
    spread = (total[2, :sequences] + total[2, sequences : 2 * sequences]) / D
    shrink = lax.rsqrt(spread + EPSILON)
    own_shrink = lax.dynamic_slice_in_dim(shrink, kv_index // 2, 1)
    hidden_share = jax.nn.silu(total[0] * own_shrink) * (total[1] * own_shrink)
    mid = lax.reduce_precision(scaled * shrink[:, None], 8, 7)

    hidden = sent_to_all(hidden_share.astype(BF16)[None], KV).reshape(sequences, 2 * HALF)

    ffn_part = jnp.dot(hidden[:, :hidden_cols], w_down, preferred_element_type=F32)
    ffn = jnp.sum(sent_to_all(ffn_part.astype(BF16), "tp").astype(F32), axis=0)
    mixture = mid + ffn

    block_sum = jnp.sum(mixture, axis=1)
    block_centre = block_sum / width
    block_square = jnp.sum((mixture - block_centre[:, None]) ** 2, axis=1)
    both = sent_to_all(jnp.concatenate([block_centre, block_square])[None], KV)
    centres, squares = both[:, 0, :sequences], both[:, 0, sequences:]
    centre = jnp.sum(centres, axis=0) / kv_size
    spread = jnp.sum(squares + width * (centres - centre) ** 2, axis=0) / D
    own = tp_index * own_cols
    mixture = lax.dynamic_slice_in_dim(mixture, own, own_cols, 1)
    gain = lax.dynamic_slice_in_dim(gains[1], own, own_cols)
    out = (mixture - centre[:, None]) * lax.rsqrt(spread[:, None] + EPSILON) * gain
    return out.astype(BF16)


def solution(mesh):
    split = Mesh(mesh.devices.reshape(8, 4, mesh.shape["tp"]), ("kv_0", "kv_1", "tp"))
    placed = (
        P(None, KV_TP),
        P(),
        P(None, KV, "tp"),
        P(None, "tp", KV),
        P(KV, "tp"),
        P(KV, "tp"),
        P(KV, "tp"),
        P(),
        P(),
        P("tp", KV),
        P(KV_TP),
        P(KV, "tp"),
        P(KV, "tp"),
        P("tp", KV),
        P(KV_TP),
    )
    return jax.shard_map(
        on_device, mesh=split, in_specs=placed, out_specs=P(None, KV_TP), check_vma=False
    )
```

```python
import jax
import jax.numpy as jnp
from jax import lax
from jax.experimental import pallas as pl
from jax.experimental.pallas import tpu as pltpu
from jax.sharding import Mesh
from jax.sharding import PartitionSpec as P

D = 4096
DH = 64
LANES = 128
KV = ("kv_0", "kv_1")
KV_TP = ("kv_0", "kv_1", "tp")
EPSILON = 1e-05
EMPTY_SCORE = -1e30
F32 = jnp.float32
BF16 = jnp.bfloat16

VMEM = pl.BlockSpec(memory_space=pltpu.VMEM)
SMEM = pl.BlockSpec(memory_space=pltpu.SMEM)
ANY = pl.BlockSpec(memory_space=pl.ANY)


def kernel(body, outs, specs, scratch=()):
    return pl.pallas_call(
        body,
        out_shape=[jax.ShapeDtypeStruct(shape, dtype) for shape, dtype in outs],
        in_specs=specs,
        out_specs=[VMEM] * len(outs),
        scratch_shapes=scratch,
    )


def exchanged(pieces, axis):
    return lax.all_to_all(pieces, axis, 0, 0, tiled=True)


def kv_index():
    return lax.axis_index("kv_0") * lax.axis_size("kv_1") + lax.axis_index("kv_1")


def iota(shape, dim):
    return lax.broadcasted_iota(jnp.int32, shape, dim)


def rounded(x):
    return x.astype(BF16).astype(F32)


def in_pieces(value, count):
    pieces = []
    for _ in range(count):
        piece = rounded(value)
        pieces.append(piece)
        value = value - piece
    return pieces


def diagonal(rows, turn):
    return iota((rows, LANES), 1) == iota((rows, LANES), 0) + rows * turn


def as_row(columns):
    rows = columns[0].shape[0]
    tile = jnp.zeros((rows, LANES), F32)
    for turn, column in enumerate(columns):
        tile = jnp.where(diagonal(rows, turn), column, tile)
    return jnp.sum(tile, axis=0, keepdims=True)


def as_column(row, rows, turns):
    mask = diagonal(rows, turns[0])
    for turn in turns[1:]:
        mask = mask | diagonal(rows, turn)
    return jnp.sum(jnp.where(mask, row, 0.0), axis=1, keepdims=True)


def summed(ref, start, size):
    total = ref[0, pl.ds(start, size)].astype(F32)
    for k in range(1, ref.shape[0]):
        total = total + ref[k, pl.ds(start, size)].astype(F32)
    return total


def k_tokens(tokens, out, tile):
    own = tokens.shape[1]
    tile[...] = jnp.zeros(tile.shape, F32)
    tile[:, :own] = tokens[...].astype(F32)
    placed = pltpu.roll(tile[...], lax.axis_index("tp") * own, 1).astype(BF16)
    for k in range(out.shape[0]):
        out[k] = placed


def k_project(recv, w_query, w_key, w_value, w_forget, w_out, out, x_out, new_rows, wf, sem):
    rows = recv.shape[1]
    width = wf.shape[0]
    start = pl.multiple_of(kv_index() * width, width)
    copy = pltpu.make_async_copy(w_forget.at[pl.ds(start, width)], wf, sem)
    copy.start()
    x = summed(recv, 0, rows)
    x_out[...] = x
    xb = x.astype(BF16)
    query = jnp.dot(xb, w_query[...], preferred_element_type=F32)
    key = jnp.dot(xb, w_key[...], preferred_element_type=F32)
    value = jnp.dot(xb, w_value[...], preferred_element_type=F32)
    new_rows[:, :DH] = key
    new_rows[:, DH:] = value
    out_sums = lax.dot_general(
        jnp.ones((8, LANES), BF16), w_out[...], (((1,), (1,)), ((), ())), preferred_element_type=F32
    )
    sums_hi, sums_lo = in_pieces(out_sums, 2)
    token_col = jnp.sum(x, axis=1, keepdims=True)
    copy.wait()
    forget = jnp.dot(xb, wf[...], preferred_element_type=F32)
    mine = iota(forget.shape, 1) == lax.axis_index("tp")
    forget_col = jnp.sum(jnp.where(mine, forget, 0.0), axis=1, keepdims=True)
    small = as_row([*in_pieces(forget_col, 2), *in_pieces(token_col, 2)])
    row = iota((8, LANES), 0)
    tail = jnp.where(row == 1, small, 0.0)
    tail = jnp.where(row == 2, sums_hi[:, :LANES], tail)
    tail = jnp.where(row == 3, sums_hi[:, LANES:], tail)
    tail = jnp.where(row == 4, sums_lo[:, :LANES], tail)
    tail = jnp.where(row == 5, sums_lo[:, LANES:], tail)
    left = query[:, :LANES].astype(BF16)
    right = query[:, LANES:].astype(BF16)
    for b in range(rows):
        own_tail = jnp.where(row == 0, new_rows[pl.ds(b, 1), :], tail).astype(BF16)
        for k in range(b, out.shape[0], rows):
            out[k, pl.ds(0, rows)] = left
            out[k, pl.ds(rows, rows)] = right
            out[k, pl.ds(2 * rows, 8)] = own_tail


def k_attend(recv, lengths, bias, cache, gate, out, tok_out, sums_out, qs, os):
    rows = cache.shape[0]
    positions = cache.shape[1]
    scale = DH**-0.5
    left = rounded(summed(recv, 0, rows))
    right = rounded(summed(recv, rows, rows))
    tail = summed(recv, 2 * rows, 8)
    new_row = rounded(tail[0:1])
    small = tail[1:2]
    sums_out[0:1, :] = tail[2:3] + tail[4:5]
    sums_out[1:2, :] = tail[3:4] + tail[5:6]
    tok_out[...] = jnp.broadcast_to(as_column(small, rows, (2, 3)), tok_out.shape)
    fetched = as_column(small, rows, (0, 1)) + bias[lax.axis_index("tp")]
    new_gate = jnp.minimum(fetched, 0.0) - jnp.log(1.0 + jnp.exp(-jnp.abs(fetched)))
    low = iota((rows, LANES), 1) < DH
    qs[pl.ds(0, rows)] = jnp.where(low, left, 0.0)
    qs[pl.ds(rows, rows)] = jnp.where(low, pltpu.roll(left, DH, 1), 0.0)
    qs[pl.ds(2 * rows, rows)] = jnp.where(low, right, 0.0)
    qs[pl.ds(3 * rows, rows)] = jnp.where(low, pltpu.roll(right, DH, 1), 0.0)
    qs[pl.ds(4 * rows, 4 * rows)] = jnp.zeros((4 * rows, LANES), F32)
    me = kv_index()
    place = me * positions + iota((8, positions), 1)
    lane = iota((8, LANES), 1)
    for b in range(rows):
        query = qs[pl.ds(b, 8, stride=rows), :]
        block = cache[b]
        scores = lax.dot_general(
            query.astype(BF16), block, (((1,), (1,)), ((), ())), preferred_element_type=F32
        )
        scores = scores * scale + (gate[b] + new_gate[b : b + 1])
        live = place < lengths[b]
        own = jnp.sum(query * new_row, axis=1, keepdims=True) * scale
        own = jnp.where(me == b, own, EMPTY_SCORE)
        top = jnp.max(jnp.where(live, scores, EMPTY_SCORE), axis=1, keepdims=True)
        top = jnp.maximum(top, own)
        weights = jnp.where(live, jnp.exp(scores - top), 0.0)
        own_weight = jnp.where(me == b, jnp.exp(own - top), 0.0)
        total = jnp.sum(weights, axis=1, keepdims=True) + own_weight
        value = jnp.dot(weights.astype(BF16), block, preferred_element_type=F32)
        value = value + rounded(own_weight) * new_row
        value = jnp.where(lane == 0, top, jnp.where(lane == 1, total, value))
        os[pl.ds(b, 8, stride=rows), :] = value
    heads = [os[pl.ds(h * rows, rows)] for h in range(4)]
    low_out = jnp.where(low, pltpu.roll(heads[0], DH, 1), heads[1]).astype(BF16)
    high_out = jnp.where(low, pltpu.roll(heads[2], DH, 1), heads[3]).astype(BF16)
    lane = iota((rows, LANES), 1)
    stats = jnp.zeros((rows, LANES), F32)
    for h in range(4):
        pieces = [*in_pieces(heads[h][:, 0:1], 3), *in_pieces(heads[h][:, 1:2], 2)]
        for k, piece in enumerate(pieces):
            stats = jnp.where(lane == 8 * h + k, piece, stats)
    stats = (stats[:8] + pltpu.roll(stats[8:], 32, 1)).astype(BF16)
    for k in range(out.shape[0]):
        out[k, pl.ds(0, rows)] = low_out
        out[k, pl.ds(rows, rows)] = high_out
        out[k, pl.ds(2 * rows, 8)] = stats


def k_combine(recv, sums, w_out, gain, out, tile):
    devices = recv.shape[0]
    rows = (recv.shape[1] - 8) // 2
    heads = 4 * DH
    source = iota((LANES, 4 * heads), 0)
    column = iota((LANES, 4 * heads), 1)
    half = (column // heads) % 2
    first = 32 * half + 8 * ((column % heads) // DH)
    is_top = column < 2 * heads
    begin = jnp.where(is_top, first, first + 3)
    end = jnp.where(is_top, first + 3, first + 5)
    spread = jnp.where((source >= begin) & (source < end), 1.0, 0.0).astype(BF16)
    stats = recv[:, pl.ds(2 * rows, 8), :].reshape(devices * 8, LANES)
    wide = jnp.dot(stats, spread, preferred_element_type=F32).reshape(devices, 8, 4 * heads)
    blocks = []
    for half in range(2):
        tops = wide[:, :, half * heads : (half + 1) * heads]
        totals = wide[:, :, (2 + half) * heads : (3 + half) * heads]
        scales = jnp.exp(tops - jnp.max(tops, axis=0, keepdims=True))
        total = jnp.sum(totals * scales, axis=0)
        low = recv[:, pl.ds(8 * half, 8), :].astype(F32)
        high = recv[:, pl.ds(rows + 8 * half, 8), :].astype(F32)
        low = jnp.sum(low * scales[:, :, :LANES], axis=0)
        high = jnp.sum(high * scales[:, :, LANES:], axis=0)
        blocks.append(jnp.concatenate([low, high], axis=1) / total)
    attended = jnp.concatenate(blocks, axis=0).astype(BF16)
    attn_part = jnp.dot(attended, w_out[...], preferred_element_type=F32).astype(BF16)
    wide = attended.astype(F32)
    mean = wide[:, :LANES] * sums[0:1, :] + wide[:, LANES:] * sums[1:2, :]
    mean_row = as_row(in_pieces(jnp.sum(mean, axis=1, keepdims=True), 2))
    own = gain.shape[1]
    tile[...] = jnp.zeros(tile.shape, F32)
    tile[0:1, :own] = gain[...]
    gains = in_pieces(pltpu.roll(tile[...], lax.axis_index("tp") * own, 1)[0:1], 3)
    row = iota((8, LANES), 0)
    tail = jnp.where(row == 0, mean_row, 0.0)
    for k, piece in enumerate(gains):
        tail = jnp.where(row == 1 + k, piece, tail)
    tail = tail.astype(BF16)
    for k in range(out.shape[0]):
        out[k, pl.ds(0, rows)] = attn_part
        out[k, pl.ds(rows, 8)] = tail


def k_expand(recv, x, tok, w_gate, w_up, out, scaled_out, tile):
    rows = x.shape[0]
    added = summed(recv, 0, rows)
    tail = summed(recv, rows, 8)
    mean = as_column(tail[0:1], rows, (0, 1))
    gain = tail[1:2] + tail[2:3] + tail[3:4]
    centre = (tok[:, 0:1] + mean) / D
    centred = x[...] + added - centre
    scaled = centred * gain
    scaled_out[...] = scaled
    squares = as_row(in_pieces(jnp.sum(centred * centred, axis=1, keepdims=True), 2))
    scaled = scaled.astype(BF16)
    pieces = tile.shape[0] // (8 * rows)
    tiles = 3 * pieces
    columns = w_gate.shape[1]
    for k, weight in enumerate((w_gate, w_up)):
        part = jnp.dot(scaled, weight[...], preferred_element_type=F32)
        pad = jnp.zeros((rows, tiles * LANES - columns), F32)
        part = jnp.concatenate([part, pad], axis=1)
        for t in range(tiles):
            at = 8 * (t // 3) + 3 * k + t % 3
            tile[pl.ds(at, rows, stride=8 * pieces), :] = part[:, t * LANES : (t + 1) * LANES]
    for h in range(pieces):
        tile[pl.ds(8 * h + 6, rows, stride=8 * pieces), :] = jnp.broadcast_to(
            squares, (rows, LANES)
        )
        tile[pl.ds(8 * h + 7, rows, stride=8 * pieces), :] = jnp.zeros((rows, LANES), F32)
    for k in range(out.shape[0]):
        out[k] = tile[pl.ds(8 * k, 8), :].astype(BF16)


def k_hidden(recv, scaled, out, mid_out):
    rows = scaled.shape[0]
    total = summed(recv, 0, 8)
    spread = as_column(total[6:7], rows, (0, 1)) / D
    shrink = lax.rsqrt(spread + EPSILON)
    mid_out[...] = rounded(scaled[...] * shrink)
    mine = iota((rows, 1), 0) == kv_index() // (out.shape[0] // rows)
    own = jnp.sum(jnp.where(mine, shrink, 0.0), axis=0, keepdims=True)
    total = total * own
    up = pltpu.roll(total, 5, 0)
    hidden = total / (1.0 + jnp.exp(-total)) * up
    hidden = jnp.where(iota((8, LANES), 0) < 3, hidden, 0.0).astype(BF16)
    for k in range(out.shape[0]):
        out[k] = hidden


def k_shrink(recv, w_down, out, tile):
    rows = out.shape[1]
    pieces = recv.shape[0] // rows
    for k in range(recv.shape[0]):
        tile[pl.ds(8 * k, 8), :] = recv[k].astype(F32)
    part = jnp.zeros((rows, LANES), F32)
    columns = w_down.shape[0]
    for t in range(3 * pieces):
        at = 8 * (t // 3) + t % 3
        size = min(LANES, columns - t * LANES)
        hidden = tile[pl.ds(at, rows, stride=8 * pieces), :][:, :size].astype(BF16)
        part = part + jnp.dot(
            hidden, w_down[pl.ds(t * LANES, size), :], preferred_element_type=F32
        )
    part = part.astype(BF16)
    for k in range(out.shape[0]):
        out[k] = part


def k_sums(recv, mid, out, mix_out):
    rows, width = mid.shape
    mixture = mid[...] + summed(recv, 0, rows)
    mix_out[...] = mixture
    centre = jnp.sum(mixture, axis=1, keepdims=True) / width
    square = jnp.sum((mixture - centre) ** 2, axis=1, keepdims=True)
    message = as_row([centre, square])
    for k in range(out.shape[0]):
        out[k] = message


def k_finish(recv, mix, gain, out):
    rows, width = mix.shape
    devices = recv.shape[0]
    total = recv[0]
    for k in range(1, devices):
        total = total + recv[k]
    middle = total / devices
    spread = (recv[0] - middle) ** 2
    for k in range(1, devices):
        spread = spread + (recv[k] - middle) ** 2
    square = jnp.where(iota((1, LANES), 1) < rows, spread * width, total)
    centre = as_column(middle, rows, (0,))
    shrink = lax.rsqrt(as_column(square, rows, (0, 1)) / D + EPSILON)
    own = out.shape[1]
    scaled = (mix[...] - centre) * shrink
    scaled = pltpu.roll(scaled, width - lax.axis_index("tp") * own, 1)[:, :own]
    out[...] = (scaled * gain[...]).astype(BF16)


def on_device(
    tokens,
    live_lengths,
    kv_cache,
    gate_sums,
    w_query,
    w_key,
    w_value,
    w_forget,
    forget_bias,
    w_out,
    first_gain,
    w_gate,
    w_up,
    w_down,
    second_gain,
):
    rows, own = tokens.shape
    kv, tp = lax.axis_size(KV), lax.axis_size("tp")
    width = own * tp
    block = ((rows, LANES), F32)
    (message,) = kernel(
        k_tokens, [((tp, rows, width), BF16)], [VMEM], [pltpu.VMEM((rows, width), F32)]
    )(tokens)
    message, x = kernel(
        k_project,
        [((kv, 2 * rows + 8, LANES), BF16), block],
        [VMEM, VMEM, VMEM, VMEM, ANY, VMEM],
        [
            pltpu.VMEM((rows, LANES), F32),
            pltpu.VMEM((width, w_forget.shape[1]), BF16),
            pltpu.SemaphoreType.DMA,
        ],
    )(exchanged(message, "tp"), w_query, w_key, w_value, w_forget, w_out)
    message, tok, sums = kernel(
        k_attend,
        [((kv, 2 * rows + 8, LANES), BF16), block, ((2, LANES), F32)],
        [VMEM, SMEM, SMEM, VMEM, VMEM],
        [pltpu.VMEM((8 * rows, LANES), F32), pltpu.VMEM((8 * rows, LANES), F32)],
    )(exchanged(message, KV), live_lengths, forget_bias, kv_cache, gate_sums)
    (message,) = kernel(
        k_combine, [((tp, rows + 8, width), BF16)], [VMEM] * 4, [pltpu.VMEM((8, width), F32)]
    )(exchanged(message, KV), sums, w_out, first_gain[None])
    message, scaled = kernel(
        k_expand,
        [((kv, 8, LANES), BF16), block],
        [VMEM] * 5,
        [pltpu.VMEM((8 * kv, LANES), F32)],
    )(exchanged(message, "tp"), x, tok, w_gate, w_up)
    message, mid = kernel(k_hidden, [((kv, 8, LANES), BF16), block], [VMEM] * 2)(
        exchanged(message, KV), scaled
    )
    (message,) = kernel(
        k_shrink, [((tp, rows, width), BF16)], [VMEM] * 2, [pltpu.VMEM((8 * kv, LANES), F32)]
    )(exchanged(message, KV), w_down)
    message, mix = kernel(k_sums, [((kv, 1, LANES), F32), block], [VMEM] * 2)(
        exchanged(message, "tp"), mid
    )
    (out,) = kernel(k_finish, [((rows, own), BF16)], [VMEM] * 3)(
        exchanged(message, KV), mix, second_gain[None]
    )
    return out


def solution(mesh):
    split = Mesh(mesh.devices.reshape(8, 4, mesh.shape["tp"]), ("kv_0", "kv_1", "tp"))
    placed = (
        P(None, KV_TP),
        P(),
        P(None, KV, "tp"),
        P(None, "tp", KV),
        P(KV, "tp"),
        P(KV, "tp"),
        P(KV, "tp"),
        P(),
        P(),
        P("tp", KV),
        P(KV_TP),
        P(KV, "tp"),
        P(KV, "tp"),
        P("tp", KV),
        P(KV_TP),
    )
    return jax.shard_map(
        on_device, mesh=split, in_specs=placed, out_specs=P(None, KV_TP), check_vma=False
    )
```

```python
import jax
import jax.numpy as jnp
from jax import lax
from jax.experimental import pallas as pl
from jax.experimental.pallas import tpu as pltpu
from jax.sharding import Mesh
from jax.sharding import PartitionSpec as P

D = 4096
DH = 64
LANES = 128
KV = ("kv_0", "kv_1")
KV_TP = ("kv_0", "kv_1", "tp")
EPSILON = 1e-05
EMPTY_SCORE = -1e30
F32 = jnp.float32
BF16 = jnp.bfloat16

VMEM = pl.BlockSpec(memory_space=pltpu.VMEM)
SMEM = pl.BlockSpec(memory_space=pltpu.SMEM)
ANY = pl.BlockSpec(memory_space=pl.ANY)


def kernel(body, outs, specs, scratch=()):
    return pl.pallas_call(
        body,
        out_shape=[pltpu.VMEM(shape, dtype) for shape, dtype in outs],
        in_specs=specs,
        out_specs=[VMEM] * len(outs),
        scratch_shapes=scratch,
        compiler_params=pltpu.CompilerParams(vmem_limit_bytes=8 * 2**20),
    )


def exchanged(pieces, axis):
    return lax.all_to_all(pieces, axis, 0, 0, tiled=True)


def kv_index():
    return lax.axis_index("kv_0") * lax.axis_size("kv_1") + lax.axis_index("kv_1")


def iota(shape, dim):
    return lax.broadcasted_iota(jnp.int32, shape, dim)


def rounded(x):
    return x.astype(BF16).astype(F32)


def in_pieces(value, count):
    pieces = []
    for _ in range(count):
        piece = rounded(value)
        pieces.append(piece)
        value = value - piece
    return pieces


def diagonal(rows, turn):
    return iota((rows, LANES), 1) == iota((rows, LANES), 0) + rows * turn


def across(left, right, sides):
    return lax.dot_general(left, right, (sides, ((), ())), preferred_element_type=F32)


LAST = ((1,), (1,))
FIRST = ((0,), (0,))


def as_row(columns):
    rows = columns[0].shape[0]
    tile = jnp.zeros((rows, LANES), F32)
    for turn, column in enumerate(columns):
        tile = jnp.where(diagonal(rows, turn), column, tile)
    return jnp.sum(tile, axis=0, keepdims=True)


def as_column(row, rows, turns):
    mask = diagonal(rows, turns[0])
    for turn in turns[1:]:
        mask = mask | diagonal(rows, turn)
    return jnp.sum(jnp.where(mask, row, 0.0), axis=1, keepdims=True)


def summed(ref, start, size):
    total = ref[0, pl.ds(start, size)].astype(F32)
    for k in range(1, ref.shape[0]):
        total = total + ref[k, pl.ds(start, size)].astype(F32)
    return total


def k_project(recv, w_query, w_key, w_value, w_forget, w_out, out, x_out, new_rows, wf, sem):
    rows = recv.shape[1]
    width = wf.shape[1]
    start = pl.multiple_of(kv_index() * width, width)
    copy = pltpu.make_async_copy(w_forget.at[:, pl.ds(start, width)], wf, sem)
    copy.start()
    same = jnp.where(iota((width, width), 0) == iota((width, width), 1), 1.0, 0.0).astype(BF16)
    x = across(recv[...], same, FIRST)
    x_out[...] = x
    rows = x.shape[0]
    xb = x.astype(BF16)
    query = jnp.dot(xb, w_query[...], preferred_element_type=F32)
    new_rows[:, :DH] = across(xb, w_key[...], LAST)
    new_rows[:, DH:] = across(xb, w_value[...], LAST)
    out_sums = across(jnp.ones((8, LANES), BF16), w_out[...], LAST)
    sums_hi, sums_lo = in_pieces(out_sums, 2)
    token_col = jnp.sum(x, axis=1, keepdims=True)
    copy.wait()
    forget = across(xb, wf[...], LAST)
    mine = iota(forget.shape, 1) == lax.axis_index("tp")
    forget_col = jnp.sum(jnp.where(mine, forget, 0.0), axis=1, keepdims=True)
    small = as_row([*in_pieces(forget_col, 2), *in_pieces(token_col, 2)])
    row = iota((8, LANES), 0)
    tail = jnp.where(row == 1, small, 0.0)
    tail = jnp.where(row == 2, sums_hi[:, :LANES], tail)
    tail = jnp.where(row == 3, sums_hi[:, LANES:], tail)
    tail = jnp.where(row == 4, sums_lo[:, :LANES], tail)
    tail = jnp.where(row == 5, sums_lo[:, LANES:], tail)
    left = query[:, :LANES].astype(BF16)
    right = query[:, LANES:].astype(BF16)
    for b in range(rows):
        own_tail = jnp.where(row == 0, new_rows[pl.ds(b, 1), :], tail).astype(BF16)
        for k in range(b, out.shape[0], rows):
            out[k, pl.ds(0, rows)] = left
            out[k, pl.ds(rows, rows)] = right
            out[k, pl.ds(2 * rows, 8)] = own_tail


def k_attend(recv, lengths, bias, cache, gate, out, tok_out, sums_out, qs, os):
    rows = cache.shape[0]
    positions = cache.shape[1]
    scale = DH**-0.5
    left = rounded(summed(recv, 0, rows))
    right = rounded(summed(recv, rows, rows))
    tail = summed(recv, 2 * rows, 8)
    new_row = rounded(tail[0:1])
    small = tail[1:2]
    sums_out[0:1, :] = tail[2:3] + tail[4:5]
    sums_out[1:2, :] = tail[3:4] + tail[5:6]
    tok_out[...] = jnp.broadcast_to(as_column(small, rows, (2, 3)), tok_out.shape)
    fetched = as_column(small, rows, (0, 1)) + bias[lax.axis_index("tp")]
    new_gate = jnp.minimum(fetched, 0.0) - jnp.log(1.0 + jnp.exp(-jnp.abs(fetched)))
    low = iota((rows, LANES), 1) < DH
    qs[pl.ds(0, rows)] = jnp.where(low, left, 0.0)
    qs[pl.ds(rows, rows)] = jnp.where(low, pltpu.roll(left, DH, 1), 0.0)
    qs[pl.ds(2 * rows, rows)] = jnp.where(low, right, 0.0)
    qs[pl.ds(3 * rows, rows)] = jnp.where(low, pltpu.roll(right, DH, 1), 0.0)
    qs[pl.ds(4 * rows, 4 * rows)] = jnp.zeros((4 * rows, LANES), F32)
    me = kv_index()
    place = me * positions + iota((8, positions), 1)
    lane = iota((8, LANES), 1)
    for b in range(rows):
        query = qs[pl.ds(b, 8, stride=rows), :]
        block = cache[b]
        scores = lax.dot_general(
            query.astype(BF16), block, (((1,), (1,)), ((), ())), preferred_element_type=F32
        )
        scores = scores * scale + (gate[b] + new_gate[b : b + 1])
        live = place < lengths[b]
        own = jnp.sum(query * new_row, axis=1, keepdims=True) * scale
        own = jnp.where(me == b, own, EMPTY_SCORE)
        top = jnp.max(jnp.where(live, scores, EMPTY_SCORE), axis=1, keepdims=True)
        top = jnp.maximum(top, own)
        weights = jnp.where(live, jnp.exp(scores - top), 0.0)
        own_weight = jnp.where(me == b, jnp.exp(own - top), 0.0)
        total = jnp.sum(weights, axis=1, keepdims=True) + own_weight
        value = jnp.dot(weights.astype(BF16), block, preferred_element_type=F32)
        value = value + rounded(own_weight) * new_row
        value = jnp.where(lane == 0, top, jnp.where(lane == 1, total, value))
        os[pl.ds(b, 8, stride=rows), :] = value
    heads = [os[pl.ds(h * rows, rows)] for h in range(4)]
    low_out = jnp.where(low, pltpu.roll(heads[0], DH, 1), heads[1]).astype(BF16)
    high_out = jnp.where(low, pltpu.roll(heads[2], DH, 1), heads[3]).astype(BF16)
    lane = iota((rows, LANES), 1)
    stats = jnp.zeros((rows, LANES), F32)
    for h in range(4):
        pieces = [*in_pieces(heads[h][:, 0:1], 3), *in_pieces(heads[h][:, 1:2], 2)]
        for k, piece in enumerate(pieces):
            stats = jnp.where(lane == 8 * h + k, piece, stats)
    stats = (stats[:8] + pltpu.roll(stats[8:], 32, 1)).astype(BF16)
    for k in range(out.shape[0]):
        out[k, pl.ds(0, rows)] = low_out
        out[k, pl.ds(rows, rows)] = high_out
        out[k, pl.ds(2 * rows, 8)] = stats


def k_combine(recv, sums, w_out, gain, out, tile):
    devices = recv.shape[0]
    rows = (recv.shape[1] - 8) // 2
    heads = 4 * DH
    source = iota((LANES, 4 * heads), 0)
    column = iota((LANES, 4 * heads), 1)
    half = (column // heads) % 2
    first = 32 * half + 8 * ((column % heads) // DH)
    is_top = column < 2 * heads
    begin = jnp.where(is_top, first, first + 3)
    end = jnp.where(is_top, first + 3, first + 5)
    spread = jnp.where((source >= begin) & (source < end), 1.0, 0.0).astype(BF16)
    stats = recv[:, pl.ds(2 * rows, 8), :].reshape(devices * 8, LANES)
    wide = jnp.dot(stats, spread, preferred_element_type=F32).reshape(devices, 8, 4 * heads)
    blocks = []
    for half in range(2):
        tops = wide[:, :, half * heads : (half + 1) * heads]
        totals = wide[:, :, (2 + half) * heads : (3 + half) * heads]
        scales = jnp.exp(tops - jnp.max(tops, axis=0, keepdims=True))
        total = jnp.sum(totals * scales, axis=0)
        low = recv[:, pl.ds(8 * half, 8), :].astype(F32)
        high = recv[:, pl.ds(rows + 8 * half, 8), :].astype(F32)
        low = jnp.sum(low * scales[:, :, :LANES], axis=0)
        high = jnp.sum(high * scales[:, :, LANES:], axis=0)
        blocks.append(jnp.concatenate([low, high], axis=1) / total)
    attended = jnp.concatenate(blocks, axis=0).astype(BF16)
    attn_part = jnp.dot(attended, w_out[...], preferred_element_type=F32).astype(BF16)
    wide = attended.astype(F32)
    mean = wide[:, :LANES] * sums[0:1, :] + wide[:, LANES:] * sums[1:2, :]
    mean_row = as_row(in_pieces(jnp.sum(mean, axis=1, keepdims=True), 2))
    own = gain.shape[1]
    tile[...] = jnp.zeros(tile.shape, F32)
    tile[0:1, :own] = gain[...]
    gains = in_pieces(pltpu.roll(tile[...], lax.axis_index("tp") * own, 1)[0:1], 3)
    row = iota((8, LANES), 0)
    tail = jnp.where(row == 0, mean_row, 0.0)
    for k, piece in enumerate(gains):
        tail = jnp.where(row == 1 + k, piece, tail)
    tail = tail.astype(BF16)
    for k in range(out.shape[0]):
        out[k, pl.ds(0, rows)] = attn_part
        out[k, pl.ds(rows, 8)] = tail


def k_expand(recv, x, tok, w_gate, w_up, out, scaled_out, tile):
    rows = x.shape[0]
    added = summed(recv, 0, rows)
    tail = summed(recv, rows, 8)
    mean = as_column(tail[0:1], rows, (0, 1))
    gain = tail[1:2] + tail[2:3] + tail[3:4]
    centre = (tok[:, 0:1] + mean) / D
    centred = x[...] + added - centre
    scaled = centred * gain
    scaled_out[...] = scaled
    squares = as_row(in_pieces(jnp.sum(centred * centred, axis=1, keepdims=True), 2))
    scaled = scaled.astype(BF16)
    pieces = tile.shape[0] // (8 * rows)
    tiles = 3 * pieces
    columns = w_gate.shape[0]
    for k, weight in enumerate((w_gate, w_up)):
        part = across(scaled, weight[...], LAST)
        pad = jnp.zeros((rows, tiles * LANES - columns), F32)
        part = jnp.concatenate([part, pad], axis=1)
        for t in range(tiles):
            at = 8 * (t // 3) + 3 * k + t % 3
            tile[pl.ds(at, rows, stride=8 * pieces), :] = part[:, t * LANES : (t + 1) * LANES]
    for h in range(pieces):
        tile[pl.ds(8 * h + 6, rows, stride=8 * pieces), :] = jnp.broadcast_to(
            squares, (rows, LANES)
        )
        tile[pl.ds(8 * h + 7, rows, stride=8 * pieces), :] = jnp.zeros((rows, LANES), F32)
    for k in range(out.shape[0]):
        out[k] = tile[pl.ds(8 * k, 8), :].astype(BF16)


def k_hidden(recv, scaled, out, mid_out):
    rows = scaled.shape[0]
    total = summed(recv, 0, 8)
    spread = as_column(total[6:7], rows, (0, 1)) / D
    shrink = lax.rsqrt(spread + EPSILON)
    mid_out[...] = rounded(scaled[...] * shrink)
    mine = iota((rows, 1), 0) == kv_index() // (out.shape[0] // rows)
    own = jnp.sum(jnp.where(mine, shrink, 0.0), axis=0, keepdims=True)
    total = total * own
    up = pltpu.roll(total, 5, 0)
    hidden = total / (1.0 + jnp.exp(-total)) * up
    hidden = jnp.where(iota((8, LANES), 0) < 3, hidden, 0.0).astype(BF16)
    for k in range(out.shape[0]):
        out[k] = hidden


def k_shrink(recv, w_down, out, tile):
    rows = out.shape[1]
    pieces = recv.shape[0] // rows
    for k in range(recv.shape[0]):
        tile[pl.ds(8 * k, 8), :] = recv[k].astype(F32)
    part = jnp.zeros((rows, LANES), F32)
    columns = w_down.shape[0]
    for t in range(3 * pieces):
        at = 8 * (t // 3) + t % 3
        size = min(LANES, columns - t * LANES)
        hidden = tile[pl.ds(at, rows, stride=8 * pieces), :][:, :size].astype(BF16)
        part = part + jnp.dot(
            hidden, w_down[pl.ds(t * LANES, size), :], preferred_element_type=F32
        )
    part = part.astype(BF16)
    for k in range(out.shape[0]):
        out[k] = part


def k_sums(recv, mid, out, mix_out):
    rows, width = mid.shape
    mixture = mid[...] + summed(recv, 0, rows)
    mix_out[...] = mixture
    centre = jnp.sum(mixture, axis=1, keepdims=True) / width
    square = jnp.sum((mixture - centre) ** 2, axis=1, keepdims=True)
    message = as_row([centre, square])
    for k in range(out.shape[0]):
        out[k] = message


def k_finish(recv, mix, gain, out, turned):
    rows, width = mix.shape
    devices = recv.shape[0]
    total = recv[0]
    for k in range(1, devices):
        total = total + recv[k]
    middle = total / devices
    spread = (recv[0] - middle) ** 2
    for k in range(1, devices):
        spread = spread + (recv[k] - middle) ** 2
    square = jnp.where(iota((1, LANES), 1) < rows, spread * width, total)
    centre = as_column(middle, rows, (0,))
    shrink = lax.rsqrt(as_column(square, rows, (0, 1)) / D + EPSILON)
    own = out.shape[0]
    scaled = ((mix[...] - centre) * shrink).T
    at = pl.multiple_of(lax.axis_index("tp") * own, own)
    turned[...] = scaled
    gain_col = jnp.sum(jnp.where(diagonal(own, 0)[:, :own], gain[...], 0.0), axis=1, keepdims=True)
    out[...] = (turned[pl.ds(at, own), :] * gain_col).astype(BF16)


def on_device(
    tokens,
    live_lengths,
    kv_cache,
    gate_sums,
    w_query,
    w_key,
    w_value,
    w_forget,
    forget_bias,
    w_out,
    first_gain,
    w_gate,
    w_up,
    w_down,
    second_gain,
):
    rows, own = tokens.shape
    kv, tp = lax.axis_size(KV), lax.axis_size("tp")
    width = own * tp
    block = ((rows, LANES), F32)
    message = jnp.broadcast_to(tokens.T[None], (tp, own, rows))
    message, x = kernel(
        k_project,
        [((kv, 2 * rows + 8, LANES), BF16), block],
        [VMEM, VMEM, VMEM, VMEM, ANY, VMEM],
        [
            pltpu.VMEM((rows, LANES), F32),
            pltpu.VMEM((w_forget.shape[1], width), BF16),
            pltpu.SemaphoreType.DMA,
        ],
    )(
        exchanged(message, "tp").reshape(width, rows),
        w_query,
        w_key.T,
        w_value.T,
        w_forget.T,
        w_out,
    )
    message, tok, sums = kernel(
        k_attend,
        [((kv, 2 * rows + 8, LANES), BF16), block, ((2, LANES), F32)],
        [VMEM, SMEM, SMEM, VMEM, VMEM],
        [pltpu.VMEM((8 * rows, LANES), F32), pltpu.VMEM((8 * rows, LANES), F32)],
    )(exchanged(message, KV), live_lengths, forget_bias, kv_cache, gate_sums)
    (message,) = kernel(
        k_combine, [((tp, rows + 8, width), BF16)], [VMEM] * 4, [pltpu.VMEM((8, width), F32)]
    )(exchanged(message, KV), sums, w_out, first_gain[None])
    message, scaled = kernel(
        k_expand,
        [((kv, 8, LANES), BF16), block],
        [VMEM] * 5,
        [pltpu.VMEM((8 * kv, LANES), F32)],
    )(exchanged(message, "tp"), x, tok, w_gate.T, w_up.T)
    message, mid = kernel(k_hidden, [((kv, 8, LANES), BF16), block], [VMEM] * 2)(
        exchanged(message, KV), scaled
    )
    (message,) = kernel(
        k_shrink, [((tp, rows, width), BF16)], [VMEM] * 2, [pltpu.VMEM((8 * kv, LANES), F32)]
    )(exchanged(message, KV), w_down)
    message, mix = kernel(k_sums, [((kv, 1, LANES), F32), block], [VMEM] * 2)(
        exchanged(message, "tp"), mid
    )
    (out,) = kernel(
        k_finish, [((own, rows), BF16)], [VMEM] * 3, [pltpu.VMEM((width, rows), F32)]
    )(exchanged(message, KV), mix, second_gain[None])
    return out.T


def solution(mesh):
    split = Mesh(mesh.devices.reshape(8, 4, mesh.shape["tp"]), ("kv_0", "kv_1", "tp"))
    placed = (
        P(None, KV_TP),
        P(),
        P(None, KV, "tp"),
        P(None, "tp", KV),
        P(KV, "tp"),
        P(KV, "tp"),
        P(KV, "tp"),
        P(),
        P(),
        P("tp", KV),
        P(KV_TP),
        P(KV, "tp"),
        P(KV, "tp"),
        P("tp", KV),
        P(KV_TP),
    )
    return jax.shard_map(
        on_device, mesh=split, in_specs=placed, out_specs=P(None, KV_TP), check_vma=False
    )
```

```python
import functools

import jax
import jax.numpy as jnp
from jax import lax
from jax.experimental import pallas as pl
from jax.experimental.pallas import tpu as pltpu
from jax.sharding import Mesh
from jax.sharding import PartitionSpec as P

D = 4096
DH = 64
LANES = 128
KV = ("kv_0", "kv_1")
KV_TP = ("kv_0", "kv_1", "tp")
EPSILON = 1e-05
EMPTY_SCORE = -1e30
F32 = jnp.float32
BF16 = jnp.bfloat16

VMEM = pl.BlockSpec(memory_space=pltpu.VMEM)
SMEM = pl.BlockSpec(memory_space=pltpu.SMEM)
ANY = pl.BlockSpec(memory_space=pl.ANY)


def kernel(body, outs, specs, scratch=(), last=False):
    return pl.pallas_call(
        body,
        out_shape=[
            jax.ShapeDtypeStruct(shape, dtype) if last else pltpu.VMEM(shape, dtype)
            for shape, dtype in outs
        ],
        in_specs=specs,
        out_specs=[VMEM] * len(outs),
        scratch_shapes=scratch,
        compiler_params=pltpu.CompilerParams(vmem_limit_bytes=8 * 2**20),
    )


def exchanged(pieces, axis):
    return lax.all_to_all(pieces, axis, 0, 0, tiled=True)


def kv_index():
    return lax.axis_index("kv_0") * lax.axis_size("kv_1") + lax.axis_index("kv_1")


def iota(shape, dim):
    return lax.broadcasted_iota(jnp.int32, shape, dim)


def rounded(x):
    return x.astype(BF16).astype(F32)


def in_pieces(value, count):
    pieces = []
    for _ in range(count):
        piece = rounded(value)
        pieces.append(piece)
        value = value - piece
    return pieces


def diagonal(rows, turn):
    return iota((rows, LANES), 1) == iota((rows, LANES), 0) + rows * turn


def across(left, right, sides):
    return lax.dot_general(left, right, (sides, ((), ())), preferred_element_type=F32)


LAST = ((1,), (1,))
FIRST = ((0,), (0,))


def as_row(columns):
    rows = columns[0].shape[0]
    tile = jnp.zeros((rows, LANES), F32)
    for turn, column in enumerate(columns):
        tile = jnp.where(diagonal(rows, turn), column, tile)
    return jnp.sum(tile, axis=0, keepdims=True)


def as_column(row, rows, turns):
    mask = diagonal(rows, turns[0])
    for turn in turns[1:]:
        mask = mask | diagonal(rows, turn)
    return jnp.sum(jnp.where(mask, row, 0.0), axis=1, keepdims=True)


def summed(ref, start, size):
    total = ref[0, pl.ds(start, size)].astype(F32)
    for k in range(1, ref.shape[0]):
        total = total + ref[k, pl.ds(start, size)].astype(F32)
    return total


def k_weights(query, key, value, forget, w_out, gain, bias, query_o, key_o, value_o, forget_o, w_out_o, tail_o, sem):
    width = forget_o.shape[1]
    start = pl.multiple_of(kv_index() * width, width)
    pairs = [(w_out, w_out_o), (query, query_o), (key, key_o), (value, value_o)]
    pairs.append((forget.at[:, pl.ds(start, width)], forget_o))
    copies = [pltpu.make_async_copy(a, b, sem.at[k]) for k, (a, b) in enumerate(pairs)]
    for copy in copies:
        copy.start()
    own = gain.shape[1]
    spread = jnp.where(iota((own, LANES), 1) == iota((own, LANES), 0) + lax.axis_index("tp") * own, 1.0, 0.0)
    column = jnp.sum(jnp.where(diagonal(own, 0)[:, :own], gain[...], 0.0), axis=1, keepdims=True)
    gains = in_pieces(jnp.sum(spread * column, axis=0, keepdims=True), 3)
    row = iota((8, LANES), 0)
    for copy in copies:
        copy.wait()
    sums = across(jnp.ones((8, LANES), BF16), w_out_o[...], LAST)
    sums_hi, sums_lo = in_pieces(sums, 2)
    tail = jnp.where(row == 2, sums_hi[:, :LANES], 0.0)
    tail = jnp.where(row == 3, sums_hi[:, LANES:], tail)
    tail = jnp.where(row == 4, sums_lo[:, :LANES], tail)
    tail_o[0] = jnp.where(row == 5, sums_lo[:, LANES:], tail)
    mine = iota(bias.shape, 1) == lax.axis_index("tp")
    once = jnp.where(kv_index() == 0, 1.0, 0.0)
    own_bias = jnp.sum(jnp.where(mine, bias[...], 0.0), axis=1, keepdims=True) * once
    tail = jnp.where(row == 0, own_bias, 0.0)
    for k, piece in enumerate(gains):
        tail = jnp.where(row == 1 + k, piece, tail)
    tail_o[1] = tail


def k_project(recv, w_query, w_key, w_value, wf, tails, out, x_out, new_rows):
    width = wf.shape[1]
    same = jnp.where(iota((width, width), 0) == iota((width, width), 1), 1.0, 0.0).astype(BF16)
    x = across(recv[...], same, FIRST)
    x_out[...] = x
    rows = x.shape[0]
    xb = x.astype(BF16)
    query = jnp.dot(xb, w_query[...], preferred_element_type=F32)
    new_rows[:, :DH] = across(xb, w_key[...], LAST)
    new_rows[:, DH:] = across(xb, w_value[...], LAST)
    forget = across(xb, wf[...], LAST)
    token_col = jnp.sum(x, axis=1, keepdims=True)
    mine = iota(forget.shape, 1) == lax.axis_index("tp")
    forget_col = jnp.sum(jnp.where(mine, forget, 0.0), axis=1, keepdims=True)
    forget_col = forget_col + tails[1, 0:1, 0:1]
    small = as_row([*in_pieces(forget_col, 2), *in_pieces(token_col, 2)])
    row = iota((8, LANES), 0)
    tail = jnp.where(row == 1, small, tails[0])
    left = query[:, :LANES].astype(BF16)
    right = query[:, LANES:].astype(BF16)
    for b in range(rows):
        own_tail = jnp.where(row == 0, new_rows[pl.ds(b, 1), :], tail).astype(BF16)
        for k in range(b, out.shape[0], rows):
            out[k, pl.ds(0, rows)] = left
            out[k, pl.ds(rows, rows)] = right
            out[k, pl.ds(2 * rows, 8)] = own_tail


def k_prepare(lengths, cache, gate, cache_o, keys_o, gate_o, gate_v, sem, gate_sem):
    rows, positions = cache.shape[:2]
    copies = [pltpu.make_async_copy(cache.at[b], cache_o.at[b], sem.at[b]) for b in range(rows)]
    gates = pltpu.make_async_copy(gate, gate_v, gate_sem)
    gates.start()
    for copy in copies:
        copy.start()
    gates.wait()
    place = kv_index() * positions + iota((8, positions), 1)
    first = iota((8, positions), 0) < 4
    for m in range(rows // 2):
        one = jnp.where(place < lengths[2 * m], gate_v[2 * m], EMPTY_SCORE)
        two = jnp.where(place < lengths[2 * m + 1], gate_v[2 * m + 1], EMPTY_SCORE)
        gate_o[m] = jnp.where(first, one, two)
    for b in range(rows):
        copies[b].wait()
        keys_o[b // 2, pl.ds(DH * (b % 2), DH), :] = cache_o[b].T[:DH]


def k_attend(recv, cache, keys, gate, out, tok_out, sums_out, qs, os):
    rows = cache.shape[0]
    heads = 4
    scale = DH**-0.5
    left = rounded(summed(recv, 0, rows))
    right = rounded(summed(recv, rows, rows))
    tail = summed(recv, 2 * rows, 8)
    new_row = rounded(tail[0:1])
    small = tail[1:2]
    sums_out[0:1, :] = tail[2:3] + tail[4:5]
    sums_out[1:2, :] = tail[3:4] + tail[5:6]
    tok_out[...] = jnp.broadcast_to(as_column(small, rows, (2, 3)), tok_out.shape)
    even = iota((rows, LANES), 0) % 2 == 0
    low = iota((rows, LANES), 1) < DH
    keep = even == low
    left_turned = pltpu.roll(left, DH, 1)
    right_turned = pltpu.roll(right, DH, 1)
    placed = (
        jnp.where(even, left, left_turned),
        jnp.where(even, left_turned, left),
        jnp.where(even, right, right_turned),
        jnp.where(even, right_turned, right),
    )
    for h, block in enumerate(placed):
        qs[pl.ds(h, rows, stride=heads), :] = jnp.where(keep, block, 0.0)
    all_rows = rows * heads
    owner = iota((all_rows, LANES), 0) // heads
    lane = iota((all_rows, LANES), 1)
    fetched = jnp.where((lane == owner) | (lane == owner + rows), small, 0.0)
    fetched = jnp.sum(fetched, axis=1, keepdims=True)
    new_gate = jnp.minimum(fetched, 0.0) - jnp.log(1.0 + jnp.exp(-jnp.abs(fetched)))
    lane = iota((1, LANES), 1)
    new_key = jnp.where(lane < DH, new_row, pltpu.roll(jnp.broadcast_to(new_row, (8, LANES)), DH, 1)[0:1])
    own = jnp.sum(qs[...] * new_key, axis=1, keepdims=True) * scale
    mine = iota((all_rows, 1), 0) // heads == kv_index()
    own = jnp.where(mine, own, EMPTY_SCORE)
    lane = iota((8, LANES), 1)
    first = iota((8, LANES), 0) < heads
    for m in range(rows // 2):
        at = slice(8 * m, 8 * m + 8)
        scores = jnp.dot(
            qs[pl.ds(8 * m, 8), :].astype(BF16), keys[m], preferred_element_type=F32
        )
        scores = scores * scale + (gate[m] + new_gate[at])
        top = jnp.maximum(jnp.max(scores, axis=1, keepdims=True), own[at])
        top = jnp.maximum(top, 0.1 * EMPTY_SCORE)
        weights = jnp.exp(scores - top)
        own_weight = jnp.exp(own[at] - top)
        total = jnp.sum(weights, axis=1, keepdims=True) + own_weight
        block = jnp.concatenate([cache[2 * m], cache[2 * m + 1]], axis=1)
        value = jnp.dot(weights.astype(BF16), block, preferred_element_type=F32)
        value = jnp.where(first, value[:, :LANES], value[:, LANES:])
        value = value + rounded(own_weight) * new_row
        os[pl.ds(8 * m, 8), :] = jnp.where(lane == 0, top, jnp.where(lane == 1, total, value))
    blocks = [os[pl.ds(h, rows, stride=heads), :] for h in range(heads)]
    low_out = jnp.where(low, pltpu.roll(blocks[0], DH, 1), blocks[1]).astype(BF16)
    high_out = jnp.where(low, pltpu.roll(blocks[2], DH, 1), blocks[3]).astype(BF16)
    lane = iota((rows, LANES), 1)
    stats = jnp.zeros((rows, LANES), F32)
    for h in range(heads):
        pieces = [*in_pieces(blocks[h][:, 0:1], 3), *in_pieces(blocks[h][:, 1:2], 2)]
        for k, piece in enumerate(pieces):
            stats = jnp.where(lane == 8 * h + k, piece, stats)
    stats = (stats[:8] + pltpu.roll(stats[8:], 32, 1)).astype(BF16)
    for k in range(out.shape[0]):
        out[k, pl.ds(0, rows)] = low_out
        out[k, pl.ds(rows, rows)] = high_out
        out[k, pl.ds(2 * rows, 8)] = stats


def k_combine(recv, sums, w_out, tails, out):
    devices = recv.shape[0]
    rows = (recv.shape[1] - 8) // 2
    heads = 4 * DH
    source = iota((LANES, 4 * heads), 0)
    column = iota((LANES, 4 * heads), 1)
    half = (column // heads) % 2
    first = 32 * half + 8 * ((column % heads) // DH)
    is_top = column < 2 * heads
    begin = jnp.where(is_top, first, first + 3)
    end = jnp.where(is_top, first + 3, first + 5)
    spread = jnp.where((source >= begin) & (source < end), 1.0, 0.0).astype(BF16)
    stats = recv[:, pl.ds(2 * rows, 8), :].reshape(devices * 8, LANES)
    wide = jnp.dot(stats, spread, preferred_element_type=F32).reshape(devices, 8, 4 * heads)
    blocks = []
    for half in range(2):
        tops = wide[:, :, half * heads : (half + 1) * heads]
        totals = wide[:, :, (2 + half) * heads : (3 + half) * heads]
        scales = jnp.exp(tops - jnp.max(tops, axis=0, keepdims=True))
        total = jnp.sum(totals * scales, axis=0)
        low = recv[:, pl.ds(8 * half, 8), :].astype(F32)
        high = recv[:, pl.ds(rows + 8 * half, 8), :].astype(F32)
        low = jnp.sum(low * scales[:, :, :LANES], axis=0)
        high = jnp.sum(high * scales[:, :, LANES:], axis=0)
        blocks.append(jnp.concatenate([low, high], axis=1) / total)
    attended = jnp.concatenate(blocks, axis=0).astype(BF16)
    attn_part = jnp.dot(attended, w_out[...], preferred_element_type=F32).astype(BF16)
    wide = attended.astype(F32)
    mean = wide[:, :LANES] * sums[0:1, :] + wide[:, LANES:] * sums[1:2, :]
    mean_row = as_row(in_pieces(jnp.sum(mean, axis=1, keepdims=True), 2))
    row = iota((8, LANES), 0)
    tail = jnp.where(row == 0, mean_row, tails[1])
    tail = tail.astype(BF16)
    for k in range(out.shape[0]):
        out[k, pl.ds(0, rows)] = attn_part
        out[k, pl.ds(rows, 8)] = tail


def k_expand(recv, x, tok, w_gate, w_up, out, scaled_out, tile):
    rows = x.shape[0]
    added = summed(recv, 0, rows)
    tail = summed(recv, rows, 8)
    mean = as_column(tail[0:1], rows, (0, 1))
    gain = tail[1:2] + tail[2:3] + tail[3:4]
    centre = (tok[:, 0:1] + mean) / D
    centred = x[...] + added - centre
    scaled = centred * gain
    scaled_out[...] = scaled
    squares = as_row(in_pieces(jnp.sum(centred * centred, axis=1, keepdims=True), 2))
    scaled = scaled.astype(BF16)
    pieces = tile.shape[0] // (8 * rows)
    tiles = 3 * pieces
    columns = w_gate.shape[0]
    for k, weight in enumerate((w_gate, w_up)):
        part = across(scaled, weight[...], LAST)
        pad = jnp.zeros((rows, tiles * LANES - columns), F32)
        part = jnp.concatenate([part, pad], axis=1)
        for t in range(tiles):
            at = 8 * (t // 3) + 3 * k + t % 3
            tile[pl.ds(at, rows, stride=8 * pieces), :] = part[:, t * LANES : (t + 1) * LANES]
    for h in range(pieces):
        tile[pl.ds(8 * h + 6, rows, stride=8 * pieces), :] = jnp.broadcast_to(
            squares, (rows, LANES)
        )
        tile[pl.ds(8 * h + 7, rows, stride=8 * pieces), :] = jnp.zeros((rows, LANES), F32)
    for k in range(out.shape[0]):
        out[k] = tile[pl.ds(8 * k, 8), :].astype(BF16)


def k_hidden(recv, scaled, out, mid_out):
    rows = scaled.shape[0]
    total = summed(recv, 0, 8)
    spread = as_column(total[6:7], rows, (0, 1)) / D
    shrink = lax.rsqrt(spread + EPSILON)
    mid_out[...] = rounded(scaled[...] * shrink)
    mine = iota((rows, 1), 0) == kv_index() // (out.shape[0] // rows)
    own = jnp.sum(jnp.where(mine, shrink, 0.0), axis=0, keepdims=True)
    total = total * own
    up = pltpu.roll(total, 5, 0)
    hidden = total / (1.0 + jnp.exp(-total)) * up
    hidden = jnp.where(iota((8, LANES), 0) < 3, hidden, 0.0).astype(BF16)
    for k in range(out.shape[0]):
        out[k] = hidden


def k_shrink(recv, w_down, out, tile):
    rows = out.shape[1]
    pieces = recv.shape[0] // rows
    for k in range(recv.shape[0]):
        tile[pl.ds(8 * k, 8), :] = recv[k].astype(F32)
    part = jnp.zeros((rows, LANES), F32)
    columns = w_down.shape[0]
    for t in range(3 * pieces):
        at = 8 * (t // 3) + t % 3
        size = min(LANES, columns - t * LANES)
        hidden = tile[pl.ds(at, rows, stride=8 * pieces), :][:, :size].astype(BF16)
        part = part + jnp.dot(
            hidden, w_down[pl.ds(t * LANES, size), :], preferred_element_type=F32
        )
    part = part.astype(BF16)
    for k in range(out.shape[0]):
        out[k] = part


def k_sums(recv, mid, out, mix_out):
    rows, width = mid.shape
    mixture = mid[...] + summed(recv, 0, rows)
    mix_out[...] = mixture
    centre = jnp.sum(mixture, axis=1, keepdims=True) / width
    square = jnp.sum((mixture - centre) ** 2, axis=1, keepdims=True)
    message = as_row([centre, square])
    for k in range(out.shape[0]):
        out[k] = message


def k_finish(recv, mix, gain, out, turned):
    rows, width = mix.shape
    devices = recv.shape[0]
    total = recv[0]
    for k in range(1, devices):
        total = total + recv[k]
    middle = total / devices
    spread = (recv[0] - middle) ** 2
    for k in range(1, devices):
        spread = spread + (recv[k] - middle) ** 2
    square = jnp.where(iota((1, LANES), 1) < rows, spread * width, total)
    centre = as_column(middle, rows, (0,))
    shrink = lax.rsqrt(as_column(square, rows, (0, 1)) / D + EPSILON)
    own = out.shape[0]
    scaled = ((mix[...] - centre) * shrink).T
    at = pl.multiple_of(lax.axis_index("tp") * own, own)
    turned[...] = scaled
    gain_col = jnp.sum(jnp.where(diagonal(own, 0)[:, :own], gain[...], 0.0), axis=1, keepdims=True)
    out[...] = (turned[pl.ds(at, own), :] * gain_col).astype(BF16)


def on_device(
    tokens,
    live_lengths,
    kv_cache,
    gate_sums,
    w_query,
    w_key,
    w_value,
    w_forget,
    forget_bias,
    w_out,
    first_gain,
    w_gate,
    w_up,
    w_down,
    second_gain,
):
    rows, own = tokens.shape
    kv, tp = lax.axis_size(KV), lax.axis_size("tp")
    width = own * tp
    block = ((rows, LANES), F32)
    message = jnp.broadcast_to(tokens.T[None], (tp, own, rows))
    in_hbm = functools.partial(pltpu.with_memory_space_constraint, memory_space=pltpu.HBM)
    recv = exchanged(message, "tp").reshape(width, rows)
    heads = w_query.shape[1]
    w_query, w_key, w_value, w_forget, w_out, tails = kernel(
        k_weights,
        [
            ((width, heads), BF16),
            ((DH, width), BF16),
            ((DH, width), BF16),
            ((w_forget.shape[1], width), BF16),
            ((heads, width), BF16),
            ((2, 8, LANES), F32),
        ],
        [ANY] * 5 + [VMEM] * 2,
        [pltpu.SemaphoreType.DMA((5,))],
    )(
        in_hbm(w_query),
        in_hbm(w_key.T),
        in_hbm(w_value.T),
        in_hbm(w_forget.T),
        in_hbm(w_out),
        first_gain[None],
        forget_bias[None],
    )
    message, x = kernel(
        k_project,
        [((kv, 2 * rows + 8, LANES), BF16), block],
        [VMEM] * 6,
        [pltpu.VMEM((rows, LANES), F32)],
    )(recv, w_query, w_key, w_value, w_forget, tails)
    recv = exchanged(message, KV)
    positions = kv_cache.shape[1]
    kv_cache, keys, gate_sums = kernel(
        k_prepare,
        [
            (kv_cache.shape, BF16),
            ((rows // 2, 2 * DH, positions), BF16),
            ((rows // 2, 8, positions), F32),
        ],
        [SMEM, ANY, ANY],
        [
            pltpu.VMEM(gate_sums.shape, F32),
            pltpu.SemaphoreType.DMA((rows,)),
            pltpu.SemaphoreType.DMA,
        ],
    )(live_lengths, in_hbm(kv_cache), in_hbm(gate_sums))
    message, tok, sums = kernel(
        k_attend,
        [((kv, 2 * rows + 8, LANES), BF16), block, ((2, LANES), F32)],
        [VMEM] * 4,
        [pltpu.VMEM((4 * rows, LANES), F32), pltpu.VMEM((4 * rows, LANES), F32)],
    )(recv, kv_cache, keys, gate_sums)
    (message,) = kernel(k_combine, [((tp, rows + 8, width), BF16)], [VMEM] * 4)(
        exchanged(message, KV), sums, w_out, tails
    )
    message, scaled = kernel(
        k_expand,
        [((kv, 8, LANES), BF16), block],
        [VMEM] * 5,
        [pltpu.VMEM((8 * kv, LANES), F32)],
    )(exchanged(message, "tp"), x, tok, w_gate.T, w_up.T)
    message, mid = kernel(k_hidden, [((kv, 8, LANES), BF16), block], [VMEM] * 2)(
        exchanged(message, KV), scaled
    )
    (message,) = kernel(
        k_shrink, [((tp, rows, width), BF16)], [VMEM] * 2, [pltpu.VMEM((8 * kv, LANES), F32)]
    )(exchanged(message, KV), w_down)
    message, mix = kernel(k_sums, [((kv, 1, LANES), F32), block], [VMEM] * 2)(
        exchanged(message, "tp"), mid
    )
    (out,) = kernel(
        k_finish, [((own, rows), BF16)], [VMEM] * 3, [pltpu.VMEM((width, rows), F32)], last=True
    )(exchanged(message, KV), mix, second_gain[None])
    return out.T


def solution(mesh):
    split = Mesh(mesh.devices.reshape(8, 4, mesh.shape["tp"]), ("kv_0", "kv_1", "tp"))
    placed = (
        P(None, KV_TP),
        P(),
        P(None, KV, "tp"),
        P(None, "tp", KV),
        P(KV, "tp"),
        P(KV, "tp"),
        P(KV, "tp"),
        P(),
        P(),
        P("tp", KV),
        P(KV_TP),
        P(KV, "tp"),
        P(KV, "tp"),
        P("tp", KV),
        P(KV_TP),
    )
    return jax.shard_map(
        on_device, mesh=split, in_specs=placed, out_specs=P(None, KV_TP), check_vma=False
    )
```

```python
import functools

import jax
import jax.numpy as jnp
from jax import lax
from jax.experimental import pallas as pl
from jax.experimental.pallas import tpu as pltpu
from jax.sharding import Mesh
from jax.sharding import PartitionSpec as P

D = 4096
DH = 64
LANES = 128
KV = ("kv_0", "kv_1")
KV_TP = ("kv_0", "kv_1", "tp")
EPSILON = 1e-05
EMPTY_SCORE = -1e30
F32 = jnp.float32
BF16 = jnp.bfloat16

VMEM = pl.BlockSpec(memory_space=pltpu.VMEM)
SMEM = pl.BlockSpec(memory_space=pltpu.SMEM)
ANY = pl.BlockSpec(memory_space=pl.ANY)


def kernel(body, outs, specs, scratch=(), last=False):
    return pl.pallas_call(
        body,
        out_shape=[
            jax.ShapeDtypeStruct(shape, dtype) if last else pltpu.VMEM(shape, dtype)
            for shape, dtype in outs
        ],
        in_specs=specs,
        out_specs=[VMEM] * len(outs),
        scratch_shapes=scratch,
        compiler_params=pltpu.CompilerParams(vmem_limit_bytes=8 * 2**20),
    )


def exchanged(pieces, axis):
    return lax.all_to_all(pieces, axis, 0, 0, tiled=True)


def kv_index():
    return lax.axis_index("kv_0") * lax.axis_size("kv_1") + lax.axis_index("kv_1")


def iota(shape, dim):
    return lax.broadcasted_iota(jnp.int32, shape, dim)


def rounded(x):
    return x.astype(BF16).astype(F32)


def in_pieces(value, count):
    pieces = []
    for _ in range(count):
        piece = rounded(value)
        pieces.append(piece)
        value = value - piece
    return pieces


def diagonal(rows, turn):
    return iota((rows, LANES), 1) == iota((rows, LANES), 0) + rows * turn


def across(left, right, sides):
    return lax.dot_general(left, right, (sides, ((), ())), preferred_element_type=F32)


LAST = ((1,), (1,))
FIRST = ((0,), (0,))


def as_row(columns):
    rows = columns[0].shape[0]
    tile = jnp.zeros((rows, LANES), F32)
    for turn, column in enumerate(columns):
        tile = jnp.where(diagonal(rows, turn), column, tile)
    return jnp.sum(tile, axis=0, keepdims=True)


def as_column(row, rows, turns):
    mask = diagonal(rows, turns[0])
    for turn in turns[1:]:
        mask = mask | diagonal(rows, turn)
    return jnp.sum(jnp.where(mask, row, 0.0), axis=1, keepdims=True)


def summed(ref, start, size):
    total = ref[0, pl.ds(start, size)].astype(F32)
    for k in range(1, ref.shape[0]):
        total = total + ref[k, pl.ds(start, size)].astype(F32)
    return total


def k_weights(
    query,
    key,
    value,
    forget,
    w_out,
    gain_hbm,
    bias_hbm,
    query_o,
    key_o,
    value_o,
    forget_o,
    w_out_o,
    tail_o,
    gain,
    bias,
    sem,
):
    width = forget_o.shape[1]
    start = pl.multiple_of(kv_index() * width, width)
    pairs = [(w_out, w_out_o), (query, query_o), (key, key_o), (value, value_o)]
    pairs.append((forget.at[:, pl.ds(start, width)], forget_o))
    pairs.extend([(gain_hbm, gain), (bias_hbm, bias)])
    copies = [pltpu.make_async_copy(a, b, sem.at[k]) for k, (a, b) in enumerate(pairs)]
    for copy in copies:
        copy.start()
    row = iota((8, LANES), 0)
    for copy in copies:
        copy.wait()
    own = gain.shape[1]
    place = iota((own, LANES), 0) + lax.axis_index("tp") * own
    spread = jnp.where(iota((own, LANES), 1) == place, 1.0, 0.0)
    column = jnp.sum(jnp.where(diagonal(own, 0)[:, :own], gain[...], 0.0), axis=1, keepdims=True)
    gains = in_pieces(jnp.sum(spread * column, axis=0, keepdims=True), 3)
    sums = across(jnp.ones((8, LANES), BF16), w_out_o[...], LAST)
    sums_hi, sums_lo = in_pieces(sums, 2)
    tail = jnp.where(row == 2, sums_hi[:, :LANES], 0.0)
    tail = jnp.where(row == 3, sums_hi[:, LANES:], tail)
    tail = jnp.where(row == 4, sums_lo[:, :LANES], tail)
    tail_o[0] = jnp.where(row == 5, sums_lo[:, LANES:], tail)
    mine = iota(bias.shape, 1) == lax.axis_index("tp")
    once = jnp.where(kv_index() == 0, 1.0, 0.0)
    own_bias = jnp.sum(jnp.where(mine, bias[...], 0.0), axis=1, keepdims=True) * once
    tail = jnp.where(row == 0, own_bias, 0.0)
    for k, piece in enumerate(gains):
        tail = jnp.where(row == 1 + k, piece, tail)
    tail_o[1] = tail


def k_project(recv, w_query, w_key, w_value, wf, tails, out, x_out, new_rows):
    width = wf.shape[1]
    same = jnp.where(iota((width, width), 0) == iota((width, width), 1), 1.0, 0.0).astype(BF16)
    x = across(recv[...], same, FIRST)
    x_out[...] = x
    rows = x.shape[0]
    xb = x.astype(BF16)
    query = jnp.dot(xb, w_query[...], preferred_element_type=F32)
    new_rows[:, :DH] = across(xb, w_key[...], LAST)
    new_rows[:, DH:] = across(xb, w_value[...], LAST)
    forget = across(xb, wf[...], LAST)
    token_col = jnp.sum(x, axis=1, keepdims=True)
    mine = iota(forget.shape, 1) == lax.axis_index("tp")
    forget_col = jnp.sum(jnp.where(mine, forget, 0.0), axis=1, keepdims=True)
    forget_col = forget_col + tails[1, 0:1, 0:1]
    small = as_row([*in_pieces(forget_col, 2), *in_pieces(token_col, 2)])
    row = iota((8, LANES), 0)
    tail = jnp.where(row == 1, small, tails[0])
    left = query[:, :LANES].astype(BF16)
    right = query[:, LANES:].astype(BF16)
    for b in range(rows):
        own_tail = jnp.where(row == 0, new_rows[pl.ds(b, 1), :], tail).astype(BF16)
        for k in range(b, out.shape[0], rows):
            out[k, pl.ds(0, rows)] = left
            out[k, pl.ds(rows, rows)] = right
            out[k, pl.ds(2 * rows, 8)] = own_tail


def k_prepare(lengths, cache, gate, keys_o, values_o, cache_v, gate_v, sem, gate_sem):
    rows, positions = cache.shape[:2]
    copies = [pltpu.make_async_copy(cache.at[b], cache_v.at[b], sem.at[b]) for b in range(rows)]
    gates = pltpu.make_async_copy(gate, gate_v, gate_sem)
    gates.start()
    for copy in copies:
        copy.start()
    gates.wait()
    place = kv_index() * positions + iota((8, positions), 1)
    row = iota((16, positions), 0)
    for m in range(rows // 2):
        extra = jnp.zeros((16, positions), F32)
        for k in range(2):
            b = 2 * m + k
            masked = jnp.where(place < lengths[b], gate_v[b], EMPTY_SCORE)
            for n, piece in enumerate(in_pieces(masked, 3)):
                extra = jnp.where(row == 3 * k + n, piece[0:1], extra)
        keys_o[m, pl.ds(2 * DH, 16), :] = extra.astype(BF16)
    for b in range(rows):
        copies[b].wait()
        keys_o[b // 2, pl.ds(DH * (b % 2), DH), :] = cache_v[b].T[:DH]
        if b % 2:
            values_o[b // 2] = jnp.concatenate(
                [cache_v[b - 1][:, DH:], cache_v[b][:, DH:]], axis=1
            )


def k_attend(recv, keys, values, out, tok_out, sums_out, qs, os):
    rows = 2 * keys.shape[0]
    heads = 4
    scale = DH**-0.5
    left = rounded(summed(recv, 0, rows))
    right = rounded(summed(recv, rows, rows))
    tail = summed(recv, 2 * rows, 8)
    new_row = rounded(tail[0:1])
    small = tail[1:2]
    sums_out[0:1, :] = tail[2:3] + tail[4:5]
    sums_out[1:2, :] = tail[3:4] + tail[5:6]
    tok_out[...] = jnp.broadcast_to(as_column(small, rows, (2, 3)), tok_out.shape)
    even = iota((rows, LANES), 0) % 2 == 0
    low = iota((rows, LANES), 1) < DH
    keep = even == low
    left_turned = pltpu.roll(left, DH, 1)
    right_turned = pltpu.roll(right, DH, 1)
    placed = (
        jnp.where(even, left, left_turned),
        jnp.where(even, left_turned, left),
        jnp.where(even, right, right_turned),
        jnp.where(even, right_turned, right),
    )
    for h, block in enumerate(placed):
        qs[pl.ds(h, rows, stride=heads), :] = jnp.where(keep, block, 0.0)
    all_rows = rows * heads
    owner = iota((all_rows, LANES), 0) // heads
    lane = iota((all_rows, LANES), 1)
    fetched = jnp.where((lane == owner) | (lane == owner + rows), small, 0.0)
    fetched = jnp.sum(fetched, axis=1, keepdims=True)
    new_gate = jnp.minimum(fetched, 0.0) - jnp.log(1.0 + jnp.exp(-jnp.abs(fetched)))
    lane = iota((1, LANES), 1)
    new_turned = pltpu.roll(jnp.broadcast_to(new_row, (8, LANES)), DH, 1)[0:1]
    new_key = jnp.where(lane < DH, new_row, new_turned)
    new_value = jnp.where(lane < DH, new_turned, new_row)
    own = jnp.sum(qs[...] * new_key, axis=1, keepdims=True) * scale
    mine = iota((all_rows, 1), 0) // heads == kv_index()
    own = jnp.where(mine, own, EMPTY_SCORE)
    lane = iota((8, LANES), 1)
    spot = jnp.where(iota((8, LANES), 0) < heads, DH, 0)
    extra = iota((8, 16), 1) - 3 * (iota((8, 16), 0) // heads)
    extra = jnp.where((extra >= 0) & (extra < 3), 1.0, 0.0)
    for m in range(rows // 2):
        at = slice(8 * m, 8 * m + 8)
        query = jnp.concatenate([qs[pl.ds(8 * m, 8), :] * scale, extra], axis=1)
        scores = jnp.dot(query.astype(BF16), keys[m], preferred_element_type=F32)
        scores = scores + new_gate[at]
        top = jnp.maximum(jnp.max(scores, axis=1, keepdims=True), own[at])
        top = jnp.maximum(top, 0.1 * EMPTY_SCORE)
        weights = jnp.exp(scores - top)
        own_weight = jnp.exp(own[at] - top)
        total = jnp.sum(weights, axis=1, keepdims=True) + own_weight
        value = jnp.dot(weights.astype(BF16), values[m], preferred_element_type=F32)
        value = value + rounded(own_weight) * new_value
        spare = jnp.where(lane == spot, top, jnp.where(lane == spot + 1, total, value))
        os[pl.ds(8 * m, 8), :] = spare
    blocks = [os[pl.ds(h, rows, stride=heads), :] for h in range(heads)]
    turned = [pltpu.roll(block, DH, 1) for block in blocks]
    firsts = [jnp.where(even, block, turn) for block, turn in zip(blocks, turned)]
    seconds = [jnp.where(even, turn, block) for block, turn in zip(blocks, turned)]
    low_out = jnp.where(low, firsts[0], seconds[1]).astype(BF16)
    high_out = jnp.where(low, firsts[2], seconds[3]).astype(BF16)
    lane = iota((rows, LANES), 1)
    stats = jnp.zeros((rows, LANES), F32)
    for h in range(heads):
        pieces = [*in_pieces(seconds[h][:, 0:1], 3), *in_pieces(seconds[h][:, 1:2], 2)]
        for k, piece in enumerate(pieces):
            stats = jnp.where(lane == 8 * h + k, piece, stats)
    stats = (stats[:8] + pltpu.roll(stats[8:], 32, 1)).astype(BF16)
    for k in range(out.shape[0]):
        out[k, pl.ds(0, rows)] = low_out
        out[k, pl.ds(rows, rows)] = high_out
        out[k, pl.ds(2 * rows, 8)] = stats


def k_combine(recv, sums, w_out, tails, out):
    devices = recv.shape[0]
    rows = (recv.shape[1] - 8) // 2
    heads = 4 * DH
    source = iota((LANES, 4 * heads), 0)
    column = iota((LANES, 4 * heads), 1)
    half = (column // heads) % 2
    first = 32 * half + 8 * ((column % heads) // DH)
    is_top = column < 2 * heads
    begin = jnp.where(is_top, first, first + 3)
    end = jnp.where(is_top, first + 3, first + 5)
    spread = jnp.where((source >= begin) & (source < end), 1.0, 0.0).astype(BF16)
    stats = recv[:, pl.ds(2 * rows, 8), :].reshape(devices * 8, LANES)
    wide = jnp.dot(stats, spread, preferred_element_type=F32).reshape(devices, 8, 4 * heads)
    blocks = []
    for half in range(2):
        tops = wide[:, :, half * heads : (half + 1) * heads]
        totals = wide[:, :, (2 + half) * heads : (3 + half) * heads]
        scales = jnp.exp(tops - jnp.max(tops, axis=0, keepdims=True))
        total = jnp.sum(totals * scales, axis=0)
        low = recv[:, pl.ds(8 * half, 8), :].astype(F32)
        high = recv[:, pl.ds(rows + 8 * half, 8), :].astype(F32)
        low = jnp.sum(low * scales[:, :, :LANES], axis=0)
        high = jnp.sum(high * scales[:, :, LANES:], axis=0)
        blocks.append(jnp.concatenate([low, high], axis=1) / total)
    attended = jnp.concatenate(blocks, axis=0).astype(BF16)
    attn_part = jnp.dot(attended, w_out[...], preferred_element_type=F32).astype(BF16)
    wide = attended.astype(F32)
    mean = wide[:, :LANES] * sums[0:1, :] + wide[:, LANES:] * sums[1:2, :]
    mean_row = as_row(in_pieces(jnp.sum(mean, axis=1, keepdims=True), 2))
    row = iota((8, LANES), 0)
    tail = jnp.where(row == 0, mean_row, tails[1])
    tail = tail.astype(BF16)
    for k in range(out.shape[0]):
        out[k, pl.ds(0, rows)] = attn_part
        out[k, pl.ds(rows, 8)] = tail


def k_expand(recv, x, tok, w_gate, w_up, out, scaled_out, tile):
    rows = x.shape[0]
    added = summed(recv, 0, rows)
    tail = summed(recv, rows, 8)
    mean = as_column(tail[0:1], rows, (0, 1))
    gain = tail[1:2] + tail[2:3] + tail[3:4]
    centre = (tok[:, 0:1] + mean) / D
    centred = x[...] + added - centre
    scaled = centred * gain
    scaled_out[...] = scaled
    squares = as_row(in_pieces(jnp.sum(centred * centred, axis=1, keepdims=True), 2))
    scaled = scaled.astype(BF16)
    pieces = tile.shape[0] // (8 * rows)
    tiles = 3 * pieces
    columns = w_gate.shape[0]
    for k, weight in enumerate((w_gate, w_up)):
        part = across(scaled, weight[...], LAST)
        pad = jnp.zeros((rows, tiles * LANES - columns), F32)
        part = jnp.concatenate([part, pad], axis=1)
        for t in range(tiles):
            at = 8 * (t // 3) + 3 * k + t % 3
            tile[pl.ds(at, rows, stride=8 * pieces), :] = part[:, t * LANES : (t + 1) * LANES]
    for h in range(pieces):
        tile[pl.ds(8 * h + 6, rows, stride=8 * pieces), :] = jnp.broadcast_to(
            squares, (rows, LANES)
        )
        tile[pl.ds(8 * h + 7, rows, stride=8 * pieces), :] = jnp.zeros((rows, LANES), F32)
    for k in range(out.shape[0]):
        out[k] = tile[pl.ds(8 * k, 8), :].astype(BF16)


def k_hidden(recv, scaled, out, mid_out):
    rows = scaled.shape[0]
    total = summed(recv, 0, 8)
    spread = as_column(total[6:7], rows, (0, 1)) / D
    shrink = lax.rsqrt(spread + EPSILON)
    mid_out[...] = rounded(scaled[...] * shrink)
    mine = iota((rows, 1), 0) == kv_index() // (out.shape[0] // rows)
    own = jnp.sum(jnp.where(mine, shrink, 0.0), axis=0, keepdims=True)
    total = total * own
    up = pltpu.roll(total, 5, 0)
    hidden = total / (1.0 + jnp.exp(-total)) * up
    hidden = jnp.where(iota((8, LANES), 0) < 3, hidden, 0.0).astype(BF16)
    for k in range(out.shape[0]):
        out[k] = hidden


def k_shrink(recv, w_down, out, tile):
    rows = out.shape[1]
    pieces = recv.shape[0] // rows
    for k in range(recv.shape[0]):
        tile[pl.ds(8 * k, 8), :] = recv[k].astype(F32)
    part = jnp.zeros((rows, LANES), F32)
    columns = w_down.shape[0]
    for t in range(3 * pieces):
        at = 8 * (t // 3) + t % 3
        size = min(LANES, columns - t * LANES)
        hidden = tile[pl.ds(at, rows, stride=8 * pieces), :][:, :size].astype(BF16)
        part = part + jnp.dot(
            hidden, w_down[pl.ds(t * LANES, size), :], preferred_element_type=F32
        )
    part = part.astype(BF16)
    for k in range(out.shape[0]):
        out[k] = part


def k_sums(recv, mid, out, mix_out):
    rows, width = mid.shape
    mixture = mid[...] + summed(recv, 0, rows)
    mix_out[...] = mixture
    centre = jnp.sum(mixture, axis=1, keepdims=True) / width
    square = jnp.sum((mixture - centre) ** 2, axis=1, keepdims=True)
    message = as_row([centre, square])
    for k in range(out.shape[0]):
        out[k] = message


def k_finish(recv, mix, gain, out, turned):
    rows, width = mix.shape
    devices = recv.shape[0]
    total = recv[0]
    for k in range(1, devices):
        total = total + recv[k]
    middle = total / devices
    spread = (recv[0] - middle) ** 2
    for k in range(1, devices):
        spread = spread + (recv[k] - middle) ** 2
    square = jnp.where(iota((1, LANES), 1) < rows, spread * width, total)
    centre = as_column(middle, rows, (0,))
    shrink = lax.rsqrt(as_column(square, rows, (0, 1)) / D + EPSILON)
    own = out.shape[0]
    scaled = ((mix[...] - centre) * shrink).T
    at = pl.multiple_of(lax.axis_index("tp") * own, own)
    turned[...] = scaled
    gain_col = jnp.sum(jnp.where(diagonal(own, 0)[:, :own], gain[...], 0.0), axis=1, keepdims=True)
    out[...] = (turned[pl.ds(at, own), :] * gain_col).astype(BF16)


def on_device(
    tokens,
    live_lengths,
    kv_cache,
    gate_sums,
    w_query,
    w_key,
    w_value,
    w_forget,
    forget_bias,
    w_out,
    first_gain,
    w_gate,
    w_up,
    w_down,
    second_gain,
):
    rows, own = tokens.shape
    kv, tp = lax.axis_size(KV), lax.axis_size("tp")
    width = own * tp
    block = ((rows, LANES), F32)
    message = jnp.broadcast_to(tokens.T[None], (tp, own, rows))
    in_hbm = functools.partial(pltpu.with_memory_space_constraint, memory_space=pltpu.HBM)
    recv = exchanged(message, "tp").reshape(width, rows)
    heads = w_query.shape[1]
    w_query, w_key, w_value, w_forget, w_out, tails = kernel(
        k_weights,
        [
            ((width, heads), BF16),
            ((DH, width), BF16),
            ((DH, width), BF16),
            ((w_forget.shape[1], width), BF16),
            ((heads, width), BF16),
            ((2, 8, LANES), F32),
        ],
        [ANY] * 7,
        [
            pltpu.VMEM((1, own), F32),
            pltpu.VMEM((1, w_forget.shape[1]), F32),
            pltpu.SemaphoreType.DMA((7,)),
        ],
    )(
        in_hbm(w_query),
        in_hbm(w_key.T),
        in_hbm(w_value.T),
        in_hbm(w_forget.T),
        in_hbm(w_out),
        in_hbm(first_gain[None]),
        in_hbm(forget_bias[None]),
    )
    message, x = kernel(
        k_project,
        [((kv, 2 * rows + 8, LANES), BF16), block],
        [VMEM] * 6,
        [pltpu.VMEM((rows, LANES), F32)],
    )(recv, w_query, w_key, w_value, w_forget, tails)
    recv = exchanged(message, KV)
    positions = kv_cache.shape[1]
    keys, values = kernel(
        k_prepare,
        [
            ((rows // 2, 2 * DH + 16, positions), BF16),
            ((rows // 2, positions, 2 * DH), BF16),
        ],
        [SMEM, ANY, ANY],
        [
            pltpu.VMEM(kv_cache.shape, BF16),
            pltpu.VMEM(gate_sums.shape, F32),
            pltpu.SemaphoreType.DMA((rows,)),
            pltpu.SemaphoreType.DMA,
        ],
    )(live_lengths, in_hbm(kv_cache), in_hbm(gate_sums))
    message, tok, sums = kernel(
        k_attend,
        [((kv, 2 * rows + 8, LANES), BF16), block, ((2, LANES), F32)],
        [VMEM] * 3,
        [pltpu.VMEM((4 * rows, LANES), F32), pltpu.VMEM((4 * rows, LANES), F32)],
    )(recv, keys, values)
    (message,) = kernel(k_combine, [((tp, rows + 8, width), BF16)], [VMEM] * 4)(
        exchanged(message, KV), sums, w_out, tails
    )
    message, scaled = kernel(
        k_expand,
        [((kv, 8, LANES), BF16), block],
        [VMEM] * 5,
        [pltpu.VMEM((8 * kv, LANES), F32)],
    )(exchanged(message, "tp"), x, tok, w_gate.T, w_up.T)
    message, mid = kernel(k_hidden, [((kv, 8, LANES), BF16), block], [VMEM] * 2)(
        exchanged(message, KV), scaled
    )
    (message,) = kernel(
        k_shrink, [((tp, rows, width), BF16)], [VMEM] * 2, [pltpu.VMEM((8 * kv, LANES), F32)]
    )(exchanged(message, KV), w_down)
    message, mix = kernel(k_sums, [((kv, 1, LANES), F32), block], [VMEM] * 2)(
        exchanged(message, "tp"), mid
    )
    (out,) = kernel(
        k_finish, [((own, rows), BF16)], [VMEM] * 3, [pltpu.VMEM((width, rows), F32)], last=True
    )(exchanged(message, KV), mix, second_gain[None])
    return out.T


def solution(mesh):
    split = Mesh(mesh.devices.reshape(8, 4, mesh.shape["tp"]), ("kv_0", "kv_1", "tp"))
    placed = (
        P(None, KV_TP),
        P(),
        P(None, KV, "tp"),
        P(None, "tp", KV),
        P(KV, "tp"),
        P(KV, "tp"),
        P(KV, "tp"),
        P(),
        P(),
        P("tp", KV),
        P(KV_TP),
        P(KV, "tp"),
        P(KV, "tp"),
        P("tp", KV),
        P(KV_TP),
    )
    return jax.shard_map(
        on_device, mesh=split, in_specs=placed, out_specs=P(None, KV_TP), check_vma=False
    )
```

```python
import functools

import jax
import jax.numpy as jnp
from jax import lax
from jax.experimental import pallas as pl
from jax.experimental.pallas import tpu as pltpu
from jax.sharding import Mesh
from jax.sharding import PartitionSpec as P

D = 4096
DH = 64
LANES = 128
KV = ("kv_0", "kv_1")
KV_TP = ("kv_0", "kv_1", "tp")
EPSILON = 1e-05
EMPTY_SCORE = -1e30
F32 = jnp.float32
BF16 = jnp.bfloat16

VMEM = pl.BlockSpec(memory_space=pltpu.VMEM)
SMEM = pl.BlockSpec(memory_space=pltpu.SMEM)
ANY = pl.BlockSpec(memory_space=pl.ANY)


def kernel(body, outs, specs, scratch=(), last=False):
    return pl.pallas_call(
        body,
        out_shape=[
            jax.ShapeDtypeStruct(shape, dtype) if last else pltpu.VMEM(shape, dtype)
            for shape, dtype in outs
        ],
        in_specs=specs,
        out_specs=[VMEM] * len(outs),
        scratch_shapes=scratch,
        compiler_params=pltpu.CompilerParams(vmem_limit_bytes=8 * 2**20),
    )


def exchanged(pieces, axis):
    return lax.all_to_all(pieces, axis, 0, 0, tiled=True)


def kv_index():
    return lax.axis_index("kv_0") * lax.axis_size("kv_1") + lax.axis_index("kv_1")


def iota(shape, dim):
    return lax.broadcasted_iota(jnp.int32, shape, dim)


def rounded(x):
    return x.astype(BF16).astype(F32)


def in_pieces(value, count):
    pieces = []
    for _ in range(count):
        piece = rounded(value)
        pieces.append(piece)
        value = value - piece
    return pieces


def diagonal(rows, turn):
    return iota((rows, LANES), 1) == iota((rows, LANES), 0) + rows * turn


def across(left, right, sides):
    return lax.dot_general(left, right, (sides, ((), ())), preferred_element_type=F32)


LAST = ((1,), (1,))
FIRST = ((0,), (0,))


def as_row(columns):
    rows = columns[0].shape[0]
    tile = jnp.zeros((rows, LANES), F32)
    for turn, column in enumerate(columns):
        tile = jnp.where(diagonal(rows, turn), column, tile)
    return jnp.sum(tile, axis=0, keepdims=True)


def as_column(row, rows, turns):
    mask = diagonal(rows, turns[0])
    for turn in turns[1:]:
        mask = mask | diagonal(rows, turn)
    return jnp.sum(jnp.where(mask, row, 0.0), axis=1, keepdims=True)


def summed(ref, start, size):
    total = ref[0, pl.ds(start, size)].astype(F32)
    for k in range(1, ref.shape[0]):
        total = total + ref[k, pl.ds(start, size)].astype(F32)
    return total


def tiles_of(block):
    return [block[4 * t : 4 * t + 4] for t in range(block.shape[0] // 4)]


def put(out, k, tiles):
    for t, tile in enumerate(tiles):
        out[k, t] = tile


def tiles_summed(ref, start, count):
    tiles = []
    for t in range(start, start + count):
        total = ref[0, t].astype(F32)
        for k in range(1, ref.shape[0]):
            total = total + ref[k, t].astype(F32)
        tiles.append(total)
    return tiles[0] if count == 1 else jnp.concatenate(tiles, axis=0)


def k_weights(
    query,
    key,
    value,
    forget,
    w_out,
    gain_hbm,
    bias_hbm,
    query_o,
    key_o,
    value_o,
    forget_o,
    w_out_o,
    tail_o,
    gain,
    bias,
    sem,
):
    width = forget_o.shape[1]
    start = pl.multiple_of(kv_index() * width, width)
    pairs = [(w_out, w_out_o), (query, query_o), (key, key_o), (value, value_o)]
    pairs.append((forget.at[:, pl.ds(start, width)], forget_o))
    pairs.extend([(gain_hbm, gain), (bias_hbm, bias)])
    copies = [pltpu.make_async_copy(a, b, sem.at[k]) for k, (a, b) in enumerate(pairs)]
    for copy in copies:
        copy.start()
    row = iota((8, LANES), 0)
    for copy in copies:
        copy.wait()
    own = gain.shape[1]
    place = iota((own, LANES), 0) + lax.axis_index("tp") * own
    spread = jnp.where(iota((own, LANES), 1) == place, 1.0, 0.0)
    column = jnp.sum(jnp.where(diagonal(own, 0)[:, :own], gain[...], 0.0), axis=1, keepdims=True)
    gains = in_pieces(jnp.sum(spread * column, axis=0, keepdims=True), 3)
    sums = across(jnp.ones((8, LANES), BF16), w_out_o[...], LAST)
    tail = jnp.where(row == 2, sums[:, :LANES], 0.0)
    tail_o[0] = jnp.where(row == 3, sums[:, LANES:], tail)
    mine = iota(bias.shape, 1) == lax.axis_index("tp")
    once = jnp.where(kv_index() == 0, 1.0, 0.0)
    own_bias = jnp.sum(jnp.where(mine, bias[...], 0.0), axis=1, keepdims=True) * once
    tail = jnp.where(row == 0, own_bias, 0.0)
    for k, piece in enumerate(gains):
        tail = jnp.where(row == 1 + k, piece, tail)
    tail_o[1] = tail


def k_project(recv, w_query, w_key, w_value, wf, tails, out, x_out, new_rows):
    width = wf.shape[1]
    same = jnp.where(iota((width, width), 0) == iota((width, width), 1), 1.0, 0.0).astype(BF16)
    x = across(recv[...], same, FIRST)
    x_out[...] = x
    rows = x.shape[0]
    xb = x.astype(BF16)
    query = jnp.dot(xb, w_query[...], preferred_element_type=F32)
    new_rows[:, :DH] = across(xb, w_key[...], LAST)
    new_rows[:, DH:] = across(xb, w_value[...], LAST)
    forget = across(xb, wf[...], LAST)
    token_col = jnp.sum(x, axis=1, keepdims=True)
    mine = iota(forget.shape, 1) == lax.axis_index("tp")
    forget_col = jnp.sum(jnp.where(mine, forget, 0.0), axis=1, keepdims=True)
    forget_col = forget_col + tails[1, 0:1, 0:1]
    small = as_row([*in_pieces(forget_col, 2), *in_pieces(token_col, 2)])
    row = iota((8, LANES), 0)
    tail = jnp.where(row == 1, small, tails[0])
    tiles = tiles_of(query[:, :LANES].astype(BF16)) + tiles_of(query[:, LANES:].astype(BF16))
    for b in range(rows):
        own_tail = jnp.where(row == 0, new_rows[pl.ds(b, 1), :], tail)[:4].astype(BF16)
        for k in range(b, out.shape[0], rows):
            put(out, k, [*tiles, own_tail])


def k_prepare(lengths, cache, gate, keys_o, values_o, gate_o, cache_v, gate_v, sem, gate_sem):
    rows, positions = cache.shape[:2]
    copies = [pltpu.make_async_copy(cache.at[b], cache_v.at[b], sem.at[b]) for b in range(rows)]
    gates = pltpu.make_async_copy(gate, gate_v, gate_sem)
    gates.start()
    for copy in copies:
        copy.start()
    gates.wait()
    place = kv_index() * positions + iota((8, positions), 1)
    first = iota((8, positions), 0) < 4
    for m in range(rows // 2):
        one = jnp.where(place < lengths[2 * m], gate_v[2 * m], EMPTY_SCORE)
        two = jnp.where(place < lengths[2 * m + 1], gate_v[2 * m + 1], EMPTY_SCORE)
        gate_o[m] = jnp.where(first, one, two)
    for b in range(rows):
        copies[b].wait()
        keys_o[b // 2, pl.ds(DH * (b % 2), DH), :] = cache_v[b].T[:DH]
        if b % 2:
            values_o[b // 2] = jnp.concatenate(
                [cache_v[b - 1][:, DH:], cache_v[b][:, DH:]], axis=1
            )


def k_attend(recv, keys, values, gate, out, tok_out, sums_out, qs, os):
    rows = 2 * keys.shape[0]
    heads = 4
    scale = DH**-0.5
    left = rounded(tiles_summed(recv, 0, rows // 4))
    right = rounded(tiles_summed(recv, rows // 4, rows // 4))
    tail = tiles_summed(recv, rows // 2, 1)
    new_row = rounded(tail[0:1])
    small = tail[1:2]
    sums_out[...] = tail[2:4]
    tok_out[...] = jnp.broadcast_to(as_column(small, rows, (2, 3)), tok_out.shape)
    even = iota((rows, LANES), 0) % 2 == 0
    low = iota((rows, LANES), 1) < DH
    keep = even == low
    left_turned = pltpu.roll(left, DH, 1)
    right_turned = pltpu.roll(right, DH, 1)
    placed = (
        jnp.where(even, left, left_turned),
        jnp.where(even, left_turned, left),
        jnp.where(even, right, right_turned),
        jnp.where(even, right_turned, right),
    )
    for h, block in enumerate(placed):
        qs[pl.ds(h, rows, stride=heads), :] = jnp.where(keep, block, 0.0)
    all_rows = rows * heads
    owner = iota((all_rows, LANES), 0) // heads
    lane = iota((all_rows, LANES), 1)
    fetched = jnp.where((lane == owner) | (lane == owner + rows), small, 0.0)
    fetched = jnp.sum(fetched, axis=1, keepdims=True)
    new_gate = jnp.minimum(fetched, 0.0) - jnp.log(1.0 + jnp.exp(-jnp.abs(fetched)))
    lane = iota((1, LANES), 1)
    new_turned = pltpu.roll(jnp.broadcast_to(new_row, (8, LANES)), DH, 1)[0:1]
    new_key = jnp.where(lane < DH, new_row, new_turned)
    new_value = jnp.where(lane < DH, new_turned, new_row)
    own = jnp.sum(qs[...] * new_key, axis=1, keepdims=True) * scale
    mine = iota((all_rows, 1), 0) // heads == kv_index()
    own = jnp.where(mine, own, EMPTY_SCORE)
    lane = iota((8, LANES), 1)
    spot = jnp.where(iota((8, LANES), 0) < heads, DH, 0)
    for m in range(rows // 2):
        at = slice(8 * m, 8 * m + 8)
        query = (qs[pl.ds(8 * m, 8), :] * scale).astype(BF16)
        scores = jnp.dot(query, keys[m], preferred_element_type=F32)
        scores = scores + (gate[m] + new_gate[at])
        top = jnp.maximum(jnp.max(scores, axis=1, keepdims=True), own[at])
        top = jnp.maximum(top, 0.1 * EMPTY_SCORE)
        weights = jnp.exp(scores - top)
        own_weight = jnp.exp(own[at] - top)
        total = jnp.sum(weights, axis=1, keepdims=True) + own_weight
        value = jnp.dot(weights.astype(BF16), values[m], preferred_element_type=F32)
        value = value + rounded(own_weight) * new_value
        spare = jnp.where(lane == spot, top, jnp.where(lane == spot + 1, total, value))
        os[pl.ds(8 * m, 8), :] = spare
    blocks = [os[pl.ds(h, rows, stride=heads), :] for h in range(heads)]
    turned = [pltpu.roll(block, DH, 1) for block in blocks]
    firsts = [jnp.where(even, block, turn) for block, turn in zip(blocks, turned)]
    seconds = [jnp.where(even, turn, block) for block, turn in zip(blocks, turned)]
    low_out = jnp.where(low, firsts[0], seconds[1]).astype(BF16)
    high_out = jnp.where(low, firsts[2], seconds[3]).astype(BF16)
    lane = iota((rows, LANES), 1)
    stats = jnp.zeros((rows, LANES), F32)
    for h in range(heads):
        pieces = [*in_pieces(seconds[h][:, 0:1], 3), *in_pieces(seconds[h][:, 1:2], 2)]
        for k, piece in enumerate(pieces):
            stats = jnp.where(lane == 8 * h + k, piece, stats)
    packed = stats[:4]
    for g in range(1, rows // 4):
        packed = packed + pltpu.roll(stats, 32 * g, 1)[4 * g : 4 * g + 4]
    tiles = [*tiles_of(low_out), *tiles_of(high_out), packed.astype(BF16)]
    for k in range(out.shape[0]):
        put(out, k, tiles)


def k_combine(recv, sums, w_out, tails, out):
    devices = recv.shape[0]
    tiles = (recv.shape[1] - 1) // 2
    rows = 4 * tiles
    heads = 4 * DH
    source = iota((LANES, 2 * heads), 0) % 32
    column = iota((LANES, 2 * heads), 1)
    first = 8 * ((column % heads) // DH)
    is_top = column < heads
    begin = jnp.where(is_top, first, first + 3)
    end = jnp.where(is_top, first + 3, first + 5)
    spread = jnp.where((source >= begin) & (source < end), 1.0, 0.0).astype(BF16)
    stats = recv[:, 2 * tiles].astype(F32)
    stats = jnp.concatenate([stats, stats], axis=1)
    group = iota(stats.shape, 2) // 32 - iota(stats.shape, 1) // 4
    blocks = []
    for half in range(2):
        mine = jnp.where(group == 2 * half, stats, 0.0).astype(BF16).reshape(devices * 8, LANES)
        wide = jnp.dot(mine, spread, preferred_element_type=F32).reshape(devices, 8, 2 * heads)
        tops = wide[:, :, :heads]
        totals = wide[:, :, heads:]
        scales = jnp.exp(tops - jnp.max(tops, axis=0, keepdims=True))
        total = jnp.sum(totals * scales, axis=0)
        sides = []
        for side in range(2):
            at = tiles * side + 2 * half
            part = [recv[:, at + t].astype(F32) for t in range(2)]
            part = jnp.concatenate(part, axis=1)
            sides.append(jnp.sum(part * scales[:, :, side * LANES : (side + 1) * LANES], axis=0))
        blocks.append(jnp.concatenate(sides, axis=1) / total)
    attended = jnp.concatenate(blocks, axis=0).astype(BF16)
    attn_part = jnp.dot(attended, w_out[...], preferred_element_type=F32).astype(BF16)
    wide = attended.astype(F32)
    mean = wide[:, :LANES] * sums[0:1, :] + wide[:, LANES:] * sums[1:2, :]
    mean_row = as_row(in_pieces(jnp.sum(mean, axis=1, keepdims=True), 2))
    row = iota((8, LANES), 0)
    tail = jnp.where(row == 0, mean_row, tails[1])
    pieces = [*tiles_of(attn_part), tail[:4].astype(BF16)]
    for k in range(out.shape[0]):
        put(out, k, pieces)


def k_expand(recv, x, tok, w_gate, w_up, out, scaled_out, tile):
    rows = x.shape[0]
    added = tiles_summed(recv, 0, rows // 4)
    tail = tiles_summed(recv, rows // 4, 1)
    mean = as_column(tail[0:1], rows, (0, 1))
    gain = tail[1:2] + tail[2:3] + tail[3:4]
    centre = (tok[:, 0:1] + mean) / D
    centred = x[...] + added - centre
    scaled = centred * gain
    scaled_out[...] = scaled
    squares = as_row(in_pieces(jnp.sum(centred * centred, axis=1, keepdims=True), 2))
    scaled = scaled.astype(BF16)
    pieces = tile.shape[0] // (8 * rows)
    tiles = 3 * pieces
    columns = w_gate.shape[0]
    for k, weight in enumerate((w_gate, w_up)):
        part = across(scaled, weight[...], LAST)
        pad = jnp.zeros((rows, tiles * LANES - columns), F32)
        part = jnp.concatenate([part, pad], axis=1)
        for t in range(tiles):
            at = 8 * (t // 3) + 3 * k + t % 3
            tile[pl.ds(at, rows, stride=8 * pieces), :] = part[:, t * LANES : (t + 1) * LANES]
    for h in range(pieces):
        tile[pl.ds(8 * h + 6, rows, stride=8 * pieces), :] = jnp.broadcast_to(
            squares, (rows, LANES)
        )
        tile[pl.ds(8 * h + 7, rows, stride=8 * pieces), :] = jnp.zeros((rows, LANES), F32)
    for k in range(out.shape[0]):
        out[k] = tile[pl.ds(8 * k, 8), :].astype(BF16)


def k_hidden(recv, scaled, out, mid_out):
    rows = scaled.shape[0]
    total = summed(recv, 0, 8)
    spread = as_column(total[6:7], rows, (0, 1)) / D
    shrink = lax.rsqrt(spread + EPSILON)
    mid_out[...] = rounded(scaled[...] * shrink)
    mine = iota((rows, 1), 0) == kv_index() // (out.shape[0] // rows)
    own = jnp.sum(jnp.where(mine, shrink, 0.0), axis=0, keepdims=True)
    total = total * own
    up = pltpu.roll(total, 5, 0)
    hidden = total / (1.0 + jnp.exp(-total)) * up
    hidden = jnp.where(iota((8, LANES), 0) < 3, hidden, 0.0).astype(BF16)
    for k in range(out.shape[0]):
        out[k] = hidden


def k_shrink(recv, w_down, out, tile):
    rows = out.shape[1]
    pieces = recv.shape[0] // rows
    for k in range(recv.shape[0]):
        tile[pl.ds(8 * k, 8), :] = recv[k].astype(F32)
    part = jnp.zeros((rows, LANES), F32)
    columns = w_down.shape[0]
    for t in range(3 * pieces):
        at = 8 * (t // 3) + t % 3
        size = min(LANES, columns - t * LANES)
        hidden = tile[pl.ds(at, rows, stride=8 * pieces), :][:, :size].astype(BF16)
        part = part + jnp.dot(
            hidden, w_down[pl.ds(t * LANES, size), :], preferred_element_type=F32
        )
    part = part.astype(BF16)
    for k in range(out.shape[0]):
        out[k] = part


def k_sums(recv, mid, out, mix_out):
    rows, width = mid.shape
    mixture = mid[...] + summed(recv, 0, rows)
    mix_out[...] = mixture
    centre = jnp.sum(mixture, axis=1, keepdims=True) / width
    square = jnp.sum((mixture - centre) ** 2, axis=1, keepdims=True)
    message = as_row([centre, square])
    for k in range(out.shape[0]):
        out[k] = message


def k_finish(recv, mix, gain, out, turned):
    rows, width = mix.shape
    devices = recv.shape[0]
    total = recv[0]
    for k in range(1, devices):
        total = total + recv[k]
    middle = total / devices
    spread = (recv[0] - middle) ** 2
    for k in range(1, devices):
        spread = spread + (recv[k] - middle) ** 2
    square = jnp.where(iota((1, LANES), 1) < rows, spread * width, total)
    centre = as_column(middle, rows, (0,))
    shrink = lax.rsqrt(as_column(square, rows, (0, 1)) / D + EPSILON)
    own = out.shape[0]
    scaled = ((mix[...] - centre) * shrink).T
    at = pl.multiple_of(lax.axis_index("tp") * own, own)
    turned[...] = scaled
    gain_col = jnp.sum(jnp.where(diagonal(own, 0)[:, :own], gain[...], 0.0), axis=1, keepdims=True)
    out[...] = (turned[pl.ds(at, own), :] * gain_col).astype(BF16)


def on_device(
    tokens,
    live_lengths,
    kv_cache,
    gate_sums,
    w_query,
    w_key,
    w_value,
    w_forget,
    forget_bias,
    w_out,
    first_gain,
    w_gate,
    w_up,
    w_down,
    second_gain,
):
    rows, own = tokens.shape
    kv, tp = lax.axis_size(KV), lax.axis_size("tp")
    width = own * tp
    block = ((rows, LANES), F32)
    message = jnp.broadcast_to(tokens.T[None], (tp, own, rows))
    in_hbm = functools.partial(pltpu.with_memory_space_constraint, memory_space=pltpu.HBM)
    recv = exchanged(message, "tp").reshape(width, rows)
    heads = w_query.shape[1]
    w_query, w_key, w_value, w_forget, w_out, tails = kernel(
        k_weights,
        [
            ((width, heads), BF16),
            ((DH, width), BF16),
            ((DH, width), BF16),
            ((w_forget.shape[1], width), BF16),
            ((heads, width), BF16),
            ((2, 8, LANES), F32),
        ],
        [ANY] * 7,
        [
            pltpu.VMEM((1, own), F32),
            pltpu.VMEM((1, w_forget.shape[1]), F32),
            pltpu.SemaphoreType.DMA((7,)),
        ],
    )(
        in_hbm(w_query),
        in_hbm(w_key.T),
        in_hbm(w_value.T),
        in_hbm(w_forget.T),
        in_hbm(w_out),
        in_hbm(first_gain[None]),
        in_hbm(forget_bias[None]),
    )
    message, x = kernel(
        k_project,
        [((kv, rows // 2 + 1, 4, LANES), BF16), block],
        [VMEM] * 6,
        [pltpu.VMEM((rows, LANES), F32)],
    )(recv, w_query, w_key, w_value, w_forget, tails)
    recv = exchanged(message, KV)
    positions = kv_cache.shape[1]
    keys, values, gate_sums = kernel(
        k_prepare,
        [
            ((rows // 2, 2 * DH, positions), BF16),
            ((rows // 2, positions, 2 * DH), BF16),
            ((rows // 2, 8, positions), F32),
        ],
        [SMEM, ANY, ANY],
        [
            pltpu.VMEM(kv_cache.shape, BF16),
            pltpu.VMEM(gate_sums.shape, F32),
            pltpu.SemaphoreType.DMA((rows,)),
            pltpu.SemaphoreType.DMA,
        ],
    )(live_lengths, in_hbm(kv_cache), in_hbm(gate_sums))
    message, tok, sums = kernel(
        k_attend,
        [((kv, rows // 2 + 1, 4, LANES), BF16), block, ((2, LANES), F32)],
        [VMEM] * 4,
        [pltpu.VMEM((4 * rows, LANES), F32), pltpu.VMEM((4 * rows, LANES), F32)],
    )(recv, keys, values, gate_sums)
    (message,) = kernel(k_combine, [((tp, rows // 4 + 1, 4, width), BF16)], [VMEM] * 4)(
        exchanged(message, KV), sums, w_out, tails
    )
    message, scaled = kernel(
        k_expand,
        [((kv, 8, LANES), BF16), block],
        [VMEM] * 5,
        [pltpu.VMEM((8 * kv, LANES), F32)],
    )(exchanged(message, "tp"), x, tok, w_gate.T, w_up.T)
    message, mid = kernel(k_hidden, [((kv, 8, LANES), BF16), block], [VMEM] * 2)(
        exchanged(message, KV), scaled
    )
    (message,) = kernel(
        k_shrink, [((tp, rows, width), BF16)], [VMEM] * 2, [pltpu.VMEM((8 * kv, LANES), F32)]
    )(exchanged(message, KV), w_down)
    message, mix = kernel(k_sums, [((kv, 1, LANES), F32), block], [VMEM] * 2)(
        exchanged(message, "tp"), mid
    )
    (out,) = kernel(
        k_finish, [((own, rows), BF16)], [VMEM] * 3, [pltpu.VMEM((width, rows), F32)], last=True
    )(exchanged(message, KV), mix, second_gain[None])
    return out.T


def solution(mesh):
    split = Mesh(mesh.devices.reshape(8, 4, mesh.shape["tp"]), ("kv_0", "kv_1", "tp"))
    placed = (
        P(None, KV_TP),
        P(),
        P(None, KV, "tp"),
        P(None, "tp", KV),
        P(KV, "tp"),
        P(KV, "tp"),
        P(KV, "tp"),
        P(),
        P(),
        P("tp", KV),
        P(KV_TP),
        P(KV, "tp"),
        P(KV, "tp"),
        P("tp", KV),
        P(KV_TP),
    )
    return jax.shard_map(
        on_device, mesh=split, in_specs=placed, out_specs=P(None, KV_TP), check_vma=False
    )
```

```python
import functools

import jax
import jax.numpy as jnp
from jax import lax
from jax.experimental import pallas as pl
from jax.experimental.pallas import tpu as pltpu
from jax.sharding import Mesh
from jax.sharding import PartitionSpec as P

D = 4096
DH = 64
LANES = 128
KV = ("kv_0", "kv_1")
KV_TP = ("kv_0", "kv_1", "tp")
EPSILON = 1e-05
EMPTY_SCORE = -1e30
F32 = jnp.float32
BF16 = jnp.bfloat16

VMEM = pl.BlockSpec(memory_space=pltpu.VMEM)
SMEM = pl.BlockSpec(memory_space=pltpu.SMEM)
ANY = pl.BlockSpec(memory_space=pl.ANY)


def kernel(body, outs, specs, scratch=(), last=False):
    return pl.pallas_call(
        body,
        out_shape=[
            jax.ShapeDtypeStruct(shape, dtype) if last else pltpu.VMEM(shape, dtype)
            for shape, dtype in outs
        ],
        in_specs=specs,
        out_specs=[VMEM] * len(outs),
        scratch_shapes=scratch,
        compiler_params=pltpu.CompilerParams(vmem_limit_bytes=8 * 2**20),
    )


def exchanged(pieces, axis):
    return lax.all_to_all(pieces, axis, 0, 0, tiled=True)


def kv_index():
    return lax.axis_index("kv_0") * lax.axis_size("kv_1") + lax.axis_index("kv_1")


def iota(shape, dim):
    return lax.broadcasted_iota(jnp.int32, shape, dim)


def rounded(x):
    return x.astype(BF16).astype(F32)


def in_pieces(value, count):
    pieces = []
    for _ in range(count):
        piece = rounded(value)
        pieces.append(piece)
        value = value - piece
    return pieces


def diagonal(rows, turn):
    return iota((rows, LANES), 1) == iota((rows, LANES), 0) + rows * turn


def across(left, right, sides):
    return lax.dot_general(left, right, (sides, ((), ())), preferred_element_type=F32)


LAST = ((1,), (1,))
FIRST = ((0,), (0,))


def as_row(columns):
    rows = columns[0].shape[0]
    tile = jnp.zeros((rows, LANES), F32)
    for turn, column in enumerate(columns):
        tile = jnp.where(diagonal(rows, turn), column, tile)
    return jnp.sum(tile, axis=0, keepdims=True)


def as_column(row, rows, turns):
    mask = diagonal(rows, turns[0])
    for turn in turns[1:]:
        mask = mask | diagonal(rows, turn)
    return jnp.sum(jnp.where(mask, row, 0.0), axis=1, keepdims=True)


def summed(ref, start, size):
    total = ref[0, pl.ds(start, size)].astype(F32)
    for k in range(1, ref.shape[0]):
        total = total + ref[k, pl.ds(start, size)].astype(F32)
    return total


def tiles_of(block):
    return [block[4 * t : 4 * t + 4] for t in range(block.shape[0] // 4)]


def put(out, k, tiles):
    for t, tile in enumerate(tiles):
        out[k, t] = tile


def tiles_summed(ref, start, count):
    tiles = []
    for t in range(start, start + count):
        total = ref[0, t].astype(F32)
        for k in range(1, ref.shape[0]):
            total = total + ref[k, t].astype(F32)
        tiles.append(total)
    return tiles[0] if count == 1 else jnp.concatenate(tiles, axis=0)


def k_weights(
    query,
    key,
    value,
    forget,
    w_out,
    gain_hbm,
    bias_hbm,
    query_o,
    key_o,
    value_o,
    forget_o,
    w_out_o,
    tail_o,
    gain,
    bias,
    sem,
):
    width = forget_o.shape[1]
    start = pl.multiple_of(kv_index() * width, width)
    pairs = [(w_out, w_out_o), (query, query_o), (key, key_o), (value, value_o)]
    pairs.append((forget.at[:, pl.ds(start, width)], forget_o))
    pairs.extend([(gain_hbm, gain), (bias_hbm, bias)])
    copies = [pltpu.make_async_copy(a, b, sem.at[k]) for k, (a, b) in enumerate(pairs)]
    for copy in copies:
        copy.start()
    row = iota((8, LANES), 0)
    for copy in copies:
        copy.wait()
    own = gain.shape[1]
    place = iota((own, LANES), 0) + lax.axis_index("tp") * own
    spread = jnp.where(iota((own, LANES), 1) == place, 1.0, 0.0)
    column = jnp.sum(jnp.where(diagonal(own, 0)[:, :own], gain[...], 0.0), axis=1, keepdims=True)
    gains = in_pieces(jnp.sum(spread * column, axis=0, keepdims=True), 3)
    sums = across(jnp.ones((8, LANES), BF16), w_out_o[...], LAST)
    tail = jnp.where(row == 2, sums[:, :LANES], 0.0)
    tail_o[0] = jnp.where(row == 3, sums[:, LANES:], tail)
    mine = iota(bias.shape, 1) == lax.axis_index("tp")
    once = jnp.where(kv_index() == 0, 1.0, 0.0)
    own_bias = jnp.sum(jnp.where(mine, bias[...], 0.0), axis=1, keepdims=True) * once
    tail = jnp.where(row == 0, own_bias, 0.0)
    for k, piece in enumerate(gains):
        tail = jnp.where(row == 1 + k, piece, tail)
    tail_o[1] = tail


def k_project(recv, w_query, w_key, w_value, wf, tails, out, x_out, new_rows):
    width = wf.shape[1]
    same = jnp.where(iota((width, width), 0) == iota((width, width), 1), 1.0, 0.0).astype(BF16)
    x = across(recv[...], same, FIRST)
    x_out[...] = x
    rows = x.shape[0]
    xb = x.astype(BF16)
    query = jnp.dot(xb, w_query[...], preferred_element_type=F32)
    new_rows[:, :DH] = across(xb, w_key[...], LAST)
    new_rows[:, DH:] = across(xb, w_value[...], LAST)
    forget = across(xb, wf[...], LAST)
    token_col = jnp.sum(x, axis=1, keepdims=True)
    mine = iota(forget.shape, 1) == lax.axis_index("tp")
    forget_col = jnp.sum(jnp.where(mine, forget, 0.0), axis=1, keepdims=True)
    forget_col = forget_col + tails[1, 0:1, 0:1]
    small = as_row([*in_pieces(forget_col, 2), *in_pieces(token_col, 2)])
    row = iota((8, LANES), 0)
    tail = jnp.where(row == 1, small, tails[0])
    tiles = tiles_of(query[:, :LANES].astype(BF16)) + tiles_of(query[:, LANES:].astype(BF16))
    for b in range(rows):
        own_tail = jnp.where(row == 0, new_rows[pl.ds(b, 1), :], tail)[:4].astype(BF16)
        for k in range(b, out.shape[0], rows):
            put(out, k, [*tiles, own_tail])


def k_prepare(lengths, cache, gate, keys_o, values_o, gate_o, cache_v, gate_v, sem, gate_sem):
    rows, positions = cache.shape[:2]
    copies = [pltpu.make_async_copy(cache.at[b], cache_v.at[b], sem.at[b]) for b in range(rows)]
    gates = pltpu.make_async_copy(gate, gate_v, gate_sem)
    gates.start()
    for copy in copies:
        copy.start()
    gates.wait()
    place = kv_index() * positions + iota((8, positions), 1)
    first = iota((8, positions), 0) < 4
    for m in range(rows // 2):
        one = jnp.where(place < lengths[2 * m], gate_v[2 * m], EMPTY_SCORE)
        two = jnp.where(place < lengths[2 * m + 1], gate_v[2 * m + 1], EMPTY_SCORE)
        gate_o[m // 2, pl.ds(8 * (m % 2), 8), :] = jnp.where(first, one, two)
    for b in range(rows):
        copies[b].wait()
        keys_o[b // 4, pl.ds(DH * (b % 4), DH), :] = cache_v[b].T[:DH]
        if b % 2:
            values_o[b // 4, :, pl.ds(LANES * (b % 4 // 2), LANES)] = jnp.concatenate(
                [cache_v[b - 1][:, DH:], cache_v[b][:, DH:]], axis=1
            )


def k_attend(recv, keys, values, gate, out, tok_out, sums_out, qs, os):
    rows = 4 * keys.shape[0]
    heads = 4
    scale = DH**-0.5
    left = rounded(tiles_summed(recv, 0, rows // 4))
    right = rounded(tiles_summed(recv, rows // 4, rows // 4))
    tail = tiles_summed(recv, rows // 2, 1)
    new_row = rounded(tail[0:1])
    small = tail[1:2]
    sums_out[...] = tail[2:4]
    tok_out[...] = jnp.broadcast_to(as_column(small, rows, (2, 3)), tok_out.shape)
    even = iota((rows, LANES), 0) % 2 == 0
    low = iota((rows, LANES), 1) < DH
    keep = even == low
    left_turned = pltpu.roll(left, DH, 1)
    right_turned = pltpu.roll(right, DH, 1)
    placed = (
        jnp.where(even, left, left_turned),
        jnp.where(even, left_turned, left),
        jnp.where(even, right, right_turned),
        jnp.where(even, right_turned, right),
    )
    for h, block in enumerate(placed):
        qs[pl.ds(h, rows, stride=heads), :] = jnp.where(keep, block, 0.0)
    all_rows = rows * heads
    owner = iota((all_rows, LANES), 0) // heads
    lane = iota((all_rows, LANES), 1)
    fetched = jnp.where((lane == owner) | (lane == owner + rows), small, 0.0)
    fetched = jnp.sum(fetched, axis=1, keepdims=True)
    new_gate = jnp.minimum(fetched, 0.0) - jnp.log(1.0 + jnp.exp(-jnp.abs(fetched)))
    lane = iota((1, LANES), 1)
    new_turned = pltpu.roll(jnp.broadcast_to(new_row, (8, LANES)), DH, 1)[0:1]
    new_key = jnp.where(lane < DH, new_row, new_turned)
    new_value = jnp.where(lane < DH, new_turned, new_row)
    own = jnp.sum(qs[...] * new_key, axis=1, keepdims=True) * scale
    mine = iota((all_rows, 1), 0) // heads == kv_index()
    own = jnp.where(mine, own, EMPTY_SCORE)
    lane = iota((16, LANES), 1)
    spot = jnp.where(iota((16, LANES), 0) % 8 < heads, DH, 0)
    upper = iota((16, LANES), 0) < 8
    for m in range(rows // 4):
        at = slice(16 * m, 16 * m + 16)
        query = qs[pl.ds(16 * m, 16), :] * scale
        query = [jnp.where(upper, query, 0.0), jnp.where(upper, 0.0, query)]
        query = jnp.concatenate(query, axis=1).astype(BF16)
        scores = jnp.dot(query, keys[m], preferred_element_type=F32)
        scores = scores + (gate[m] + new_gate[at])
        top = jnp.maximum(jnp.max(scores, axis=1, keepdims=True), own[at])
        top = jnp.maximum(top, 0.1 * EMPTY_SCORE)
        weights = jnp.exp(scores - top)
        own_weight = jnp.exp(own[at] - top)
        total = jnp.sum(weights, axis=1, keepdims=True) + own_weight
        value = jnp.dot(weights.astype(BF16), values[m], preferred_element_type=F32)
        value = jnp.where(upper, value[:, :LANES], value[:, LANES:])
        value = value + rounded(own_weight) * new_value
        spare = jnp.where(lane == spot, top, jnp.where(lane == spot + 1, total, value))
        os[pl.ds(16 * m, 16), :] = spare
    blocks = [os[pl.ds(h, rows, stride=heads), :] for h in range(heads)]
    turned = [pltpu.roll(block, DH, 1) for block in blocks]
    firsts = [jnp.where(even, block, turn) for block, turn in zip(blocks, turned)]
    seconds = [jnp.where(even, turn, block) for block, turn in zip(blocks, turned)]
    low_out = jnp.where(low, firsts[0], seconds[1]).astype(BF16)
    high_out = jnp.where(low, firsts[2], seconds[3]).astype(BF16)
    lane = iota((rows, LANES), 1)
    stats = jnp.zeros((rows, LANES), F32)
    for h in range(heads):
        pieces = [*in_pieces(seconds[h][:, 0:1], 3), *in_pieces(seconds[h][:, 1:2], 2)]
        for k, piece in enumerate(pieces):
            stats = jnp.where(lane == 8 * h + k, piece, stats)
    packed = stats[:4]
    for g in range(1, rows // 4):
        packed = packed + pltpu.roll(stats, 32 * g, 1)[4 * g : 4 * g + 4]
    tiles = [*tiles_of(low_out), *tiles_of(high_out), packed.astype(BF16)]
    for k in range(out.shape[0]):
        put(out, k, tiles)


def k_combine(recv, sums, w_out, tails, out):
    devices = recv.shape[0]
    tiles = (recv.shape[1] - 1) // 2
    rows = 4 * tiles
    heads = 4 * DH
    source = iota((LANES, 2 * heads), 0) % 32
    column = iota((LANES, 2 * heads), 1)
    first = 8 * ((column % heads) // DH)
    is_top = column < heads
    begin = jnp.where(is_top, first, first + 3)
    end = jnp.where(is_top, first + 3, first + 5)
    spread = jnp.where((source >= begin) & (source < end), 1.0, 0.0).astype(BF16)
    stats = recv[:, 2 * tiles].astype(F32)
    stats = jnp.concatenate([stats, stats], axis=1)
    group = iota(stats.shape, 2) // 32 - iota(stats.shape, 1) // 4
    blocks = []
    for half in range(2):
        mine = jnp.where(group == 2 * half, stats, 0.0).astype(BF16).reshape(devices * 8, LANES)
        wide = jnp.dot(mine, spread, preferred_element_type=F32).reshape(devices, 8, 2 * heads)
        tops = wide[:, :, :heads]
        totals = wide[:, :, heads:]
        scales = jnp.exp(tops - jnp.max(tops, axis=0, keepdims=True))
        total = jnp.sum(totals * scales, axis=0)
        sides = []
        for side in range(2):
            at = tiles * side + 2 * half
            part = [recv[:, at + t].astype(F32) for t in range(2)]
            part = jnp.concatenate(part, axis=1)
            sides.append(jnp.sum(part * scales[:, :, side * LANES : (side + 1) * LANES], axis=0))
        blocks.append(jnp.concatenate(sides, axis=1) / total)
    attended = jnp.concatenate(blocks, axis=0).astype(BF16)
    attn_part = jnp.dot(attended, w_out[...], preferred_element_type=F32).astype(BF16)
    wide = attended.astype(F32)
    mean = wide[:, :LANES] * sums[0:1, :] + wide[:, LANES:] * sums[1:2, :]
    mean_row = as_row(in_pieces(jnp.sum(mean, axis=1, keepdims=True), 2))
    row = iota((8, LANES), 0)
    tail = jnp.where(row == 0, mean_row, tails[1])
    pieces = [*tiles_of(attn_part), tail[:4].astype(BF16)]
    for k in range(out.shape[0]):
        put(out, k, pieces)


def k_expand(recv, x, tok, w_gate, w_up, out, scaled_out, tile):
    rows = x.shape[0]
    added = tiles_summed(recv, 0, rows // 4)
    tail = tiles_summed(recv, rows // 4, 1)
    mean = as_column(tail[0:1], rows, (0, 1))
    gain = tail[1:2] + tail[2:3] + tail[3:4]
    centre = (tok[:, 0:1] + mean) / D
    centred = x[...] + added - centre
    scaled = centred * gain
    scaled_out[...] = scaled
    squares = as_row(in_pieces(jnp.sum(centred * centred, axis=1, keepdims=True), 2))
    scaled = scaled.astype(BF16)
    pieces = tile.shape[0] // (8 * rows)
    tiles = 3 * pieces
    columns = w_gate.shape[0]
    for k, weight in enumerate((w_gate, w_up)):
        part = across(scaled, weight[...], LAST)
        pad = jnp.zeros((rows, tiles * LANES - columns), F32)
        part = jnp.concatenate([part, pad], axis=1)
        for t in range(tiles):
            at = 8 * (t // 3) + 3 * k + t % 3
            tile[pl.ds(at, rows, stride=8 * pieces), :] = part[:, t * LANES : (t + 1) * LANES]
    for h in range(pieces):
        tile[pl.ds(8 * h + 6, rows, stride=8 * pieces), :] = jnp.broadcast_to(
            squares, (rows, LANES)
        )
        tile[pl.ds(8 * h + 7, rows, stride=8 * pieces), :] = jnp.zeros((rows, LANES), F32)
    for k in range(out.shape[0]):
        out[k] = tile[pl.ds(8 * k, 8), :].astype(BF16)


def k_hidden(recv, scaled, out, mid_out):
    rows = scaled.shape[0]
    total = summed(recv, 0, 8)
    spread = as_column(total[6:7], rows, (0, 1)) / D
    shrink = lax.rsqrt(spread + EPSILON)
    mid_out[...] = rounded(scaled[...] * shrink)
    mine = iota((rows, 1), 0) == kv_index() // (out.shape[0] // rows)
    own = jnp.sum(jnp.where(mine, shrink, 0.0), axis=0, keepdims=True)
    total = total * own
    up = pltpu.roll(total, 5, 0)
    hidden = total / (1.0 + jnp.exp(-total)) * up
    hidden = jnp.where(iota((8, LANES), 0) < 3, hidden, 0.0)[:4].astype(BF16)
    for k in range(out.shape[0]):
        out[k] = hidden


def k_shrink(recv, w_down, out, tile):
    rows = out.shape[1]
    pieces = recv.shape[0] // rows
    for k in range(recv.shape[0]):
        tile[pl.ds(4 * k, 4), :] = recv[k].astype(F32)
    part = jnp.zeros((rows, LANES), F32)
    columns = w_down.shape[0]
    for t in range(3 * pieces):
        at = 4 * (t // 3) + t % 3
        size = min(LANES, columns - t * LANES)
        hidden = tile[pl.ds(at, rows, stride=4 * pieces), :][:, :size].astype(BF16)
        part = part + jnp.dot(
            hidden, w_down[pl.ds(t * LANES, size), :], preferred_element_type=F32
        )
    part = part.astype(BF16)
    for k in range(out.shape[0]):
        out[k] = part


def k_sums(recv, mid, out, mix_out):
    rows, width = mid.shape
    mixture = mid[...] + summed(recv, 0, rows)
    mix_out[...] = mixture
    centre = jnp.sum(mixture, axis=1, keepdims=True) / width
    square = jnp.sum((mixture - centre) ** 2, axis=1, keepdims=True)
    message = as_row([centre, square])
    for k in range(out.shape[0]):
        out[k] = message


def k_finish(recv, mix, gain, out, turned):
    rows, width = mix.shape
    devices = recv.shape[0]
    total = recv[0]
    for k in range(1, devices):
        total = total + recv[k]
    middle = total / devices
    spread = (recv[0] - middle) ** 2
    for k in range(1, devices):
        spread = spread + (recv[k] - middle) ** 2
    square = jnp.where(iota((1, LANES), 1) < rows, spread * width, total)
    centre = as_column(middle, rows, (0,))
    shrink = lax.rsqrt(as_column(square, rows, (0, 1)) / D + EPSILON)
    own = out.shape[0]
    scaled = ((mix[...] - centre) * shrink).T
    at = pl.multiple_of(lax.axis_index("tp") * own, own)
    turned[...] = scaled
    gain_col = jnp.sum(jnp.where(diagonal(own, 0)[:, :own], gain[...], 0.0), axis=1, keepdims=True)
    out[...] = (turned[pl.ds(at, own), :] * gain_col).astype(BF16)


def on_device(
    tokens,
    live_lengths,
    kv_cache,
    gate_sums,
    w_query,
    w_key,
    w_value,
    w_forget,
    forget_bias,
    w_out,
    first_gain,
    w_gate,
    w_up,
    w_down,
    second_gain,
):
    rows, own = tokens.shape
    kv, tp = lax.axis_size(KV), lax.axis_size("tp")
    width = own * tp
    block = ((rows, LANES), F32)
    message = jnp.broadcast_to(tokens.T[None], (tp, own, rows))
    in_hbm = functools.partial(pltpu.with_memory_space_constraint, memory_space=pltpu.HBM)
    recv = exchanged(message, "tp").reshape(width, rows)
    heads = w_query.shape[1]
    w_query, w_key, w_value, w_forget, w_out, tails = kernel(
        k_weights,
        [
            ((width, heads), BF16),
            ((DH, width), BF16),
            ((DH, width), BF16),
            ((w_forget.shape[1], width), BF16),
            ((heads, width), BF16),
            ((2, 8, LANES), F32),
        ],
        [ANY] * 7,
        [
            pltpu.VMEM((1, own), F32),
            pltpu.VMEM((1, w_forget.shape[1]), F32),
            pltpu.SemaphoreType.DMA((7,)),
        ],
    )(
        in_hbm(w_query),
        in_hbm(w_key.T),
        in_hbm(w_value.T),
        in_hbm(w_forget.T),
        in_hbm(w_out),
        in_hbm(first_gain[None]),
        in_hbm(forget_bias[None]),
    )
    message, x = kernel(
        k_project,
        [((kv, rows // 2 + 1, 4, LANES), BF16), block],
        [VMEM] * 6,
        [pltpu.VMEM((rows, LANES), F32)],
    )(recv, w_query, w_key, w_value, w_forget, tails)
    recv = exchanged(message, KV)
    positions = kv_cache.shape[1]
    keys, values, gate_sums = kernel(
        k_prepare,
        [
            ((rows // 4, 4 * DH, positions), BF16),
            ((rows // 4, positions, 4 * DH), BF16),
            ((rows // 4, 16, positions), F32),
        ],
        [SMEM, ANY, ANY],
        [
            pltpu.VMEM(kv_cache.shape, BF16),
            pltpu.VMEM(gate_sums.shape, F32),
            pltpu.SemaphoreType.DMA((rows,)),
            pltpu.SemaphoreType.DMA,
        ],
    )(live_lengths, in_hbm(kv_cache), in_hbm(gate_sums))
    message, tok, sums = kernel(
        k_attend,
        [((kv, rows // 2 + 1, 4, LANES), BF16), block, ((2, LANES), F32)],
        [VMEM] * 4,
        [pltpu.VMEM((4 * rows, LANES), F32), pltpu.VMEM((4 * rows, LANES), F32)],
    )(recv, keys, values, gate_sums)
    (message,) = kernel(k_combine, [((tp, rows // 4 + 1, 4, width), BF16)], [VMEM] * 4)(
        exchanged(message, KV), sums, w_out, tails
    )
    message, scaled = kernel(
        k_expand,
        [((kv, 8, LANES), BF16), block],
        [VMEM] * 5,
        [pltpu.VMEM((8 * kv, LANES), F32)],
    )(exchanged(message, "tp"), x, tok, w_gate.T, w_up.T)
    message, mid = kernel(k_hidden, [((kv, 4, LANES), BF16), block], [VMEM] * 2)(
        exchanged(message, KV), scaled
    )
    (message,) = kernel(
        k_shrink, [((tp, rows, width), BF16)], [VMEM] * 2, [pltpu.VMEM((4 * kv, LANES), F32)]
    )(exchanged(message, KV), w_down)
    message, mix = kernel(k_sums, [((kv, 1, LANES), F32), block], [VMEM] * 2)(
        exchanged(message, "tp"), mid
    )
    (out,) = kernel(
        k_finish, [((own, rows), BF16)], [VMEM] * 3, [pltpu.VMEM((width, rows), F32)], last=True
    )(exchanged(message, KV), mix, second_gain[None])
    return out.T


def solution(mesh):
    split = Mesh(mesh.devices.reshape(8, 4, mesh.shape["tp"]), ("kv_0", "kv_1", "tp"))
    placed = (
        P(None, KV_TP),
        P(),
        P(None, KV, "tp"),
        P(None, "tp", KV),
        P(KV, "tp"),
        P(KV, "tp"),
        P(KV, "tp"),
        P(),
        P(),
        P("tp", KV),
        P(KV_TP),
        P(KV, "tp"),
        P(KV, "tp"),
        P("tp", KV),
        P(KV_TP),
    )
    return jax.shard_map(
        on_device, mesh=split, in_specs=placed, out_specs=P(None, KV_TP), check_vma=False
    )
```

```python
import functools

import jax
import jax.numpy as jnp
from jax import lax
from jax.experimental import pallas as pl
from jax.experimental.pallas import tpu as pltpu
from jax.sharding import Mesh
from jax.sharding import PartitionSpec as P

D = 4096
DH = 64
LANES = 128
KV = ("kv_0", "kv_1")
KV_TP = ("kv_0", "kv_1", "tp")
EPSILON = 1e-05
EMPTY_SCORE = -1e30
F32 = jnp.float32
BF16 = jnp.bfloat16

VMEM = pl.BlockSpec(memory_space=pltpu.VMEM)
SMEM = pl.BlockSpec(memory_space=pltpu.SMEM)
ANY = pl.BlockSpec(memory_space=pl.ANY)


def kernel(body, outs, specs, scratch=(), last=False, flops=None):
    return pl.pallas_call(
        body,
        out_shape=[
            jax.ShapeDtypeStruct(shape, dtype) if last else pltpu.VMEM(shape, dtype)
            for shape, dtype in outs
        ],
        in_specs=specs,
        out_specs=[VMEM] * len(outs),
        scratch_shapes=scratch,
        cost_estimate=flops
        and pl.CostEstimate(flops=flops, bytes_accessed=flops // 100, transcendentals=0),
        compiler_params=pltpu.CompilerParams(vmem_limit_bytes=8 * 2**20),
    )


def exchanged(pieces, axis):
    return lax.all_to_all(pieces, axis, 0, 0, tiled=True)


def kv_index():
    return lax.axis_index("kv_0") * lax.axis_size("kv_1") + lax.axis_index("kv_1")


def iota(shape, dim):
    return lax.broadcasted_iota(jnp.int32, shape, dim)


def rounded(x):
    return x.astype(BF16).astype(F32)


def in_pieces(value, count):
    pieces = []
    for _ in range(count):
        piece = rounded(value)
        pieces.append(piece)
        value = value - piece
    return pieces


def diagonal(rows, turn):
    return iota((rows, LANES), 1) == iota((rows, LANES), 0) + rows * turn


def across(left, right, sides):
    return lax.dot_general(left, right, (sides, ((), ())), preferred_element_type=F32)


LAST = ((1,), (1,))
FIRST = ((0,), (0,))


def as_row(columns):
    rows = columns[0].shape[0]
    tile = jnp.zeros((rows, LANES), F32)
    for turn, column in enumerate(columns):
        tile = jnp.where(diagonal(rows, turn), column, tile)
    return jnp.sum(tile, axis=0, keepdims=True)


def as_column(row, rows, turns):
    mask = diagonal(rows, turns[0])
    for turn in turns[1:]:
        mask = mask | diagonal(rows, turn)
    return jnp.sum(jnp.where(mask, row, 0.0), axis=1, keepdims=True)


def summed(ref, start, size):
    total = ref[0, pl.ds(start, size)].astype(F32)
    for k in range(1, ref.shape[0]):
        total = total + ref[k, pl.ds(start, size)].astype(F32)
    return total


def tiles_of(block):
    return [block[4 * t : 4 * t + 4] for t in range(block.shape[0] // 4)]


def put(out, k, tiles):
    for t, tile in enumerate(tiles):
        out[k, t] = tile


def tiles_summed(ref, start, count):
    tiles = []
    for t in range(start, start + count):
        total = ref[0, t].astype(F32)
        for k in range(1, ref.shape[0]):
            total = total + ref[k, t].astype(F32)
        tiles.append(total)
    return tiles[0] if count == 1 else jnp.concatenate(tiles, axis=0)


def k_start(turned_hbm, gain_hbm, out, turned, gain, sem):
    pairs = ((turned_hbm, turned), (gain_hbm, gain))
    copies = [pltpu.make_async_copy(a, b, sem.at[k]) for k, (a, b) in enumerate(pairs)]
    for copy in copies:
        copy.start()
    for copy in copies:
        copy.wait()
    own, rows = turned.shape
    column = jnp.sum(jnp.where(diagonal(own, 0)[:, :own], gain[...], 0.0), axis=1, keepdims=True)
    pad = jnp.zeros((own, LANES - rows), F32)
    tile = jnp.concatenate([turned[...].astype(F32), pad], axis=1)
    for k, piece in enumerate(in_pieces(column, 3)):
        tile = jnp.where(iota(tile.shape, 1) == rows + k, piece, tile)
    tile = tile.astype(BF16)
    for k in range(out.shape[0]):
        out[k] = tile


def k_project(recv, w_query, w_key, w_value, w_forget, w_out, bias, out, x_out, gain_out, new_rows):
    width = recv.shape[0]
    same = jnp.where(iota((width, width), 0) == iota((width, width), 1), 1.0, 0.0).astype(BF16)
    rows = new_rows.shape[0]
    both = across(recv[:, : 2 * rows], same, FIRST)
    x = both[:rows]
    x_out[...] = x
    gain = both[rows : rows + 1] + both[rows + 1 : rows + 2] + both[rows + 2 : rows + 3]
    gain_out[...] = jnp.broadcast_to(gain, gain_out.shape)
    xb = x.astype(BF16)
    row = iota((8, LANES), 0)
    sums = across(jnp.ones((8, LANES), BF16), w_out[...], LAST)
    mine = iota(bias.shape, 1) == lax.axis_index("tp")
    once = jnp.where(kv_index() == 0, 1.0, 0.0)
    own_bias = jnp.sum(jnp.where(mine, bias[...], 0.0), axis=1, keepdims=True) * once
    query = jnp.dot(xb, w_query[...], preferred_element_type=F32)
    new_rows[:, :DH] = across(xb, w_key[...], LAST)
    new_rows[:, DH:] = across(xb, w_value[...], LAST)
    start = pl.multiple_of(kv_index() * width, width)
    forget = across(xb, w_forget[:, pl.ds(start, width)], LAST)
    token_col = jnp.sum(x, axis=1, keepdims=True)
    mine = iota(forget.shape, 1) == lax.axis_index("tp")
    forget_col = jnp.sum(jnp.where(mine, forget, 0.0), axis=1, keepdims=True)
    forget_col = forget_col + own_bias
    small = as_row([*in_pieces(forget_col, 2), *in_pieces(token_col, 2)])
    tail = jnp.where(row == 1, small, 0.0)
    tail = jnp.where(row == 2, sums[:, :LANES], tail)
    tail = jnp.where(row == 3, sums[:, LANES:], tail)
    tiles = tiles_of(query[:, :LANES].astype(BF16)) + tiles_of(query[:, LANES:].astype(BF16))
    for b in range(rows):
        own_tail = jnp.where(row == 0, new_rows[pl.ds(b, 1), :], tail)[:4].astype(BF16)
        for k in range(b, out.shape[0], rows):
            put(out, k, [*tiles, own_tail])


def k_prepare(lengths, cache, gate, keys_o, values_o, gate_o, cache_v, gate_v, sem, gate_sem):
    rows, positions = cache.shape[:2]
    copies = [pltpu.make_async_copy(cache.at[b], cache_v.at[b], sem.at[b]) for b in range(rows)]
    gates = pltpu.make_async_copy(gate, gate_v, gate_sem)
    gates.start()
    for copy in copies:
        copy.start()
    gates.wait()
    place = kv_index() * positions + iota((8, positions), 1)
    first = iota((8, positions), 0) < 4
    for m in range(rows // 2):
        one = jnp.where(place < lengths[2 * m], gate_v[2 * m], EMPTY_SCORE)
        two = jnp.where(place < lengths[2 * m + 1], gate_v[2 * m + 1], EMPTY_SCORE)
        gate_o[m // 2, pl.ds(8 * (m % 2), 8), :] = jnp.where(first, one, two)
    for b in range(rows):
        copies[b].wait()
        keys_o[b // 4, pl.ds(DH * (b % 4), DH), :] = cache_v[b].T[:DH]
        if b % 2:
            values_o[b // 4, :, pl.ds(LANES * (b % 4 // 2), LANES)] = jnp.concatenate(
                [cache_v[b - 1][:, DH:], cache_v[b][:, DH:]], axis=1
            )


def k_attend(recv, keys, values, gate, out, tok_out, sums_out, qs, os):
    rows = 4 * keys.shape[0]
    heads = 4
    scale = DH**-0.5
    left = rounded(tiles_summed(recv, 0, rows // 4))
    right = rounded(tiles_summed(recv, rows // 4, rows // 4))
    tail = tiles_summed(recv, rows // 2, 1)
    new_row = rounded(tail[0:1])
    small = tail[1:2]
    sums_out[...] = tail[2:4]
    tok_out[...] = jnp.broadcast_to(as_column(small, rows, (2, 3)), tok_out.shape)
    even = iota((rows, LANES), 0) % 2 == 0
    low = iota((rows, LANES), 1) < DH
    keep = even == low
    left_turned = pltpu.roll(left, DH, 1)
    right_turned = pltpu.roll(right, DH, 1)
    placed = (
        jnp.where(even, left, left_turned),
        jnp.where(even, left_turned, left),
        jnp.where(even, right, right_turned),
        jnp.where(even, right_turned, right),
    )
    for h, block in enumerate(placed):
        qs[pl.ds(h, rows, stride=heads), :] = jnp.where(keep, block, 0.0)
    all_rows = rows * heads
    owner = iota((all_rows, LANES), 0) // heads
    lane = iota((all_rows, LANES), 1)
    fetched = jnp.where((lane == owner) | (lane == owner + rows), small, 0.0)
    fetched = jnp.sum(fetched, axis=1, keepdims=True)
    new_gate = jnp.minimum(fetched, 0.0) - jnp.log(1.0 + jnp.exp(-jnp.abs(fetched)))
    lane = iota((1, LANES), 1)
    new_turned = pltpu.roll(jnp.broadcast_to(new_row, (8, LANES)), DH, 1)[0:1]
    new_key = jnp.where(lane < DH, new_row, new_turned)
    new_value = jnp.where(lane < DH, new_turned, new_row)
    own = jnp.sum(qs[...] * new_key, axis=1, keepdims=True) * scale
    mine = iota((all_rows, 1), 0) // heads == kv_index()
    own = jnp.where(mine, own, EMPTY_SCORE)
    lane = iota((16, LANES), 1)
    spot = jnp.where(iota((16, LANES), 0) % 8 < heads, DH, 0)
    upper = iota((16, LANES), 0) < 8
    for m in range(rows // 4):
        at = slice(16 * m, 16 * m + 16)
        query = qs[pl.ds(16 * m, 16), :] * scale
        query = [jnp.where(upper, query, 0.0), jnp.where(upper, 0.0, query)]
        query = jnp.concatenate(query, axis=1).astype(BF16)
        scores = jnp.dot(query, keys[m], preferred_element_type=F32)
        scores = scores + (gate[m] + new_gate[at])
        top = jnp.maximum(jnp.max(scores, axis=1, keepdims=True), own[at])
        top = jnp.maximum(top, 0.1 * EMPTY_SCORE)
        weights = jnp.exp(scores - top)
        own_weight = jnp.exp(own[at] - top)
        total = jnp.sum(weights, axis=1, keepdims=True) + own_weight
        value = jnp.dot(weights.astype(BF16), values[m], preferred_element_type=F32)
        value = jnp.where(upper, value[:, :LANES], value[:, LANES:])
        value = value + rounded(own_weight) * new_value
        spare = jnp.where(lane == spot, top, jnp.where(lane == spot + 1, total, value))
        os[pl.ds(16 * m, 16), :] = spare
    blocks = [os[pl.ds(h, rows, stride=heads), :] for h in range(heads)]
    turned = [pltpu.roll(block, DH, 1) for block in blocks]
    firsts = [jnp.where(even, block, turn) for block, turn in zip(blocks, turned)]
    seconds = [jnp.where(even, turn, block) for block, turn in zip(blocks, turned)]
    low_out = jnp.where(low, firsts[0], seconds[1]).astype(BF16)
    high_out = jnp.where(low, firsts[2], seconds[3]).astype(BF16)
    lane = iota((rows, LANES), 1)
    stats = jnp.zeros((rows, LANES), F32)
    for h in range(heads):
        pieces = [*in_pieces(seconds[h][:, 0:1], 3), *in_pieces(seconds[h][:, 1:2], 2)]
        for k, piece in enumerate(pieces):
            stats = jnp.where(lane == 8 * h + k, piece, stats)
    packed = stats[:4]
    for g in range(1, rows // 4):
        packed = packed + pltpu.roll(stats, 32 * g, 1)[4 * g : 4 * g + 4]
    tiles = [*tiles_of(low_out), *tiles_of(high_out), packed.astype(BF16)]
    for k in range(out.shape[0]):
        put(out, k, tiles)


def k_combine(recv, sums, w_out, out):
    devices = recv.shape[0]
    tiles = (recv.shape[1] - 1) // 2
    rows = 4 * tiles
    heads = 4 * DH
    source = iota((LANES, 2 * heads), 0) % 32
    column = iota((LANES, 2 * heads), 1)
    first = 8 * ((column % heads) // DH)
    is_top = column < heads
    begin = jnp.where(is_top, first, first + 3)
    end = jnp.where(is_top, first + 3, first + 5)
    spread = jnp.where((source >= begin) & (source < end), 1.0, 0.0).astype(BF16)
    stats = recv[:, 2 * tiles].astype(F32)
    stats = jnp.concatenate([stats, stats], axis=1)
    group = iota(stats.shape, 2) // 32 - iota(stats.shape, 1) // 4
    blocks = []
    for half in range(2):
        mine = jnp.where(group == 2 * half, stats, 0.0).astype(BF16).reshape(devices * 8, LANES)
        wide = jnp.dot(mine, spread, preferred_element_type=F32).reshape(devices, 8, 2 * heads)
        tops = wide[:, :, :heads]
        totals = wide[:, :, heads:]
        scales = jnp.exp(tops - jnp.max(tops, axis=0, keepdims=True))
        total = jnp.sum(totals * scales, axis=0)
        sides = []
        for side in range(2):
            at = tiles * side + 2 * half
            part = [recv[:, at + t].astype(F32) for t in range(2)]
            part = jnp.concatenate(part, axis=1)
            sides.append(jnp.sum(part * scales[:, :, side * LANES : (side + 1) * LANES], axis=0))
        blocks.append(jnp.concatenate(sides, axis=1) / total)
    attended = jnp.concatenate(blocks, axis=0).astype(BF16)
    wide = attended.astype(F32)
    mean = wide[:, :LANES] * sums[0:1, :] + wide[:, LANES:] * sums[1:2, :]
    mean = jnp.sum(mean, axis=1, keepdims=True) / D
    attn_part = jnp.dot(attended, w_out[...], preferred_element_type=F32)
    attn_part = (attn_part - mean).astype(BF16)
    for k in range(out.shape[0]):
        out[k] = attn_part


def k_expand(recv, x, tok, gain, w_gate, w_up, out, scaled_out, tile):
    rows = x.shape[0]
    centred = x[...] - tok[:, 0:1] / D + summed(recv, 0, rows)
    scaled = centred * gain[0:1, :]
    scaled_out[...] = scaled
    squares = as_row(in_pieces(jnp.sum(centred * centred, axis=1, keepdims=True), 2))
    scaled = scaled.astype(BF16)
    pieces = tile.shape[0] // (8 * rows)
    tiles = 3 * pieces
    columns = w_gate.shape[0]
    for k, weight in enumerate((w_gate, w_up)):
        part = across(scaled, weight[...], LAST)
        pad = jnp.zeros((rows, tiles * LANES - columns), F32)
        part = jnp.concatenate([part, pad], axis=1)
        for t in range(tiles):
            at = 8 * (t // 3) + 3 * k + t % 3
            tile[pl.ds(at, rows, stride=8 * pieces), :] = part[:, t * LANES : (t + 1) * LANES]
    for h in range(pieces):
        tile[pl.ds(8 * h + 6, rows, stride=8 * pieces), :] = jnp.broadcast_to(
            squares, (rows, LANES)
        )
        tile[pl.ds(8 * h + 7, rows, stride=8 * pieces), :] = jnp.zeros((rows, LANES), F32)
    for k in range(out.shape[0]):
        out[k] = tile[pl.ds(8 * k, 8), :].astype(BF16)


def k_hidden(recv, scaled, out, mid_out):
    rows = scaled.shape[0]
    total = summed(recv, 0, 8)
    spread = as_column(total[6:7], rows, (0, 1)) / D
    shrink = lax.rsqrt(spread + EPSILON)
    mid_out[...] = rounded(scaled[...] * shrink)
    mine = iota((rows, 1), 0) == kv_index() // (out.shape[0] // rows)
    own = jnp.sum(jnp.where(mine, shrink, 0.0), axis=0, keepdims=True)
    total = total * own
    up = pltpu.roll(total, 5, 0)
    hidden = total / (1.0 + jnp.exp(-total)) * up
    hidden = jnp.where(iota((8, LANES), 0) < 3, hidden, 0.0)[:4].astype(BF16)
    for k in range(out.shape[0]):
        out[k] = hidden


def k_shrink(recv, w_down, out, tile):
    rows = out.shape[1]
    pieces = recv.shape[0] // rows
    for k in range(recv.shape[0]):
        tile[pl.ds(4 * k, 4), :] = recv[k].astype(F32)
    part = jnp.zeros((rows, LANES), F32)
    columns = w_down.shape[0]
    for t in range(3 * pieces):
        at = 4 * (t // 3) + t % 3
        size = min(LANES, columns - t * LANES)
        hidden = tile[pl.ds(at, rows, stride=4 * pieces), :][:, :size].astype(BF16)
        part = part + jnp.dot(
            hidden, w_down[pl.ds(t * LANES, size), :], preferred_element_type=F32
        )
    part = part.astype(BF16)
    for k in range(out.shape[0]):
        out[k] = part


def k_sums(recv, mid, out, mix_out):
    rows, width = mid.shape
    mixture = mid[...] + summed(recv, 0, rows)
    mix_out[...] = mixture
    centre = jnp.sum(mixture, axis=1, keepdims=True) / width
    square = jnp.sum((mixture - centre) ** 2, axis=1, keepdims=True)
    message = as_row([centre, square])
    for k in range(out.shape[0]):
        out[k] = message


def k_finish(recv, mix, gain, out, turned):
    rows, width = mix.shape
    devices = recv.shape[0]
    total = recv[0]
    for k in range(1, devices):
        total = total + recv[k]
    middle = total / devices
    spread = (recv[0] - middle) ** 2
    for k in range(1, devices):
        spread = spread + (recv[k] - middle) ** 2
    square = jnp.where(iota((1, LANES), 1) < rows, spread * width, total)
    centre = as_column(middle, rows, (0,))
    shrink = lax.rsqrt(as_column(square, rows, (0, 1)) / D + EPSILON)
    own = out.shape[0]
    scaled = ((mix[...] - centre) * shrink).T
    at = pl.multiple_of(lax.axis_index("tp") * own, own)
    turned[...] = scaled
    gain_col = jnp.sum(jnp.where(diagonal(own, 0)[:, :own], gain[...], 0.0), axis=1, keepdims=True)
    out[...] = (turned[pl.ds(at, own), :] * gain_col).astype(BF16)


def on_device(
    tokens,
    live_lengths,
    kv_cache,
    gate_sums,
    w_query,
    w_key,
    w_value,
    w_forget,
    forget_bias,
    w_out,
    first_gain,
    w_gate,
    w_up,
    w_down,
    second_gain,
):
    rows, own = tokens.shape
    kv, tp = lax.axis_size(KV), lax.axis_size("tp")
    width = own * tp
    block = ((rows, LANES), F32)
    in_hbm = functools.partial(pltpu.with_memory_space_constraint, memory_space=pltpu.HBM)
    (message,) = kernel(
        k_start,
        [((tp, own, LANES), BF16)],
        [ANY] * 2,
        [
            pltpu.VMEM((own, rows), BF16),
            pltpu.VMEM((1, own), F32),
            pltpu.SemaphoreType.DMA((2,)),
        ],
        flops=10**11,
    )(in_hbm(tokens.T), in_hbm(first_gain[None]))
    recv = exchanged(message, "tp").reshape(width, LANES)
    message, x, gain = kernel(
        k_project,
        [((kv, rows // 2 + 1, 4, LANES), BF16), block, ((8, LANES), F32)],
        [VMEM] * 7,
        [pltpu.VMEM((rows, LANES), F32)],
    )(
        recv,
        w_query,
        w_key.T,
        w_value.T,
        w_forget.T,
        w_out,
        forget_bias[None],
    )
    recv = exchanged(message, KV)
    positions = kv_cache.shape[1]
    keys, values, gate_sums = kernel(
        k_prepare,
        [
            ((rows // 4, 4 * DH, positions), BF16),
            ((rows // 4, positions, 4 * DH), BF16),
            ((rows // 4, 16, positions), F32),
        ],
        [SMEM, ANY, ANY],
        [
            pltpu.VMEM(kv_cache.shape, BF16),
            pltpu.VMEM(gate_sums.shape, F32),
            pltpu.SemaphoreType.DMA((rows,)),
            pltpu.SemaphoreType.DMA,
        ],
    )(live_lengths, in_hbm(kv_cache), in_hbm(gate_sums))
    message, tok, sums = kernel(
        k_attend,
        [((kv, rows // 2 + 1, 4, LANES), BF16), block, ((2, LANES), F32)],
        [VMEM] * 4,
        [pltpu.VMEM((4 * rows, LANES), F32), pltpu.VMEM((4 * rows, LANES), F32)],
    )(recv, keys, values, gate_sums)
    (message,) = kernel(k_combine, [((tp, rows, width), BF16)], [VMEM] * 3)(
        exchanged(message, KV), sums, w_out
    )
    message, scaled = kernel(
        k_expand,
        [((kv, 8, LANES), BF16), block],
        [VMEM] * 6,
        [pltpu.VMEM((8 * kv, LANES), F32)],
    )(exchanged(message, "tp"), x, tok, gain, w_gate.T, w_up.T)
    message, mid = kernel(k_hidden, [((kv, 4, LANES), BF16), block], [VMEM] * 2)(
        exchanged(message, KV), scaled
    )
    (message,) = kernel(
        k_shrink, [((tp, rows, width), BF16)], [VMEM] * 2, [pltpu.VMEM((4 * kv, LANES), F32)]
    )(exchanged(message, KV), w_down)
    message, mix = kernel(k_sums, [((kv, 1, LANES), F32), block], [VMEM] * 2)(
        exchanged(message, "tp"), mid
    )
    (out,) = kernel(
        k_finish, [((own, rows), BF16)], [VMEM] * 3, [pltpu.VMEM((width, rows), F32)], last=True
    )(exchanged(message, KV), mix, second_gain[None])
    return out.T


def solution(mesh):
    split = Mesh(mesh.devices.reshape(8, 4, mesh.shape["tp"]), ("kv_0", "kv_1", "tp"))
    placed = (
        P(None, KV_TP),
        P(),
        P(None, KV, "tp"),
        P(None, "tp", KV),
        P(KV, "tp"),
        P(KV, "tp"),
        P(KV, "tp"),
        P(),
        P(),
        P("tp", KV),
        P(KV_TP),
        P(KV, "tp"),
        P(KV, "tp"),
        P("tp", KV),
        P(KV_TP),
    )
    return jax.shard_map(
        on_device, mesh=split, in_specs=placed, out_specs=P(None, KV_TP), check_vma=False
    )
```

```python
import functools

import jax
import jax.numpy as jnp
from jax import lax
from jax.experimental import pallas as pl
from jax.experimental.pallas import tpu as pltpu
from jax.sharding import Mesh
from jax.sharding import PartitionSpec as P

D = 4096
DH = 64
LANES = 128
KV = ("kv_0", "kv_1")
KV_TP = ("kv_0", "kv_1", "tp")
EPSILON = 1e-05
EMPTY_SCORE = -1e30
F32 = jnp.float32
BF16 = jnp.bfloat16

VMEM = pl.BlockSpec(memory_space=pltpu.VMEM)
SMEM = pl.BlockSpec(memory_space=pltpu.SMEM)
ANY = pl.BlockSpec(memory_space=pl.ANY)


def kernel(body, outs, specs, scratch=(), last=False, flops=None):
    return pl.pallas_call(
        body,
        out_shape=[
            jax.ShapeDtypeStruct(shape, dtype) if last else pltpu.VMEM(shape, dtype)
            for shape, dtype in outs
        ],
        in_specs=specs,
        out_specs=[VMEM] * len(outs),
        scratch_shapes=scratch,
        cost_estimate=flops
        and pl.CostEstimate(flops=flops, bytes_accessed=flops // 100, transcendentals=0),
        compiler_params=pltpu.CompilerParams(vmem_limit_bytes=8 * 2**20),
    )


def exchanged(pieces, axis):
    return lax.all_to_all(pieces, axis, 0, 0, tiled=True)


def kv_index():
    return lax.axis_index("kv_0") * lax.axis_size("kv_1") + lax.axis_index("kv_1")


def iota(shape, dim):
    return lax.broadcasted_iota(jnp.int32, shape, dim)


def rounded(x):
    return x.astype(BF16).astype(F32)


def in_pieces(value, count):
    pieces = []
    for _ in range(count):
        piece = rounded(value)
        pieces.append(piece)
        value = value - piece
    return pieces


def diagonal(rows, turn):
    return iota((rows, LANES), 1) == iota((rows, LANES), 0) + rows * turn


def across(left, right, sides):
    return lax.dot_general(left, right, (sides, ((), ())), preferred_element_type=F32)


LAST = ((1,), (1,))
FIRST = ((0,), (0,))


def as_row(columns):
    rows = columns[-1].shape[0]
    tile = jnp.zeros((rows, LANES), F32)
    for turn, column in enumerate(columns):
        if column is None:
            continue
        tile = jnp.where(diagonal(rows, turn), column, tile)
    return jnp.sum(tile, axis=0, keepdims=True)


def as_column(row, rows, turns):
    mask = diagonal(rows, turns[0])
    for turn in turns[1:]:
        mask = mask | diagonal(rows, turn)
    return jnp.sum(jnp.where(mask, row, 0.0), axis=1, keepdims=True)


def summed(ref, start, size):
    total = ref[0, pl.ds(start, size)].astype(F32)
    for k in range(1, ref.shape[0]):
        total = total + ref[k, pl.ds(start, size)].astype(F32)
    return total


def tiles_of(block):
    return [block[4 * t : 4 * t + 4] for t in range(block.shape[0] // 4)]


def put(out, k, tiles):
    for t, tile in enumerate(tiles):
        out[k, t] = tile


def tiles_summed(ref, start, count):
    tiles = []
    for t in range(start, start + count):
        total = ref[0, t].astype(F32)
        for k in range(1, ref.shape[0]):
            total = total + ref[k, t].astype(F32)
        tiles.append(total)
    return tiles[0] if count == 1 else jnp.concatenate(tiles, axis=0)


def k_start(turned_hbm, gain_hbm, out, turned, gain, sem):
    pairs = ((turned_hbm, turned), (gain_hbm, gain))
    copies = [pltpu.make_async_copy(a, b, sem.at[k]) for k, (a, b) in enumerate(pairs)]
    for copy in copies:
        copy.start()
    for copy in copies:
        copy.wait()
    own, rows = turned.shape
    column = jnp.sum(jnp.where(diagonal(own, 0)[:, :own], gain[...], 0.0), axis=1, keepdims=True)
    tile = turned[...].astype(F32)
    pieces = [jnp.broadcast_to(piece, (own, rows)) for piece in in_pieces(column, 3)]
    lane = iota((own, rows), 1)
    extra = jnp.where(lane == 0, pieces[0], jnp.where(lane == 1, pieces[1], pieces[2]))
    half = own // 2
    pad = jnp.zeros((half, LANES - 4 * rows), F32)
    sides = [tile[:half], extra[:half], tile[half:], extra[half:], pad]
    tile = jnp.concatenate(sides, axis=1).astype(BF16)
    for k in range(out.shape[0]):
        out[k] = tile


def k_project(recv, w_query, w_key, w_value, w_forget, w_out, bias, out, x_out, gain_out, new_rows):
    width = x_out.shape[1]
    rows = new_rows.shape[0]
    sent = recv.shape[0]
    source = iota((sent, width), 0)
    target = 2 * source - source % 4
    place = iota((sent, width), 1)
    both = jnp.zeros((2 * rows, width), F32)
    for side in range(2):
        spread = jnp.where(place == target + 4 * side, 1.0, 0.0).astype(BF16)
        part = recv[:, 2 * rows * side : 2 * rows * (side + 1)]
        both = both + across(part, spread, FIRST)
    x = both[:rows]
    x_out[...] = x
    gain = both[rows : rows + 1] + both[rows + 1 : rows + 2] + both[rows + 2 : rows + 3]
    gain_out[...] = jnp.broadcast_to(gain, gain_out.shape)
    xb = x.astype(BF16)
    row = iota((8, LANES), 0)
    sums = across(jnp.ones((8, LANES), BF16), w_out[...], LAST)
    mine = iota(bias.shape, 1) == lax.axis_index("tp")
    once = jnp.where(kv_index() == 0, 1.0, 0.0)
    own_bias = jnp.sum(jnp.where(mine, bias[...], 0.0), axis=1, keepdims=True) * once
    query = jnp.dot(xb, w_query[...], preferred_element_type=F32)
    new_rows[:, :DH] = across(xb, w_key[...], LAST)
    new_rows[:, DH:] = across(xb, w_value[...], LAST)
    start = pl.multiple_of(kv_index() * width, width)
    forget = across(xb, w_forget[:, pl.ds(start, width)], LAST)
    token_col = jnp.sum(x, axis=1, keepdims=True)
    mine = iota(forget.shape, 1) == lax.axis_index("tp")
    forget_col = jnp.sum(jnp.where(mine, forget, 0.0), axis=1, keepdims=True)
    forget_col = forget_col + own_bias
    small = as_row([*in_pieces(forget_col, 2), *in_pieces(token_col, 2)])
    tail = jnp.where(row == 1, small, 0.0)
    tail = jnp.where(row == 2, sums[:, :LANES], tail)
    tail = jnp.where(row == 3, sums[:, LANES:], tail)
    tiles = tiles_of(query[:, :LANES].astype(BF16)) + tiles_of(query[:, LANES:].astype(BF16))
    for b in range(rows):
        own_tail = jnp.where(row == 0, new_rows[pl.ds(b, 1), :], tail)[:4].astype(BF16)
        for k in range(b, out.shape[0], rows):
            put(out, k, [*tiles, own_tail])


def k_prepare(lengths, cache, gate, keys_o, values_o, gate_o, cache_v, gate_v, sem, gate_sem):
    rows, positions = cache.shape[:2]
    copies = [pltpu.make_async_copy(cache.at[b], cache_v.at[b], sem.at[b]) for b in range(rows)]
    gates = pltpu.make_async_copy(gate, gate_v, gate_sem)
    gates.start()
    for copy in copies:
        copy.start()
    gates.wait()
    place = kv_index() * positions + iota((8, positions), 1)
    first = iota((8, positions), 0) < 4
    for m in range(rows // 2):
        one = jnp.where(place < lengths[2 * m], gate_v[2 * m], EMPTY_SCORE)
        two = jnp.where(place < lengths[2 * m + 1], gate_v[2 * m + 1], EMPTY_SCORE)
        gate_o[m // 2, pl.ds(8 * (m % 2), 8), :] = jnp.where(first, one, two)
    for b in range(rows):
        copies[b].wait()
        keys_o[b // 4, pl.ds(DH * (b % 4), DH), :] = cache_v[b].T[:DH]
        if b % 2:
            values_o[b // 4, :, pl.ds(LANES * (b % 4 // 2), LANES)] = jnp.concatenate(
                [cache_v[b - 1][:, DH:], cache_v[b][:, DH:]], axis=1
            )


def k_attend(recv, keys, values, gate, out, tok_out, sums_out, qs, os):
    rows = 4 * keys.shape[0]
    heads = 4
    scale = DH**-0.5
    left = rounded(tiles_summed(recv, 0, rows // 4))
    right = rounded(tiles_summed(recv, rows // 4, rows // 4))
    tail = tiles_summed(recv, rows // 2, 1)
    new_row = rounded(tail[0:1])
    small = tail[1:2]
    sums_out[...] = tail[2:4]
    tok_out[...] = jnp.broadcast_to(as_column(small, rows, (2, 3)), tok_out.shape)
    even = iota((rows, LANES), 0) % 2 == 0
    low = iota((rows, LANES), 1) < DH
    keep = even == low
    left_turned = pltpu.roll(left, DH, 1)
    right_turned = pltpu.roll(right, DH, 1)
    placed = (
        jnp.where(even, left, left_turned),
        jnp.where(even, left_turned, left),
        jnp.where(even, right, right_turned),
        jnp.where(even, right_turned, right),
    )
    for h, block in enumerate(placed):
        qs[pl.ds(h, rows, stride=heads), :] = jnp.where(keep, block, 0.0)
    all_rows = rows * heads
    owner = iota((all_rows, LANES), 0) // heads
    lane = iota((all_rows, LANES), 1)
    fetched = jnp.where((lane == owner) | (lane == owner + rows), small, 0.0)
    fetched = jnp.sum(fetched, axis=1, keepdims=True)
    new_gate = jnp.minimum(fetched, 0.0) - jnp.log(1.0 + jnp.exp(-jnp.abs(fetched)))
    lane = iota((1, LANES), 1)
    new_turned = pltpu.roll(jnp.broadcast_to(new_row, (8, LANES)), DH, 1)[0:1]
    new_key = jnp.where(lane < DH, new_row, new_turned)
    new_value = jnp.where(lane < DH, new_turned, new_row)
    own = jnp.sum(qs[...] * new_key, axis=1, keepdims=True) * scale
    mine = iota((all_rows, 1), 0) // heads == kv_index()
    own = jnp.where(mine, own, EMPTY_SCORE)
    lane = iota((16, LANES), 1)
    spot = jnp.where(iota((16, LANES), 0) % 8 < heads, DH, 0)
    upper = iota((16, LANES), 0) < 8
    for m in range(rows // 4):
        at = slice(16 * m, 16 * m + 16)
        query = qs[pl.ds(16 * m, 16), :] * scale
        query = [jnp.where(upper, query, 0.0), jnp.where(upper, 0.0, query)]
        query = jnp.concatenate(query, axis=1).astype(BF16)
        scores = jnp.dot(query, keys[m], preferred_element_type=F32)
        scores = scores + (gate[m] + new_gate[at])
        top = jnp.maximum(jnp.max(scores, axis=1, keepdims=True), own[at])
        top = jnp.maximum(top, 0.1 * EMPTY_SCORE)
        weights = jnp.exp(scores - top)
        own_weight = jnp.exp(own[at] - top)
        total = jnp.sum(weights, axis=1, keepdims=True) + own_weight
        value = jnp.dot(weights.astype(BF16), values[m], preferred_element_type=F32)
        value = jnp.where(upper, value[:, :LANES], value[:, LANES:])
        value = value + rounded(own_weight) * new_value
        spare = jnp.where(lane == spot, top, jnp.where(lane == spot + 1, total, value))
        os[pl.ds(16 * m, 16), :] = spare
    blocks = [os[pl.ds(h, rows, stride=heads), :] for h in range(heads)]
    turned = [pltpu.roll(block, DH, 1) for block in blocks]
    firsts = [jnp.where(even, block, turn) for block, turn in zip(blocks, turned)]
    seconds = [jnp.where(even, turn, block) for block, turn in zip(blocks, turned)]
    low_out = jnp.where(low, firsts[0], seconds[1]).astype(BF16)
    high_out = jnp.where(low, firsts[2], seconds[3]).astype(BF16)
    lane = iota((rows, LANES), 1)
    stats = jnp.zeros((rows, LANES), F32)
    for h in range(heads):
        pieces = [*in_pieces(seconds[h][:, 0:1], 3), *in_pieces(seconds[h][:, 1:2], 2)]
        for k, piece in enumerate(pieces):
            stats = jnp.where(lane == 8 * h + k, piece, stats)
    packed = stats[:4]
    for g in range(1, rows // 4):
        packed = packed + pltpu.roll(stats, 32 * g, 1)[4 * g : 4 * g + 4]
    tiles = [*tiles_of(low_out), *tiles_of(high_out), packed.astype(BF16)]
    for k in range(out.shape[0]):
        put(out, k, tiles)


def k_combine(recv, sums, w_out, out):
    devices = recv.shape[0]
    tiles = (recv.shape[1] - 1) // 2
    rows = 4 * tiles
    heads = 4 * DH
    source = iota((LANES, 2 * heads), 0) % 32
    column = iota((LANES, 2 * heads), 1)
    first = 8 * ((column % heads) // DH)
    is_top = column < heads
    begin = jnp.where(is_top, first, first + 3)
    end = jnp.where(is_top, first + 3, first + 5)
    spread = jnp.where((source >= begin) & (source < end), 1.0, 0.0).astype(BF16)
    stats = recv[:, 2 * tiles].astype(F32)
    stats = jnp.concatenate([stats, stats], axis=1)
    group = iota(stats.shape, 2) // 32 - iota(stats.shape, 1) // 4
    blocks = []
    for half in range(2):
        mine = jnp.where(group == 2 * half, stats, 0.0).astype(BF16).reshape(devices * 8, LANES)
        wide = jnp.dot(mine, spread, preferred_element_type=F32).reshape(devices, 8, 2 * heads)
        tops = wide[:, :, :heads]
        totals = wide[:, :, heads:]
        scales = jnp.exp(tops - jnp.max(tops, axis=0, keepdims=True))
        total = jnp.sum(totals * scales, axis=0)
        sides = []
        for side in range(2):
            at = tiles * side + 2 * half
            part = [recv[:, at + t].astype(F32) for t in range(2)]
            part = jnp.concatenate(part, axis=1)
            sides.append(jnp.sum(part * scales[:, :, side * LANES : (side + 1) * LANES], axis=0))
        blocks.append(jnp.concatenate(sides, axis=1) / total)
    attended = jnp.concatenate(blocks, axis=0).astype(BF16)
    wide = attended.astype(F32)
    mean = wide[:, :LANES] * sums[0:1, :] + wide[:, LANES:] * sums[1:2, :]
    mean = jnp.sum(mean, axis=1, keepdims=True) / D
    attn_part = jnp.dot(attended, w_out[...], preferred_element_type=F32)
    attn_part = (attn_part - mean).astype(BF16)
    for k in range(out.shape[0]):
        out[k] = attn_part


def k_expand(recv, x, tok, gain, w_gate, w_up, out, scaled_out, tile):
    rows = x.shape[0]
    centred = x[...] - tok[:, 0:1] / D + summed(recv, 0, rows)
    scaled = centred * gain[0:1, :]
    scaled_out[...] = scaled
    squares = in_pieces(jnp.sum(centred * centred, axis=1, keepdims=True), 2)
    squares = as_row([None] * 6 + squares)
    scaled = scaled.astype(BF16)
    pieces = out.shape[0] // rows
    size = w_gate.shape[0] // pieces
    stride = 6 * pieces
    pad = jnp.zeros((rows, 3 * LANES - size), F32)
    for k, weight in enumerate((w_gate, w_up)):
        part = across(scaled, weight[...], LAST)
        for h in range(pieces):
            share = jnp.concatenate([part[:, h * size : (h + 1) * size], pad], axis=1)
            for t in range(3):
                block = share[:, t * LANES : (t + 1) * LANES]
                if t == 2 and k == 0:
                    block = block + squares
                tile[pl.ds(6 * h + 3 * k + t, rows, stride=stride), :] = block
    for k in range(out.shape[0]):
        for t in range(3):
            out[k, t] = tile[pl.ds(6 * k + 2 * t, 2), :].astype(BF16)


def k_hidden(recv, scaled, out, mid_out):
    rows = scaled.shape[0]
    total = jnp.concatenate(
        [jnp.sum(recv[:, t].astype(F32), axis=0) for t in range(recv.shape[1])], axis=0
    )
    spread = as_column(total[2:3], rows, (6, 7)) / D
    shrink = lax.rsqrt(spread + EPSILON)
    mid_out[...] = rounded(scaled[...] * shrink)
    mine = iota((rows, 1), 0) == kv_index() // (out.shape[0] // rows)
    own = jnp.sum(jnp.where(mine, shrink, 0.0), axis=0, keepdims=True)
    total = total * own
    gate, up = total[:3], total[3:6]
    hidden = gate / (1.0 + jnp.exp(-gate)) * up
    hidden = jnp.concatenate([hidden, jnp.zeros((1, LANES), F32)], axis=0).astype(BF16)
    for k in range(out.shape[0]):
        out[k] = hidden


def k_shrink(recv, w_down, out, tile):
    rows = out.shape[1]
    pieces = recv.shape[0] // rows
    for k in range(recv.shape[0]):
        tile[pl.ds(4 * k, 4), :] = recv[k].astype(F32)
    part = jnp.zeros((rows, LANES), F32)
    share = w_down.shape[0] // pieces
    for t in range(3 * pieces):
        at = 4 * (t // 3) + t % 3
        start = share * (t // 3) + LANES * (t % 3)
        size = min(LANES, share - LANES * (t % 3))
        hidden = tile[pl.ds(at, rows, stride=4 * pieces), :][:, :size].astype(BF16)
        part = part + jnp.dot(hidden, w_down[pl.ds(start, size), :], preferred_element_type=F32)
    part = part.astype(BF16)
    for k in range(out.shape[0]):
        out[k] = part


def k_sums(recv, mid, out, mix_out):
    rows, width = mid.shape
    mixture = mid[...] + summed(recv, 0, rows)
    mix_out[...] = mixture
    centre = jnp.sum(mixture, axis=1, keepdims=True) / width
    square = jnp.sum((mixture - centre) ** 2, axis=1, keepdims=True)
    message = as_row([centre, square])
    for k in range(out.shape[0]):
        out[k] = message


def k_finish(recv, mix, gain, out, turned):
    rows, width = mix.shape
    devices = recv.shape[0]
    total = recv[0]
    for k in range(1, devices):
        total = total + recv[k]
    middle = total / devices
    spread = (recv[0] - middle) ** 2
    for k in range(1, devices):
        spread = spread + (recv[k] - middle) ** 2
    square = jnp.where(iota((1, LANES), 1) < rows, spread * width, total)
    centre = as_column(middle, rows, (0,))
    shrink = lax.rsqrt(as_column(square, rows, (0, 1)) / D + EPSILON)
    own = out.shape[0]
    scaled = ((mix[...] - centre) * shrink).T
    at = pl.multiple_of(lax.axis_index("tp") * own, own)
    turned[...] = scaled
    gain_col = jnp.sum(jnp.where(diagonal(own, 0)[:, :own], gain[...], 0.0), axis=1, keepdims=True)
    out[...] = (turned[pl.ds(at, own), :] * gain_col).astype(BF16)


def on_device(
    tokens,
    live_lengths,
    kv_cache,
    gate_sums,
    w_query,
    w_key,
    w_value,
    w_forget,
    forget_bias,
    w_out,
    first_gain,
    w_gate,
    w_up,
    w_down,
    second_gain,
):
    rows, own = tokens.shape
    kv, tp = lax.axis_size(KV), lax.axis_size("tp")
    width = own * tp
    block = ((rows, LANES), F32)
    in_hbm = functools.partial(pltpu.with_memory_space_constraint, memory_space=pltpu.HBM)
    (message,) = kernel(
        k_start,
        [((tp, own // 2, LANES), BF16)],
        [ANY] * 2,
        [
            pltpu.VMEM((own, rows), BF16),
            pltpu.VMEM((1, own), F32),
            pltpu.SemaphoreType.DMA((2,)),
        ],
        flops=10**11,
    )(in_hbm(tokens.T), in_hbm(first_gain[None]))
    recv = exchanged(message, "tp").reshape(width // 2, LANES)
    message, x, gain = kernel(
        k_project,
        [((kv, rows // 2 + 1, 4, LANES), BF16), block, ((8, LANES), F32)],
        [VMEM] * 7,
        [pltpu.VMEM((rows, LANES), F32)],
    )(
        recv,
        w_query,
        w_key.T,
        w_value.T,
        w_forget.T,
        w_out,
        forget_bias[None],
    )
    recv = exchanged(message, KV)
    positions = kv_cache.shape[1]
    keys, values, gate_sums = kernel(
        k_prepare,
        [
            ((rows // 4, 4 * DH, positions), BF16),
            ((rows // 4, positions, 4 * DH), BF16),
            ((rows // 4, 16, positions), F32),
        ],
        [SMEM, ANY, ANY],
        [
            pltpu.VMEM(kv_cache.shape, BF16),
            pltpu.VMEM(gate_sums.shape, F32),
            pltpu.SemaphoreType.DMA((rows,)),
            pltpu.SemaphoreType.DMA,
        ],
    )(live_lengths, in_hbm(kv_cache), in_hbm(gate_sums))
    message, tok, sums = kernel(
        k_attend,
        [((kv, rows // 2 + 1, 4, LANES), BF16), block, ((2, LANES), F32)],
        [VMEM] * 4,
        [pltpu.VMEM((4 * rows, LANES), F32), pltpu.VMEM((4 * rows, LANES), F32)],
    )(recv, keys, values, gate_sums)
    (message,) = kernel(k_combine, [((tp, rows, width), BF16)], [VMEM] * 3)(
        exchanged(message, KV), sums, w_out
    )
    message, scaled = kernel(
        k_expand,
        [((kv, 3, 2, LANES), BF16), block],
        [VMEM] * 6,
        [pltpu.VMEM((6 * kv, LANES), F32)],
    )(exchanged(message, "tp"), x, tok, gain, w_gate.T, w_up.T)
    message, mid = kernel(k_hidden, [((kv, 4, LANES), BF16), block], [VMEM] * 2)(
        exchanged(message, KV), scaled
    )
    (message,) = kernel(
        k_shrink, [((tp, rows, width), BF16)], [VMEM] * 2, [pltpu.VMEM((4 * kv, LANES), F32)]
    )(exchanged(message, KV), w_down)
    message, mix = kernel(k_sums, [((kv, 1, LANES), F32), block], [VMEM] * 2)(
        exchanged(message, "tp"), mid
    )
    (out,) = kernel(
        k_finish, [((own, rows), BF16)], [VMEM] * 3, [pltpu.VMEM((width, rows), F32)], last=True
    )(exchanged(message, KV), mix, second_gain[None])
    return out.T


def solution(mesh):
    split = Mesh(mesh.devices.reshape(8, 4, mesh.shape["tp"]), ("kv_0", "kv_1", "tp"))
    placed = (
        P(None, KV_TP),
        P(),
        P(None, KV, "tp"),
        P(None, "tp", KV),
        P(KV, "tp"),
        P(KV, "tp"),
        P(KV, "tp"),
        P(),
        P(),
        P("tp", KV),
        P(KV_TP),
        P(KV, "tp"),
        P(KV, "tp"),
        P("tp", KV),
        P(KV_TP),
    )
    return jax.shard_map(
        on_device, mesh=split, in_specs=placed, out_specs=P(None, KV_TP), check_vma=False
    )
```

```python
import functools

import jax
import jax.numpy as jnp
from jax import lax
from jax.experimental import pallas as pl
from jax.experimental.pallas import tpu as pltpu
from jax.sharding import Mesh
from jax.sharding import PartitionSpec as P


D = 4096
DH = 64
LANES = 128
SPARE = 96
KV = ("kv_0", "kv_1", "kv_2")
KV_TP = ("kv_0", "kv_1", "kv_2", "tp")
EPSILON = 1e-05
EMPTY_SCORE = -1e30
F32 = jnp.float32
BF16 = jnp.bfloat16

VMEM = pl.BlockSpec(memory_space=pltpu.VMEM)
SMEM = pl.BlockSpec(memory_space=pltpu.SMEM)
ANY = pl.BlockSpec(memory_space=pl.ANY)


def kernel(body, outs, specs, scratch=(), last=False, flops=None):
    return pl.pallas_call(
        body,
        out_shape=[
            jax.ShapeDtypeStruct(shape, dtype) if last else pltpu.VMEM(shape, dtype)
            for shape, dtype in outs
        ],
        in_specs=specs,
        out_specs=[VMEM] * len(outs),
        scratch_shapes=scratch,
        cost_estimate=flops
        and pl.CostEstimate(flops=flops, bytes_accessed=flops // 100, transcendentals=0),
        compiler_params=pltpu.CompilerParams(vmem_limit_bytes=8 * 2**20),
    )


def exchanged(pieces, axis):
    return lax.all_to_all(pieces, axis, 0, 0, tiled=True)


def kv_index():
    index = lax.axis_index(KV[0])
    for axis in KV[1:]:
        index = index * lax.axis_size(axis) + lax.axis_index(axis)
    return index


def iota(shape, dim):
    return lax.broadcasted_iota(jnp.int32, shape, dim)


def rounded(x):
    return x.astype(BF16).astype(F32)


def in_pieces(value, count):
    pieces = []
    for _ in range(count):
        piece = rounded(value)
        pieces.append(piece)
        value = value - piece
    return pieces


def diagonal(rows, turn):
    return iota((rows, LANES), 1) == iota((rows, LANES), 0) + rows * turn


def across(left, right, sides):
    return lax.dot_general(left, right, (sides, ((), ())), preferred_element_type=F32)


LAST = ((1,), (1,))
FIRST = ((0,), (0,))


def as_row(columns):
    rows = columns[0].shape[0]
    tile = jnp.zeros((rows, LANES), F32)
    for turn, column in enumerate(columns):
        tile = jnp.where(diagonal(rows, turn), column, tile)
    return jnp.sum(tile, axis=0, keepdims=True)


def as_column(row, rows, turns):
    mask = diagonal(rows, turns[0])
    for turn in turns[1:]:
        mask = mask | diagonal(rows, turn)
    return jnp.sum(jnp.where(mask, row, 0.0), axis=1, keepdims=True)


def summed(ref, start, size):
    total = ref[0, pl.ds(start, size)].astype(F32)
    for k in range(1, ref.shape[0]):
        total = total + ref[k, pl.ds(start, size)].astype(F32)
    return total


def tiles_of(block):
    return [block[4 * t : 4 * t + 4] for t in range(block.shape[0] // 4)]


def put(out, k, tiles):
    for t, tile in enumerate(tiles):
        out[k, t] = tile


def tiles_summed(ref, start, count):
    tiles = []
    for t in range(start, start + count):
        total = ref[0, t].astype(F32)
        for k in range(1, ref.shape[0]):
            total = total + ref[k, t].astype(F32)
        tiles.append(total)
    return tiles[0] if count == 1 else jnp.concatenate(tiles, axis=0)


def k_start(turned_hbm, gain_hbm, out, turned, gain, sem):
    pairs = ((turned_hbm, turned), (gain_hbm, gain))
    copies = [pltpu.make_async_copy(a, b, sem.at[k]) for k, (a, b) in enumerate(pairs)]
    for copy in copies:
        copy.start()
    for copy in copies:
        copy.wait()
    own, rows = turned.shape
    column = jnp.sum(jnp.where(diagonal(own, 0)[:, :own], gain[...], 0.0), axis=1, keepdims=True)
    pad = jnp.zeros((own, LANES - rows), F32)
    tile = jnp.concatenate([turned[...].astype(F32), pad], axis=1)
    for k, piece in enumerate(in_pieces(column, 3)):
        tile = jnp.where(iota(tile.shape, 1) == rows + k, piece, tile)
    tile = tile.astype(BF16)
    for k in range(out.shape[0]):
        out[k] = tile


def k_project(recv, w_query, w_key, w_value, w_forget, w_out, bias, out, x_out, gain_out, new_rows):
    width = recv.shape[0]
    same = jnp.where(iota((width, width), 0) == iota((width, width), 1), 1.0, 0.0).astype(BF16)
    rows = new_rows.shape[0]
    both = across(recv[:, : 2 * rows], same, FIRST)
    x = both[:rows]
    x_out[...] = x
    gain = both[rows : rows + 1] + both[rows + 1 : rows + 2] + both[rows + 2 : rows + 3]
    gain_out[...] = jnp.broadcast_to(gain, gain_out.shape)
    xb = x.astype(BF16)
    row = iota((8, LANES), 0)
    sums = across(jnp.ones((8, LANES), BF16), w_out[...], LAST)
    mine = iota(bias.shape, 1) == lax.axis_index("tp")
    once = jnp.where(kv_index() == 0, 1.0, 0.0)
    own_bias = jnp.sum(jnp.where(mine, bias[...], 0.0), axis=1, keepdims=True) * once
    query = jnp.dot(xb, w_query[...], preferred_element_type=F32)
    new_rows[:, :DH] = across(xb, w_key[...], LAST)
    new_rows[:, DH:] = across(xb, w_value[...], LAST)
    start = pl.multiple_of(kv_index() * width, width)
    forget = across(xb, w_forget[:, pl.ds(start, width)], LAST)
    token_col = jnp.sum(x, axis=1, keepdims=True)
    mine = iota(forget.shape, 1) == lax.axis_index("tp")
    forget_col = jnp.sum(jnp.where(mine, forget, 0.0), axis=1, keepdims=True)
    forget_col = forget_col + own_bias
    small = as_row([*in_pieces(forget_col, 2), *in_pieces(token_col, 2)])
    tail = jnp.where(row == 1, small, 0.0)
    tail = jnp.where(row == 2, sums[:, :LANES], tail)
    tail = jnp.where(row == 3, sums[:, LANES:], tail)
    tiles = tiles_of(query[:, :LANES].astype(BF16)) + tiles_of(query[:, LANES:].astype(BF16))
    for b in range(rows):
        own_tail = jnp.where(row == 0, new_rows[pl.ds(b, 1), :], tail)[:4].astype(BF16)
        for k in range(b, out.shape[0], rows):
            put(out, k, [*tiles, own_tail])


def k_prepare(lengths, cache, gate, keys_o, values_o, gate_o, cache_v, gate_v, sem, gate_sem):
    rows, positions = cache.shape[:2]
    copies = [pltpu.make_async_copy(cache.at[b], cache_v.at[b], sem.at[b]) for b in range(rows)]
    gates = pltpu.make_async_copy(gate, gate_v, gate_sem)
    gates.start()
    for copy in copies:
        copy.start()
    gates.wait()
    place = kv_index() * positions + iota((8, positions), 1)
    first = iota((8, positions), 0) < 4
    for m in range(rows // 2):
        one = jnp.where(place < lengths[2 * m], gate_v[2 * m], EMPTY_SCORE)
        two = jnp.where(place < lengths[2 * m + 1], gate_v[2 * m + 1], EMPTY_SCORE)
        gate_o[m // 2, pl.ds(8 * (m % 2), 8), :] = jnp.where(first, one, two)
    for b in range(rows):
        copies[b].wait()
        keys_o[b // 4, pl.ds(DH * (b % 4), DH), :] = cache_v[b].T[:DH]
        if b % 2:
            values_o[b // 4, :, pl.ds(LANES * (b % 4 // 2), LANES)] = jnp.concatenate(
                [cache_v[b - 1][:, DH:], cache_v[b][:, DH:]], axis=1
            )


def k_attend(recv, keys, values, gate, arrived, out, tok_out, sums_out, qs, os):
    rows = 4 * keys.shape[0]
    heads = 4
    scale = DH**-0.5
    left = rounded(tiles_summed(recv, 0, rows // 4))
    right = rounded(tiles_summed(recv, rows // 4, rows // 4))
    tail = tiles_summed(recv, rows // 2, 1)
    new_row = rounded(tail[0:1])
    small = tail[1:2]
    sums_out[...] = tail[2:4]
    tok_out[...] = jnp.broadcast_to(as_column(small, rows, (2, 3)), tok_out.shape)
    even = iota((rows, LANES), 0) % 2 == 0
    low = iota((rows, LANES), 1) < DH
    keep = even == low
    left_turned = pltpu.roll(left, DH, 1)
    right_turned = pltpu.roll(right, DH, 1)
    placed = (
        jnp.where(even, left, left_turned),
        jnp.where(even, left_turned, left),
        jnp.where(even, right, right_turned),
        jnp.where(even, right_turned, right),
    )
    for h, block in enumerate(placed):
        qs[pl.ds(h, rows, stride=heads), :] = jnp.where(keep, block, 0.0)
    all_rows = rows * heads
    owner = iota((all_rows, LANES), 0) // heads
    lane = iota((all_rows, LANES), 1)
    fetched = jnp.where((lane == owner) | (lane == owner + rows), small, 0.0)
    fetched = jnp.sum(fetched, axis=1, keepdims=True)
    new_gate = jnp.minimum(fetched, 0.0) - jnp.log(1.0 + jnp.exp(-jnp.abs(fetched)))
    lane = iota((1, LANES), 1)
    new_turned = pltpu.roll(jnp.broadcast_to(new_row, (8, LANES)), DH, 1)[0:1]
    new_key = jnp.where(lane < DH, new_row, new_turned)
    new_value = jnp.where(lane < DH, new_turned, new_row)
    own = jnp.sum(qs[...] * new_key, axis=1, keepdims=True) * scale
    mine = iota((all_rows, 1), 0) // heads == kv_index()
    own = jnp.where(mine, own, EMPTY_SCORE)
    lane = iota((16, LANES), 1)
    spot = jnp.where(iota((16, LANES), 0) % 8 < heads, DH, 0)
    upper = iota((16, LANES), 0) < 8
    for m in range(rows // 4):
        at = slice(16 * m, 16 * m + 16)
        query = qs[pl.ds(16 * m, 16), :] * scale
        query = [jnp.where(upper, query, 0.0), jnp.where(upper, 0.0, query)]
        query = jnp.concatenate(query, axis=1).astype(BF16)
        scores = jnp.dot(query, keys[m], preferred_element_type=F32)
        scores = scores + (gate[m] + new_gate[at])
        top = jnp.maximum(jnp.max(scores, axis=1, keepdims=True), own[at])
        top = jnp.maximum(top, 0.1 * EMPTY_SCORE)
        weights = jnp.exp(scores - top)
        own_weight = jnp.exp(own[at] - top)
        total = jnp.sum(weights, axis=1, keepdims=True) + own_weight
        value = jnp.dot(weights.astype(BF16), values[m], preferred_element_type=F32)
        value = jnp.where(upper, value[:, :LANES], value[:, LANES:])
        value = value + rounded(own_weight) * new_value
        spare = jnp.where(lane == spot, top, jnp.where(lane == spot + 1, total, value))
        os[pl.ds(16 * m, 16), :] = spare
    blocks = [os[pl.ds(h, rows, stride=heads), :] for h in range(heads)]
    turned = [pltpu.roll(block, DH, 1) for block in blocks]
    firsts = [jnp.where(even, block, turn) for block, turn in zip(blocks, turned)]
    seconds = [jnp.where(even, turn, block) for block, turn in zip(blocks, turned)]
    low_out = jnp.where(low, firsts[0], seconds[1]).astype(BF16)
    high_out = jnp.where(low, firsts[2], seconds[3]).astype(BF16)
    lane = iota((rows, LANES), 1)
    stats = jnp.zeros((rows, LANES), F32)
    for h in range(heads):
        pieces = [*in_pieces(seconds[h][:, 0:1], 3), *in_pieces(seconds[h][:, 1:2], 2)]
        for k, piece in enumerate(pieces):
            stats = jnp.where(lane == 8 * h + k, piece, stats)
    packed = stats[:4]
    for g in range(1, rows // 4):
        packed = packed + pltpu.roll(stats, 32 * g, 1)[4 * g : 4 * g + 4]
    tiles = [*tiles_of(low_out), *tiles_of(high_out), packed.astype(BF16)]
    for k in range(out.shape[0]):
        put(out, k, tiles)


def k_combine(recv, sums, w_out, out):
    devices = recv.shape[0]
    tiles = (recv.shape[1] - 1) // 2
    heads = 4 * DH
    source = iota((LANES, 2 * heads), 0) % 32
    column = iota((LANES, 2 * heads), 1)
    first = 8 * ((column % heads) // DH)
    is_top = column < heads
    begin = jnp.where(is_top, first, first + 3)
    end = jnp.where(is_top, first + 3, first + 5)
    spread = jnp.where((source >= begin) & (source < end), 1.0, 0.0).astype(BF16)
    stats = recv[:, 2 * tiles].astype(F32)
    stats = jnp.concatenate([stats, stats], axis=1)
    group = iota(stats.shape, 2) // 32 - iota(stats.shape, 1) // 4
    blocks = []
    for half in range(2):
        mine = jnp.where(group == 2 * half, stats, 0.0).astype(BF16).reshape(devices * 8, LANES)
        wide = jnp.dot(mine, spread, preferred_element_type=F32).reshape(devices, 8, 2 * heads)
        tops = wide[:, :, :heads]
        totals = wide[:, :, heads:]
        scales = jnp.exp(tops - jnp.max(tops, axis=0, keepdims=True))
        total = jnp.sum(totals * scales, axis=0)
        sides = []
        for side in range(2):
            at = tiles * side + 2 * half
            part = [recv[:, at + t].astype(F32) for t in range(2)]
            part = jnp.concatenate(part, axis=1)
            sides.append(jnp.sum(part * scales[:, :, side * LANES : (side + 1) * LANES], axis=0))
        blocks.append(jnp.concatenate(sides, axis=1) / total)
    attended = jnp.concatenate(blocks, axis=0).astype(BF16)
    wide = attended.astype(F32)
    mean = wide[:, :LANES] * sums[0:1, :] + wide[:, LANES:] * sums[1:2, :]
    mean = jnp.sum(mean, axis=1, keepdims=True) / D
    attn_part = jnp.dot(attended, w_out[...], preferred_element_type=F32)
    attn_part = (attn_part - mean).astype(BF16)
    for k in range(out.shape[0]):
        out[k] = attn_part


def k_expand(recv, x, tok, gain, w_gate, w_up, out, scaled_out):
    rows = x.shape[0]
    centred = x[...] - tok[:, 0:1] / D + summed(recv, 0, rows)
    scaled = centred * gain[0:1, :]
    scaled_out[...] = scaled
    squares = in_pieces(jnp.sum(centred * centred, axis=1, keepdims=True), 2)
    scaled = scaled.astype(BF16)
    parts = out.shape[0]
    size = w_gate.shape[0] // parts
    pad = jnp.zeros((rows, 3 * LANES - size), F32)
    lane = iota((rows, LANES), 1)
    for k, weight in enumerate((w_gate, w_up)):
        part = across(scaled, weight[...], LAST)
        for h in range(parts):
            share = jnp.concatenate([part[:, h * size : (h + 1) * size], pad], axis=1)
            for t in range(3):
                block = share[:, t * LANES : (t + 1) * LANES]
                if t == 2 and k == 0:
                    for n, piece in enumerate(squares):
                        block = jnp.where(lane == SPARE + n, piece, block)
                out[h, pl.ds((3 * k + t) * rows, rows)] = block.astype(BF16)


def k_gather(recv, out):
    rows = recv.shape[1] // 6
    lane = iota((rows, LANES), 1)
    for t in range(6):
        block = summed(recv, t * rows, rows)
        if t == 2:
            square = block[:, SPARE : SPARE + 1] + block[:, SPARE + 1 : SPARE + 2]
            for n, piece in enumerate(in_pieces(square, 2)):
                block = jnp.where(lane == SPARE + n, piece, block)
        block = block.astype(BF16)
        for k in range(out.shape[0]):
            out[k, pl.ds(t * rows, rows)] = block


def k_hidden(recv, scaled, w_own, w_other, out, mid_out):
    rows = scaled.shape[0]
    blocks = [summed(recv, t * rows, rows) for t in range(6)]
    spread = (blocks[2][:, SPARE : SPARE + 1] + blocks[2][:, SPARE + 1 : SPARE + 2]) / D
    shrink = lax.rsqrt(spread + EPSILON)
    mid_out[...] = rounded(scaled[...] * shrink)
    side = lax.axis_index("kv_2")
    size = w_own.shape[0] // 2
    copies = out.shape[0] // 2
    parts = [jnp.zeros((rows, LANES), F32)] * 2
    for t in range(3):
        gate = blocks[t] * shrink
        up = blocks[3 + t] * shrink
        width = min(LANES, size - t * LANES)
        hidden = (gate / (1.0 + jnp.exp(-gate)) * up)[:, :width].astype(BF16)
        at = pl.ds(pl.multiple_of(side * size + t * LANES, 16), width)
        for n, weight in enumerate((w_own, w_other)):
            parts[n] = parts[n] + jnp.dot(hidden, weight[at, :], preferred_element_type=F32)
    for n, start in enumerate((side * copies, (1 - side) * copies)):
        part = parts[n].astype(BF16)
        for k in range(copies):
            out[start + k] = part


def k_sums(recv, mid, out, mix_out):
    rows, width = mid.shape
    mixture = mid[...] + summed(recv, 0, rows)
    mix_out[...] = mixture
    centre = jnp.sum(mixture, axis=1, keepdims=True) / width
    square = jnp.sum((mixture - centre) ** 2, axis=1, keepdims=True)
    message = as_row([centre, square])
    for k in range(out.shape[0]):
        out[k] = message


def k_finish(recv, mix, gain, out, turned):
    rows, width = mix.shape
    devices = recv.shape[0]
    total = recv[0]
    for k in range(1, devices):
        total = total + recv[k]
    middle = total / devices
    spread = (recv[0] - middle) ** 2
    for k in range(1, devices):
        spread = spread + (recv[k] - middle) ** 2
    square = jnp.where(iota((1, LANES), 1) < rows, spread * width, total)
    centre = as_column(middle, rows, (0,))
    shrink = lax.rsqrt(as_column(square, rows, (0, 1)) / D + EPSILON)
    own = out.shape[0]
    scaled = ((mix[...] - centre) * shrink).T
    at = pl.multiple_of(lax.axis_index("tp") * own, own)
    turned[...] = scaled
    gain_col = jnp.sum(jnp.where(diagonal(own, 0)[:, :own], gain[...], 0.0), axis=1, keepdims=True)
    out[...] = (turned[pl.ds(at, own), :] * gain_col).astype(BF16)


def on_device(
    tokens,
    live_lengths,
    kv_cache,
    gate_sums,
    w_query,
    w_key,
    w_value,
    w_forget,
    forget_bias,
    w_out,
    first_gain,
    w_gate,
    w_up,
    w_down,
    second_gain,
):
    rows, own = tokens.shape
    kv, tp = lax.axis_size(KV), lax.axis_size("tp")
    width = own * tp
    block = ((rows, LANES), F32)
    in_hbm = functools.partial(pltpu.with_memory_space_constraint, memory_space=pltpu.HBM)
    (message,) = kernel(
        k_start,
        [((tp, own, LANES), BF16)],
        [ANY] * 2,
        [
            pltpu.VMEM((own, rows), BF16),
            pltpu.VMEM((1, own), F32),
            pltpu.SemaphoreType.DMA((2,)),
        ],
        flops=10**11,
    )(in_hbm(tokens.T), in_hbm(first_gain[None]))
    recv = exchanged(message, "tp").reshape(width, LANES)
    message, x, gain = kernel(
        k_project,
        [((kv, rows // 2 + 1, 4, LANES), BF16), block, ((8, LANES), F32)],
        [VMEM] * 7,
        [pltpu.VMEM((rows, LANES), F32)],
    )(
        recv,
        w_query,
        w_key.T,
        w_value.T,
        w_forget.T,
        w_out,
        forget_bias[None],
    )
    recv = exchanged(message, KV)
    w_other = lax.ppermute(w_down, "kv_2", [(0, 1), (1, 0)])
    positions = kv_cache.shape[1]
    prepare = kernel(
        k_prepare,
        [
            ((rows // 4, 4 * DH, positions), BF16),
            ((rows // 4, positions, 4 * DH), BF16),
            ((rows // 4, 16, positions), F32),
        ],
        [SMEM, ANY, ANY],
        [
            pltpu.VMEM(kv_cache.shape, BF16),
            pltpu.VMEM(gate_sums.shape, F32),
            pltpu.SemaphoreType.DMA((rows,)),
            pltpu.SemaphoreType.DMA,
        ],
    )
    keys, values, gate_sums = prepare(live_lengths, in_hbm(kv_cache), in_hbm(gate_sums))
    attend = kernel(
        k_attend,
        [((kv, rows // 2 + 1, 4, LANES), BF16), block, ((2, LANES), F32)],
        [VMEM] * 5,
        [pltpu.VMEM((4 * rows, LANES), F32), pltpu.VMEM((4 * rows, LANES), F32)],
    )
    message, tok, sums = attend(recv, keys, values, gate_sums, w_other)
    (message,) = kernel(k_combine, [((tp, rows, width), BF16)], [VMEM] * 3)(
        exchanged(message, KV), sums, w_out
    )
    pair = lax.axis_size("kv_2")
    message, scaled = kernel(
        k_expand, [((pair, 6 * rows, LANES), BF16), block], [VMEM] * 6
    )(exchanged(message, "tp"), x, tok, gain, w_gate.T, w_up.T)
    (message,) = kernel(k_gather, [((kv // pair, 6 * rows, LANES), BF16)], [VMEM])(
        exchanged(message, "kv_2")
    )
    message, mid = kernel(
        k_hidden, [((pair * tp, rows, width), BF16), block], [VMEM] * 4
    )(exchanged(message, ("kv_0", "kv_1")), scaled, w_down, w_other)
    message, mix = kernel(k_sums, [((kv, 1, LANES), F32), block], [VMEM] * 2)(
        exchanged(message, ("kv_2", "tp")), mid
    )
    (out,) = kernel(
        k_finish, [((own, rows), BF16)], [VMEM] * 3, [pltpu.VMEM((width, rows), F32)], last=True
    )(exchanged(message, KV), mix, second_gain[None])
    return out.T


def solution(mesh):
    split = Mesh(mesh.devices.reshape(8, 2, 2, mesh.shape["tp"]), KV_TP)
    placed = (
        P(None, KV_TP),
        P(),
        P(None, KV, "tp"),
        P(None, "tp", KV),
        P(KV, "tp"),
        P(KV, "tp"),
        P(KV, "tp"),
        P(),
        P(),
        P("tp", KV),
        P(KV_TP),
        P(KV, "tp"),
        P(KV, "tp"),
        P("tp", KV),
        P(KV_TP),
    )

    return jax.shard_map(
        on_device, mesh=split, in_specs=placed, out_specs=P(None, KV_TP), check_vma=False
    )
```

```python
import functools

import jax
import jax.numpy as jnp
from jax import lax
from jax.experimental import pallas as pl
from jax.experimental.pallas import tpu as pltpu
from jax.sharding import Mesh
from jax.sharding import PartitionSpec as P

D = 4096
DH = 64
LANES = 128
KV = ("kv_0", "kv_1")
KV_TP = ("kv_0", "kv_1", "tp")
EPSILON = 1e-05
EMPTY_SCORE = -1e30
F32 = jnp.float32
BF16 = jnp.bfloat16

VMEM = pl.BlockSpec(memory_space=pltpu.VMEM)
SMEM = pl.BlockSpec(memory_space=pltpu.SMEM)
ANY = pl.BlockSpec(memory_space=pl.ANY)


def kernel(body, outs, specs, scratch=(), last=False, flops=None):
    return pl.pallas_call(
        body,
        out_shape=[
            jax.ShapeDtypeStruct(shape, dtype) if last else pltpu.VMEM(shape, dtype)
            for shape, dtype in outs
        ],
        in_specs=specs,
        out_specs=[VMEM] * len(outs),
        scratch_shapes=scratch,
        cost_estimate=flops
        and pl.CostEstimate(flops=flops, bytes_accessed=flops // 100, transcendentals=0),
        compiler_params=pltpu.CompilerParams(vmem_limit_bytes=8 * 2**20),
    )


def exchanged(pieces, axis):
    return lax.all_to_all(pieces, axis, 0, 0, tiled=True)


def kv_index():
    return lax.axis_index("kv_0") * lax.axis_size("kv_1") + lax.axis_index("kv_1")


def iota(shape, dim):
    return lax.broadcasted_iota(jnp.int32, shape, dim)


def rounded(x):
    return x.astype(BF16).astype(F32)


def in_pieces(value, count):
    pieces = []
    for _ in range(count):
        piece = rounded(value)
        pieces.append(piece)
        value = value - piece
    return pieces


def diagonal(rows, turn):
    return iota((rows, LANES), 1) == iota((rows, LANES), 0) + rows * turn


def across(left, right, sides):
    return lax.dot_general(left, right, (sides, ((), ())), preferred_element_type=F32)


LAST = ((1,), (1,))
FIRST = ((0,), (0,))


def as_row(columns):
    rows = columns[0].shape[0]
    tile = jnp.zeros((rows, LANES), F32)
    for turn, column in enumerate(columns):
        tile = jnp.where(diagonal(rows, turn), column, tile)
    return jnp.sum(tile, axis=0, keepdims=True)


def as_column(row, rows, turns):
    mask = diagonal(rows, turns[0])
    for turn in turns[1:]:
        mask = mask | diagonal(rows, turn)
    return jnp.sum(jnp.where(mask, row, 0.0), axis=1, keepdims=True)


def summed(ref, start, size):
    total = ref[0, pl.ds(start, size)].astype(F32)
    for k in range(1, ref.shape[0]):
        total = total + ref[k, pl.ds(start, size)].astype(F32)
    return total


def tiles_of(block):
    return [block[4 * t : 4 * t + 4] for t in range(block.shape[0] // 4)]


def put(out, k, tiles):
    for t, tile in enumerate(tiles):
        out[k, t] = tile


def tiles_summed(ref, start, count):
    tiles = []
    for t in range(start, start + count):
        total = ref[0, t].astype(F32)
        for k in range(1, ref.shape[0]):
            total = total + ref[k, t].astype(F32)
        tiles.append(total)
    return tiles[0] if count == 1 else jnp.concatenate(tiles, axis=0)


def k_start(turned_hbm, gain_hbm, out, turned, gain, sem):
    pairs = ((turned_hbm, turned), (gain_hbm, gain))
    copies = [pltpu.make_async_copy(a, b, sem.at[k]) for k, (a, b) in enumerate(pairs)]
    for copy in copies:
        copy.start()
    for copy in copies:
        copy.wait()
    own, rows = turned.shape
    column = jnp.sum(jnp.where(diagonal(own, 0)[:, :own], gain[...], 0.0), axis=1, keepdims=True)
    pad = jnp.zeros((own, LANES - rows), F32)
    tile = jnp.concatenate([turned[...].astype(F32), pad], axis=1)
    for k, piece in enumerate(in_pieces(column, 3)):
        tile = jnp.where(iota(tile.shape, 1) == rows + k, piece, tile)
    tile = tile.astype(BF16)
    for k in range(out.shape[0]):
        out[k] = tile


def k_project(recv, w_query, w_key, w_value, w_forget, w_out, bias, out, x_out, gain_out, new_rows):
    width = recv.shape[0]
    same = jnp.where(iota((width, width), 0) == iota((width, width), 1), 1.0, 0.0).astype(BF16)
    rows = new_rows.shape[0]
    both = across(recv[:, : 2 * rows], same, FIRST)
    x = both[:rows]
    x_out[...] = x
    gain = both[rows : rows + 1] + both[rows + 1 : rows + 2] + both[rows + 2 : rows + 3]
    gain_out[...] = jnp.broadcast_to(gain, gain_out.shape)
    xb = x.astype(BF16)
    row = iota((8, LANES), 0)
    sums = across(jnp.ones((8, LANES), BF16), w_out[...], LAST)
    mine = iota(bias.shape, 1) == lax.axis_index("tp")
    once = jnp.where(kv_index() == 0, 1.0, 0.0)
    own_bias = jnp.sum(jnp.where(mine, bias[...], 0.0), axis=1, keepdims=True) * once
    query = jnp.dot(xb, w_query[...], preferred_element_type=F32)
    new_rows[:, :DH] = across(xb, w_key[...], LAST)
    new_rows[:, DH:] = across(xb, w_value[...], LAST)
    start = pl.multiple_of(kv_index() * width, width)
    forget = across(xb, w_forget[:, pl.ds(start, width)], LAST)
    token_col = jnp.sum(x, axis=1, keepdims=True)
    mine = iota(forget.shape, 1) == lax.axis_index("tp")
    forget_col = jnp.sum(jnp.where(mine, forget, 0.0), axis=1, keepdims=True)
    forget_col = forget_col + own_bias
    small = as_row([*in_pieces(forget_col, 2), *in_pieces(token_col, 2)])
    tail = jnp.where(row == 1, small, 0.0)
    tail = jnp.where(row == 2, sums[:, :LANES], tail)
    tail = jnp.where(row == 3, sums[:, LANES:], tail)
    tiles = tiles_of(query[:, :LANES].astype(BF16)) + tiles_of(query[:, LANES:].astype(BF16))
    for b in range(rows):
        own_tail = jnp.where(row == 0, new_rows[pl.ds(b, 1), :], tail)[:4].astype(BF16)
        for k in range(b, out.shape[0], rows):
            put(out, k, [*tiles, own_tail])


def k_prepare(lengths, cache, gate, keys_o, values_o, gate_o, cache_v, gate_v, sem, gate_sem):
    rows, positions = cache.shape[:2]
    copies = [pltpu.make_async_copy(cache.at[b], cache_v.at[b], sem.at[b]) for b in range(rows)]
    gates = pltpu.make_async_copy(gate, gate_v, gate_sem)
    gates.start()
    for copy in copies:
        copy.start()
    gates.wait()
    place = kv_index() * positions + iota((8, positions), 1)
    first = iota((8, positions), 0) < 4
    for m in range(rows // 2):
        one = jnp.where(place < lengths[2 * m], gate_v[2 * m], EMPTY_SCORE)
        two = jnp.where(place < lengths[2 * m + 1], gate_v[2 * m + 1], EMPTY_SCORE)
        gate_o[m // 2, pl.ds(8 * (m % 2), 8), :] = jnp.where(first, one, two)
    for b in range(rows):
        copies[b].wait()
        keys_o[b // 4, pl.ds(DH * (b % 4), DH), :] = cache_v[b].T[:DH]
        if b % 2:
            values_o[b // 4, :, pl.ds(LANES * (b % 4 // 2), LANES)] = jnp.concatenate(
                [cache_v[b - 1][:, DH:], cache_v[b][:, DH:]], axis=1
            )


def k_attend(recv, keys, values, gate, out, tok_out, sums_out, qs, firsts, seconds):
    rows = 4 * keys.shape[0]
    heads = 4
    scale = DH**-0.5
    left = rounded(tiles_summed(recv, 0, rows // 4))
    right = rounded(tiles_summed(recv, rows // 4, rows // 4))
    tail = tiles_summed(recv, rows // 2, 1)
    new_row = rounded(tail[0:1])
    small = tail[1:2]
    sums_out[...] = tail[2:4]
    tok_out[...] = jnp.broadcast_to(as_column(small, rows, (2, 3)), tok_out.shape)
    even = iota((rows, LANES), 0) % 2 == 0
    low = iota((rows, LANES), 1) < DH
    keep = even == low
    left_turned = pltpu.roll(left, DH, 1)
    right_turned = pltpu.roll(right, DH, 1)
    placed = (
        jnp.where(even, left, left_turned),
        jnp.where(even, left_turned, left),
        jnp.where(even, right, right_turned),
        jnp.where(even, right_turned, right),
    )
    for h, block in enumerate(placed):
        qs[pl.ds(h, rows, stride=heads), :] = jnp.where(keep, block, 0.0)
    all_rows = rows * heads
    owner = iota((all_rows, LANES), 0) // heads
    lane = iota((all_rows, LANES), 1)
    fetched = jnp.where((lane == owner) | (lane == owner + rows), small, 0.0)
    fetched = jnp.sum(fetched, axis=1, keepdims=True)
    new_gate = jnp.minimum(fetched, 0.0) - jnp.log(1.0 + jnp.exp(-jnp.abs(fetched)))
    lane = iota((1, LANES), 1)
    new_turned = pltpu.roll(jnp.broadcast_to(new_row, (8, LANES)), DH, 1)[0:1]
    new_key = jnp.where(lane < DH, new_row, new_turned)
    new_value = jnp.where(lane < DH, new_turned, new_row)
    own = jnp.sum(qs[...] * new_key, axis=1, keepdims=True) * scale
    mine = iota((all_rows, 1), 0) // heads == kv_index()
    own = jnp.where(mine, own, EMPTY_SCORE)
    lane = iota((16, LANES), 1)
    spot = jnp.where(iota((16, LANES), 0) % 8 < heads, DH, 0)
    upper = iota((16, LANES), 0) < 8
    straight = iota((16, LANES), 0) % 8 < heads
    for m in range(rows // 4):
        at = slice(16 * m, 16 * m + 16)
        query = qs[pl.ds(16 * m, 16), :] * scale
        query = [jnp.where(upper, query, 0.0), jnp.where(upper, 0.0, query)]
        query = jnp.concatenate(query, axis=1).astype(BF16)
        scores = jnp.dot(query, keys[m], preferred_element_type=F32)
        scores = scores + (gate[m] + new_gate[at])
        top = jnp.maximum(jnp.max(scores, axis=1, keepdims=True), own[at])
        top = jnp.maximum(top, 0.1 * EMPTY_SCORE)
        weights = jnp.exp(scores - top)
        own_weight = jnp.exp(own[at] - top)
        total = jnp.sum(weights, axis=1, keepdims=True) + own_weight
        value = jnp.dot(weights.astype(BF16), values[m], preferred_element_type=F32)
        value = jnp.where(upper, value[:, :LANES], value[:, LANES:])
        value = value + rounded(own_weight) * new_value
        spare = jnp.where(lane == spot, top, jnp.where(lane == spot + 1, total, value))
        turned = pltpu.roll(spare, DH, 1)
        firsts[pl.ds(16 * m, 16), :] = jnp.where(straight, spare, turned)
        seconds[pl.ds(16 * m, 16), :] = jnp.where(straight, turned, spare)
        for side in range(2):
            at = 16 * m + 2 * side
            left = firsts[pl.ds(at, 4, stride=heads), :]
            right = seconds[pl.ds(at + 1, 4, stride=heads), :]
            tile = jnp.where(low[:4], left, right).astype(BF16)
            for k in range(out.shape[0]):
                out[k, rows // 4 * side + m] = tile
    blocks = [seconds[pl.ds(h, rows, stride=heads), :] for h in range(heads)]
    lane = iota((rows, LANES), 1)
    stats = jnp.zeros((rows, LANES), F32)
    for h in range(heads):
        pieces = [*in_pieces(blocks[h][:, 0:1], 3), *in_pieces(blocks[h][:, 1:2], 2)]
        for k, piece in enumerate(pieces):
            stats = jnp.where(lane == 8 * h + k, piece, stats)
    packed = stats[:4]
    for g in range(1, rows // 4):
        packed = packed + pltpu.roll(stats, 32 * g, 1)[4 * g : 4 * g + 4]
    packed = packed.astype(BF16)
    for k in range(out.shape[0]):
        out[k, rows // 2] = packed


def k_combine(recv, sums, w_out, out):
    devices = recv.shape[0]
    tiles = (recv.shape[1] - 1) // 2
    rows = 4 * tiles
    heads = 4 * DH
    source = iota((LANES, 2 * heads), 0) % 32
    column = iota((LANES, 2 * heads), 1)
    first = 8 * ((column % heads) // DH)
    is_top = column < heads
    begin = jnp.where(is_top, first, first + 3)
    end = jnp.where(is_top, first + 3, first + 5)
    spread = jnp.where((source >= begin) & (source < end), 1.0, 0.0).astype(BF16)
    stats = recv[:, 2 * tiles].astype(F32)
    stats = jnp.concatenate([stats, stats], axis=1)
    group = iota(stats.shape, 2) // 32 - iota(stats.shape, 1) // 4
    blocks = []
    for half in range(2):
        mine = jnp.where(group == 2 * half, stats, 0.0).astype(BF16).reshape(devices * 8, LANES)
        wide = jnp.dot(mine, spread, preferred_element_type=F32).reshape(devices, 8, 2 * heads)
        tops = wide[:, :, :heads]
        totals = wide[:, :, heads:]
        scales = jnp.exp(tops - jnp.max(tops, axis=0, keepdims=True))
        total = jnp.sum(totals * scales, axis=0)
        sides = []
        for side in range(2):
            at = tiles * side + 2 * half
            part = [recv[:, at + t].astype(F32) for t in range(2)]
            part = jnp.concatenate(part, axis=1)
            sides.append(jnp.sum(part * scales[:, :, side * LANES : (side + 1) * LANES], axis=0))
        blocks.append(jnp.concatenate(sides, axis=1) / total)
    attended = jnp.concatenate(blocks, axis=0).astype(BF16)
    wide = attended.astype(F32)
    mean = wide[:, :LANES] * sums[0:1, :] + wide[:, LANES:] * sums[1:2, :]
    mean = jnp.sum(mean, axis=1, keepdims=True) / D
    attn_part = jnp.dot(attended, w_out[...], preferred_element_type=F32)
    attn_part = (attn_part - mean).astype(BF16)
    for k in range(out.shape[0]):
        out[k] = attn_part


def k_expand(recv, x, tok, gain, w_gate, w_up, out, scaled_out, tile):
    rows = x.shape[0]
    centred = x[...] - tok[:, 0:1] / D + summed(recv, 0, rows)
    scaled = centred * gain[0:1, :]
    scaled_out[...] = scaled
    squares = as_row(in_pieces(jnp.sum(centred * centred, axis=1, keepdims=True), 2))
    scaled = scaled.astype(BF16)
    pieces = tile.shape[0] // (8 * rows)
    tiles = 3 * pieces
    columns = w_gate.shape[0]
    for k, weight in enumerate((w_gate, w_up)):
        part = across(scaled, weight[...], LAST)
        pad = jnp.zeros((rows, tiles * LANES - columns), F32)
        part = jnp.concatenate([part, pad], axis=1)
        for t in range(tiles):
            at = 8 * (t // 3) + 3 * k + t % 3
            tile[pl.ds(at, rows, stride=8 * pieces), :] = part[:, t * LANES : (t + 1) * LANES]
    for h in range(pieces):
        tile[pl.ds(8 * h + 6, rows, stride=8 * pieces), :] = jnp.broadcast_to(
            squares, (rows, LANES)
        )
        tile[pl.ds(8 * h + 7, rows, stride=8 * pieces), :] = jnp.zeros((rows, LANES), F32)
    for k in range(out.shape[0]):
        out[k] = tile[pl.ds(8 * k, 8), :].astype(BF16)


def k_hidden(recv, scaled, out, mid_out):
    rows = scaled.shape[0]
    total = summed(recv, 0, 8)
    spread = as_column(total[6:7], rows, (0, 1)) / D
    shrink = lax.rsqrt(spread + EPSILON)
    mid_out[...] = rounded(scaled[...] * shrink)
    mine = iota((rows, 1), 0) == kv_index() // (out.shape[0] // rows)
    own = jnp.sum(jnp.where(mine, shrink, 0.0), axis=0, keepdims=True)
    total = total * own
    up = pltpu.roll(total, 5, 0)
    hidden = total / (1.0 + jnp.exp(-total)) * up
    hidden = jnp.where(iota((8, LANES), 0) < 3, hidden, 0.0)[:4].astype(BF16)
    for k in range(out.shape[0]):
        out[k] = hidden


def k_shrink(recv, w_down, out, tile):
    rows = out.shape[1]
    pieces = recv.shape[0] // rows
    for k in range(recv.shape[0]):
        tile[pl.ds(4 * k, 4), :] = recv[k].astype(F32)
    part = jnp.zeros((rows, LANES), F32)
    columns = w_down.shape[0]
    for t in range(3 * pieces):
        at = 4 * (t // 3) + t % 3
        size = min(LANES, columns - t * LANES)
        hidden = tile[pl.ds(at, rows, stride=4 * pieces), :][:, :size].astype(BF16)
        part = part + jnp.dot(
            hidden, w_down[pl.ds(t * LANES, size), :], preferred_element_type=F32
        )
    part = part.astype(BF16)
    for k in range(out.shape[0]):
        out[k] = part


def k_sums(recv, mid, out, own_out, turned):
    rows, width = mid.shape
    mixture = mid[...] + summed(recv, 0, rows)
    centre = jnp.sum(mixture, axis=1, keepdims=True) / width
    square = jnp.sum((mixture - centre) ** 2, axis=1, keepdims=True)
    message = as_row([centre, square])
    for k in range(out.shape[0]):
        out[k] = message
    turned[...] = mixture.T
    own = own_out.shape[0]
    start = pl.multiple_of(lax.axis_index("tp") * own, own)
    own_out[...] = turned[pl.ds(start, own), :]


def k_finish(recv, mix, gain, out):
    own, rows = mix.shape
    devices = recv.shape[0]
    total = recv[0]
    for k in range(1, devices):
        total = total + recv[k]
    middle = total / devices
    spread = (recv[0] - middle) ** 2
    for k in range(1, devices):
        spread = spread + (recv[k] - middle) ** 2
    spread = spread[:, :rows] * (D // devices) + total[:, rows : 2 * rows]
    shrink = lax.rsqrt(spread / D + EPSILON)
    column = jnp.sum(jnp.where(diagonal(own, 0)[:, :own], gain[...], 0.0), axis=1, keepdims=True)
    out[...] = ((mix[...] - middle[:, :rows]) * shrink * column).astype(BF16)


def on_device(
    tokens,
    live_lengths,
    kv_cache,
    gate_sums,
    w_query,
    w_key,
    w_value,
    w_forget,
    forget_bias,
    w_out,
    first_gain,
    w_gate,
    w_up,
    w_down,
    second_gain,
):
    rows, own = tokens.shape
    kv, tp = lax.axis_size(KV), lax.axis_size("tp")
    width = own * tp
    block = ((rows, LANES), F32)
    in_hbm = functools.partial(pltpu.with_memory_space_constraint, memory_space=pltpu.HBM)
    (message,) = kernel(
        k_start,
        [((tp, own, LANES), BF16)],
        [ANY] * 2,
        [
            pltpu.VMEM((own, rows), BF16),
            pltpu.VMEM((1, own), F32),
            pltpu.SemaphoreType.DMA((2,)),
        ],
        flops=10**11,
    )(in_hbm(tokens.T), in_hbm(first_gain[None]))
    recv = exchanged(message, "tp").reshape(width, LANES)
    message, x, gain = kernel(
        k_project,
        [((kv, rows // 2 + 1, 4, LANES), BF16), block, ((8, LANES), F32)],
        [VMEM] * 7,
        [pltpu.VMEM((rows, LANES), F32)],
    )(
        recv,
        w_query,
        w_key.T,
        w_value.T,
        w_forget.T,
        w_out,
        forget_bias[None],
    )
    recv = exchanged(message, KV)
    positions = kv_cache.shape[1]
    keys, values, gate_sums = kernel(
        k_prepare,
        [
            ((rows // 4, 4 * DH, positions), BF16),
            ((rows // 4, positions, 4 * DH), BF16),
            ((rows // 4, 16, positions), F32),
        ],
        [SMEM, ANY, ANY],
        [
            pltpu.VMEM(kv_cache.shape, BF16),
            pltpu.VMEM(gate_sums.shape, F32),
            pltpu.SemaphoreType.DMA((rows,)),
            pltpu.SemaphoreType.DMA,
        ],
    )(live_lengths, in_hbm(kv_cache), in_hbm(gate_sums))
    message, tok, sums = kernel(
        k_attend,
        [((kv, rows // 2 + 1, 4, LANES), BF16), block, ((2, LANES), F32)],
        [VMEM] * 4,
        [pltpu.VMEM((4 * rows, LANES), F32)] * 3,
    )(recv, keys, values, gate_sums)
    (message,) = kernel(k_combine, [((tp, rows, width), BF16)], [VMEM] * 3)(
        exchanged(message, KV), sums, w_out
    )
    message, scaled = kernel(
        k_expand,
        [((kv, 8, LANES), BF16), block],
        [VMEM] * 6,
        [pltpu.VMEM((8 * kv, LANES), F32)],
    )(exchanged(message, "tp"), x, tok, gain, w_gate.T, w_up.T)
    message, mid = kernel(k_hidden, [((kv, 4, LANES), BF16), block], [VMEM] * 2)(
        exchanged(message, KV), scaled
    )
    (message,) = kernel(
        k_shrink, [((tp, rows, width), BF16)], [VMEM] * 2, [pltpu.VMEM((4 * kv, LANES), F32)]
    )(exchanged(message, KV), w_down)
    message, mix = kernel(
        k_sums,
        [((kv, 1, LANES), F32), ((own, rows), F32)],
        [VMEM] * 2,
        [pltpu.VMEM((width, rows), F32)],
    )(
        exchanged(message, "tp"), mid
    )
    (out,) = kernel(k_finish, [((own, rows), BF16)], [VMEM] * 3, last=True)(exchanged(message, KV), mix, second_gain[None])
    return out.T


def solution(mesh):
    split = Mesh(mesh.devices.reshape(8, 4, mesh.shape["tp"]), ("kv_0", "kv_1", "tp"))
    placed = (
        P(None, KV_TP),
        P(),
        P(None, KV, "tp"),
        P(None, "tp", KV),
        P(KV, "tp"),
        P(KV, "tp"),
        P(KV, "tp"),
        P(),
        P(),
        P("tp", KV),
        P(KV_TP),
        P(KV, "tp"),
        P(KV, "tp"),
        P("tp", KV),
        P(KV_TP),
    )
    return jax.shard_map(
        on_device, mesh=split, in_specs=placed, out_specs=P(None, KV_TP), check_vma=False
    )
```

```python
import functools

import jax
import jax.numpy as jnp
from jax import lax
from jax.experimental import pallas as pl
from jax.experimental.pallas import tpu as pltpu
from jax.sharding import Mesh
from jax.sharding import PartitionSpec as P

D = 4096
DH = 64
LANES = 128
KV = ("kv_0", "kv_1")
KV_TP = ("kv_0", "kv_1", "tp")
EPSILON = 1e-05
EMPTY_SCORE = -1e30
F32 = jnp.float32
BF16 = jnp.bfloat16

VMEM = pl.BlockSpec(memory_space=pltpu.VMEM)
SMEM = pl.BlockSpec(memory_space=pltpu.SMEM)
ANY = pl.BlockSpec(memory_space=pl.ANY)


def kernel(body, outs, specs, scratch=(), last=False, flops=None):
    return pl.pallas_call(
        body,
        out_shape=[
            jax.ShapeDtypeStruct(shape, dtype) if last else pltpu.VMEM(shape, dtype)
            for shape, dtype in outs
        ],
        in_specs=specs,
        out_specs=[VMEM] * len(outs),
        scratch_shapes=scratch,
        cost_estimate=flops
        and pl.CostEstimate(flops=flops, bytes_accessed=flops // 100, transcendentals=0),
        compiler_params=pltpu.CompilerParams(vmem_limit_bytes=8 * 2**20),
    )


def exchanged(pieces, axis):
    return lax.all_to_all(pieces, axis, 0, 0, tiled=True)


def kv_index():
    return lax.axis_index("kv_0") * lax.axis_size("kv_1") + lax.axis_index("kv_1")


def iota(shape, dim):
    return lax.broadcasted_iota(jnp.int32, shape, dim)


def rounded(x):
    return x.astype(BF16).astype(F32)


def in_pieces(value, count):
    pieces = []
    for _ in range(count):
        piece = rounded(value)
        pieces.append(piece)
        value = value - piece
    return pieces


def diagonal(rows, turn):
    return iota((rows, LANES), 1) == iota((rows, LANES), 0) + rows * turn


def across(left, right, sides):
    return lax.dot_general(left, right, (sides, ((), ())), preferred_element_type=F32)


LAST = ((1,), (1,))
FIRST = ((0,), (0,))


def as_row(columns):
    rows = columns[0].shape[0]
    tile = jnp.zeros((rows, LANES), F32)
    for turn, column in enumerate(columns):
        tile = jnp.where(diagonal(rows, turn), column, tile)
    return jnp.sum(tile, axis=0, keepdims=True)


def as_column(row, rows, turns):
    mask = diagonal(rows, turns[0])
    for turn in turns[1:]:
        mask = mask | diagonal(rows, turn)
    return jnp.sum(jnp.where(mask, row, 0.0), axis=1, keepdims=True)


def summed(ref, start, size):
    total = ref[0, pl.ds(start, size)].astype(F32)
    for k in range(1, ref.shape[0]):
        total = total + ref[k, pl.ds(start, size)].astype(F32)
    return total


def tiles_of(block):
    return [block[4 * t : 4 * t + 4] for t in range(block.shape[0] // 4)]


def put(out, k, tiles):
    for t, tile in enumerate(tiles):
        out[k, t] = tile


def tiles_summed(ref, start, count):
    tiles = []
    for t in range(start, start + count):
        total = ref[0, t].astype(F32)
        for k in range(1, ref.shape[0]):
            total = total + ref[k, t].astype(F32)
        tiles.append(total)
    return tiles[0] if count == 1 else jnp.concatenate(tiles, axis=0)


def k_start(turned_hbm, gain_hbm, out, turned, gain, sem):
    pairs = ((turned_hbm, turned), (gain_hbm, gain))
    copies = [pltpu.make_async_copy(a, b, sem.at[k]) for k, (a, b) in enumerate(pairs)]
    for copy in copies:
        copy.start()
    for copy in copies:
        copy.wait()
    own, rows = turned.shape
    column = jnp.sum(jnp.where(diagonal(own, 0)[:, :own], gain[...], 0.0), axis=1, keepdims=True)
    pad = jnp.zeros((own, LANES - rows), F32)
    tile = jnp.concatenate([turned[...].astype(F32), pad], axis=1)
    for k, piece in enumerate(in_pieces(column, 3)):
        tile = jnp.where(iota(tile.shape, 1) == rows + k, piece, tile)
    tile = tile.astype(BF16)
    for k in range(out.shape[0]):
        out[k] = tile


def k_project(recv, w_query, w_key, w_value, w_forget, w_out, bias, out, x_out, gain_out, new_rows):
    width = recv.shape[0]
    same = jnp.where(iota((width, width), 0) == iota((width, width), 1), 1.0, 0.0).astype(BF16)
    rows = new_rows.shape[0]
    both = across(recv[:, : 2 * rows], same, FIRST)
    x = both[:rows]
    x_out[...] = x
    gain = both[rows : rows + 1] + both[rows + 1 : rows + 2] + both[rows + 2 : rows + 3]
    gain_out[...] = jnp.broadcast_to(gain, gain_out.shape)
    xb = x.astype(BF16)
    row = iota((8, LANES), 0)
    sums = across(jnp.ones((8, LANES), BF16), w_out[...], LAST)
    mine = iota(bias.shape, 1) == lax.axis_index("tp")
    once = jnp.where(kv_index() == 0, 1.0, 0.0)
    own_bias = jnp.sum(jnp.where(mine, bias[...], 0.0), axis=1, keepdims=True) * once
    query = jnp.dot(xb, w_query[...], preferred_element_type=F32)
    new_rows[:, :DH] = across(xb, w_key[...], LAST)
    new_rows[:, DH:] = across(xb, w_value[...], LAST)
    start = pl.multiple_of(kv_index() * width, width)
    forget = across(xb, w_forget[:, pl.ds(start, width)], LAST)
    token_col = jnp.sum(x, axis=1, keepdims=True)
    mine = iota(forget.shape, 1) == lax.axis_index("tp")
    forget_col = jnp.sum(jnp.where(mine, forget, 0.0), axis=1, keepdims=True)
    forget_col = forget_col + own_bias
    small = as_row([*in_pieces(forget_col, 2), *in_pieces(token_col, 2)])
    tail = jnp.where(row == 1, small, 0.0)
    tail = jnp.where(row == 2, sums[:, :LANES], tail)
    tail = jnp.where(row == 3, sums[:, LANES:], tail)
    tiles = tiles_of(query[:, :LANES].astype(BF16)) + tiles_of(query[:, LANES:].astype(BF16))
    for b in range(rows):
        own_tail = jnp.where(row == 0, new_rows[pl.ds(b, 1), :], tail)[:4].astype(BF16)
        for k in range(b, out.shape[0], rows):
            put(out, k, [*tiles, own_tail])


def k_prepare(lengths, cache, gate, keys_o, values_o, gate_o, cache_v, gate_v, sem, gate_sem):
    rows, positions = cache.shape[:2]
    copies = [pltpu.make_async_copy(cache.at[b], cache_v.at[b], sem.at[b]) for b in range(rows)]
    gates = pltpu.make_async_copy(gate, gate_v, gate_sem)
    gates.start()
    for copy in copies:
        copy.start()
    gates.wait()
    place = kv_index() * positions + iota((8, positions), 1)
    first = iota((8, positions), 0) < 4
    for m in range(rows // 2):
        one = jnp.where(place < lengths[2 * m], gate_v[2 * m], EMPTY_SCORE)
        two = jnp.where(place < lengths[2 * m + 1], gate_v[2 * m + 1], EMPTY_SCORE)
        gate_o[m // 2, pl.ds(8 * (m % 2), 8), :] = jnp.where(first, one, two)
    for b in range(rows):
        copies[b].wait()
        keys_o[b // 4, pl.ds(DH * (b % 4), DH), :] = cache_v[b].T[:DH]
        if b % 2:
            values_o[b // 4, :, pl.ds(LANES * (b % 4 // 2), LANES)] = jnp.concatenate(
                [cache_v[b - 1][:, DH:], cache_v[b][:, DH:]], axis=1
            )


def k_attend(recv, keys, values, gate, out, tok_out, sums_out, qs, firsts, seconds, stats):
    rows = 4 * keys.shape[0]
    heads = 4
    scale = DH**-0.5
    left = rounded(tiles_summed(recv, 0, rows // 4))
    right = rounded(tiles_summed(recv, rows // 4, rows // 4))
    tail = tiles_summed(recv, rows // 2, 1)
    new_row = rounded(tail[0:1])
    small = tail[1:2]
    sums_out[...] = tail[2:4]
    tok_out[...] = jnp.broadcast_to(as_column(small, rows, (2, 3)), tok_out.shape)
    even = iota((rows, LANES), 0) % 2 == 0
    low = iota((rows, LANES), 1) < DH
    keep = even == low
    left_turned = pltpu.roll(left, DH, 1)
    right_turned = pltpu.roll(right, DH, 1)
    placed = (
        jnp.where(even, left, left_turned),
        jnp.where(even, left_turned, left),
        jnp.where(even, right, right_turned),
        jnp.where(even, right_turned, right),
    )
    for h, block in enumerate(placed):
        qs[pl.ds(h, rows, stride=heads), :] = jnp.where(keep, block, 0.0)
    all_rows = rows * heads
    owner = iota((all_rows, LANES), 0) // heads
    lane = iota((all_rows, LANES), 1)
    fetched = jnp.where((lane == owner) | (lane == owner + rows), small, 0.0)
    fetched = jnp.sum(fetched, axis=1, keepdims=True)
    new_gate = jnp.minimum(fetched, 0.0) - jnp.log(1.0 + jnp.exp(-jnp.abs(fetched)))
    lane = iota((1, LANES), 1)
    new_turned = pltpu.roll(jnp.broadcast_to(new_row, (8, LANES)), DH, 1)[0:1]
    new_key = jnp.where(lane < DH, new_row, new_turned)
    new_value = jnp.where(lane < DH, new_turned, new_row)
    own = jnp.sum(qs[...] * new_key, axis=1, keepdims=True) * scale
    mine = iota((all_rows, 1), 0) // heads == kv_index()
    own = jnp.where(mine, own, EMPTY_SCORE)
    lane = iota((16, LANES), 1)
    spot = jnp.where(iota((16, LANES), 0) % 8 < heads, DH, 0)
    upper = iota((16, LANES), 0) < 8
    straight = iota((16, LANES), 0) % 8 < heads
    packed = jnp.zeros((4, LANES), F32)
    for m in range(rows // 4):
        at = slice(16 * m, 16 * m + 16)
        query = qs[pl.ds(16 * m, 16), :] * scale
        query = [jnp.where(upper, query, 0.0), jnp.where(upper, 0.0, query)]
        query = jnp.concatenate(query, axis=1).astype(BF16)
        scores = jnp.dot(query, keys[m], preferred_element_type=F32)
        scores = scores + (gate[m] + new_gate[at])
        top = jnp.maximum(jnp.max(scores, axis=1, keepdims=True), own[at])
        top = jnp.maximum(top, 0.1 * EMPTY_SCORE)
        weights = jnp.exp(scores - top)
        own_weight = jnp.exp(own[at] - top)
        total = jnp.sum(weights, axis=1, keepdims=True) + own_weight
        value = jnp.dot(weights.astype(BF16), values[m], preferred_element_type=F32)
        value = jnp.where(upper, value[:, :LANES], value[:, LANES:])
        value = value + rounded(own_weight) * new_value
        spare = jnp.where(lane == spot, top, jnp.where(lane == spot + 1, total, value))
        turned = pltpu.roll(spare, DH, 1)
        firsts[pl.ds(16 * m, 16), :] = jnp.where(straight, spare, turned)
        second = jnp.where(straight, turned, spare)
        seconds[pl.ds(16 * m, 16), :] = second
        pieces = in_pieces(second, 3)
        stat = jnp.where(lane < 5, pltpu.roll(pieces[2], 4, 1), 0.0)
        stat = jnp.where(lane < 4, pltpu.roll(pieces[1], 2, 1), stat)
        stats[pl.ds(16 * m, 16), :] = jnp.where(lane < 2, pieces[0], stat)
        for h in range(heads):
            stat = stats[pl.ds(16 * m + h, 4, stride=heads), :]
            packed = packed + pltpu.roll(stat, 32 * m + 8 * h, 1)
        for side in range(2):
            at = 16 * m + 2 * side
            left = firsts[pl.ds(at, 4, stride=heads), :]
            right = seconds[pl.ds(at + 1, 4, stride=heads), :]
            tile = jnp.where(low[:4], left, right).astype(BF16)
            for k in range(out.shape[0]):
                out[k, rows // 4 * side + m] = tile
    packed = packed.astype(BF16)
    for k in range(out.shape[0]):
        out[k, rows // 2] = packed


def k_combine(recv, sums, w_out, out):
    devices = recv.shape[0]
    tiles = (recv.shape[1] - 1) // 2
    rows = 4 * tiles
    heads = 4 * DH
    source = iota((LANES, 2 * LANES), 0)
    column = iota((LANES, 2 * LANES), 1)
    place = source % 8
    is_top = column < LANES
    wanted = (place < 5) & (is_top == (place % 2 == 0))
    wanted = wanted & (source // 8 == column % LANES // 8)
    pick = jnp.where(wanted, 1.0, 0.0).astype(BF16)
    stats = recv[:, 2 * tiles].astype(F32)
    stats = jnp.concatenate([stats, stats], axis=1).astype(BF16).reshape(devices * 8, LANES)
    stats = jnp.dot(stats, pick, preferred_element_type=F32).reshape(devices, 8, 2 * LANES)
    tops = stats[:, :, :LANES]
    totals = stats[:, :, LANES:]
    scales = jnp.exp(tops - jnp.max(tops, axis=0, keepdims=True))
    joint = jnp.sum(totals * scales, axis=0, keepdims=True)
    shares = in_pieces(scales * (1.0 / joint), 2)
    source = iota((2 * LANES, heads), 0) % LANES
    column = iota((2 * LANES, heads), 1)
    wanted = (source % 8 == 0) & (source % 32 // 8 == column // DH)
    spread = jnp.where(wanted, 1.0, 0.0).astype(BF16)
    group = iota(tops.shape, 2) // 32 - iota(tops.shape, 1) // 4
    blocks = []
    for half in range(2):
        mine = [jnp.where(group == 2 * half, share, 0.0) for share in shares]
        mine = jnp.concatenate(mine, axis=2).astype(BF16).reshape(devices * 8, 2 * LANES)
        wide = jnp.dot(mine, spread, preferred_element_type=F32).reshape(devices, 8, heads)
        sides = []
        for side in range(2):
            at = tiles * side + 2 * half
            part = [recv[:, at + t].astype(F32) for t in range(2)]
            part = jnp.concatenate(part, axis=1)
            sides.append(jnp.sum(part * wide[:, :, side * LANES : (side + 1) * LANES], axis=0))
        blocks.append(jnp.concatenate(sides, axis=1))
    attended = jnp.concatenate(blocks, axis=0).astype(BF16)
    wide = attended.astype(F32)
    mean = wide[:, :LANES] * sums[0:1, :] + wide[:, LANES:] * sums[1:2, :]
    mean = jnp.sum(mean, axis=1, keepdims=True) / D
    attn_part = jnp.dot(attended, w_out[...], preferred_element_type=F32)
    attn_part = (attn_part - mean).astype(BF16)
    for k in range(out.shape[0]):
        out[k] = attn_part


def k_expand(recv, x, tok, gain, w_gate, w_up, out, scaled_out, tile):
    rows = x.shape[0]
    centred = x[...] - tok[:, 0:1] / D + summed(recv, 0, rows)
    scaled = centred * gain[0:1, :]
    scaled_out[...] = scaled
    squares = as_row(in_pieces(jnp.sum(centred * centred, axis=1, keepdims=True), 2))
    scaled = scaled.astype(BF16)
    pieces = tile.shape[0] // (8 * rows)
    tiles = 3 * pieces
    columns = w_gate.shape[0]
    for k, weight in enumerate((w_gate, w_up)):
        part = across(scaled, weight[...], LAST)
        pad = jnp.zeros((rows, tiles * LANES - columns), F32)
        part = jnp.concatenate([part, pad], axis=1)
        for t in range(tiles):
            at = 8 * (t // 3) + 3 * k + t % 3
            tile[pl.ds(at, rows, stride=8 * pieces), :] = part[:, t * LANES : (t + 1) * LANES]
    for h in range(pieces):
        tile[pl.ds(8 * h + 6, rows, stride=8 * pieces), :] = jnp.broadcast_to(
            squares, (rows, LANES)
        )
        tile[pl.ds(8 * h + 7, rows, stride=8 * pieces), :] = jnp.zeros((rows, LANES), F32)
    for k in range(out.shape[0]):
        out[k] = tile[pl.ds(8 * k, 8), :].astype(BF16)


def k_hidden(recv, scaled, out, mid_out):
    rows = scaled.shape[0]
    total = summed(recv, 0, 8)
    spread = as_column(total[6:7], rows, (0, 1)) / D
    shrink = lax.rsqrt(spread + EPSILON)
    mid_out[...] = rounded(scaled[...] * shrink)
    mine = iota((rows, 1), 0) == kv_index() // (out.shape[0] // rows)
    own = jnp.sum(jnp.where(mine, shrink, 0.0), axis=0, keepdims=True)
    total = total * own
    up = pltpu.roll(total, 5, 0)
    hidden = total / (1.0 + jnp.exp(-total)) * up
    hidden = jnp.where(iota((8, LANES), 0) < 3, hidden, 0.0)[:4].astype(BF16)
    for k in range(out.shape[0]):
        out[k] = hidden


def k_shrink(recv, w_down, out, tile):
    rows = out.shape[1]
    pieces = recv.shape[0] // rows
    for k in range(recv.shape[0]):
        tile[pl.ds(4 * k, 4), :] = recv[k].astype(F32)
    part = jnp.zeros((rows, LANES), F32)
    columns = w_down.shape[0]
    for t in range(3 * pieces):
        at = 4 * (t // 3) + t % 3
        size = min(LANES, columns - t * LANES)
        hidden = tile[pl.ds(at, rows, stride=4 * pieces), :][:, :size].astype(BF16)
        part = part + jnp.dot(
            hidden, w_down[pl.ds(t * LANES, size), :], preferred_element_type=F32
        )
    part = part.astype(BF16)
    for k in range(out.shape[0]):
        out[k] = part


def k_sums(recv, mid, out, own_out, turned):
    rows, width = mid.shape
    mixture = mid[...] + summed(recv, 0, rows)
    centre = jnp.sum(mixture, axis=1, keepdims=True) / width
    square = jnp.sum((mixture - centre) ** 2, axis=1, keepdims=True)
    message = as_row([centre, square])
    for k in range(out.shape[0]):
        out[k] = message
    turned[...] = mixture.T
    own = own_out.shape[0]
    start = pl.multiple_of(lax.axis_index("tp") * own, own)
    own_out[...] = turned[pl.ds(start, own), :]


def k_finish(recv, mix, gain, out):
    own, rows = mix.shape
    devices = recv.shape[0]
    total = recv[0]
    for k in range(1, devices):
        total = total + recv[k]
    middle = total / devices
    spread = (recv[0] - middle) ** 2
    for k in range(1, devices):
        spread = spread + (recv[k] - middle) ** 2
    spread = spread[:, :rows] * (D // devices) + total[:, rows : 2 * rows]
    shrink = lax.rsqrt(spread / D + EPSILON)
    column = jnp.sum(jnp.where(diagonal(own, 0)[:, :own], gain[...], 0.0), axis=1, keepdims=True)
    out[...] = ((mix[...] - middle[:, :rows]) * shrink * column).astype(BF16)


def on_device(
    tokens,
    live_lengths,
    kv_cache,
    gate_sums,
    w_query,
    w_key,
    w_value,
    w_forget,
    forget_bias,
    w_out,
    first_gain,
    w_gate,
    w_up,
    w_down,
    second_gain,
):
    rows, own = tokens.shape
    kv, tp = lax.axis_size(KV), lax.axis_size("tp")
    width = own * tp
    block = ((rows, LANES), F32)
    in_hbm = functools.partial(pltpu.with_memory_space_constraint, memory_space=pltpu.HBM)
    (message,) = kernel(
        k_start,
        [((tp, own, LANES), BF16)],
        [ANY] * 2,
        [
            pltpu.VMEM((own, rows), BF16),
            pltpu.VMEM((1, own), F32),
            pltpu.SemaphoreType.DMA((2,)),
        ],
        flops=10**11,
    )(in_hbm(tokens.T), in_hbm(first_gain[None]))
    recv = exchanged(message, "tp").reshape(width, LANES)
    message, x, gain = kernel(
        k_project,
        [((kv, rows // 2 + 1, 4, LANES), BF16), block, ((8, LANES), F32)],
        [VMEM] * 7,
        [pltpu.VMEM((rows, LANES), F32)],
    )(
        recv,
        w_query,
        w_key.T,
        w_value.T,
        w_forget.T,
        w_out,
        forget_bias[None],
    )
    recv = exchanged(message, KV)
    positions = kv_cache.shape[1]
    keys, values, gate_sums = kernel(
        k_prepare,
        [
            ((rows // 4, 4 * DH, positions), BF16),
            ((rows // 4, positions, 4 * DH), BF16),
            ((rows // 4, 16, positions), F32),
        ],
        [SMEM, ANY, ANY],
        [
            pltpu.VMEM(kv_cache.shape, BF16),
            pltpu.VMEM(gate_sums.shape, F32),
            pltpu.SemaphoreType.DMA((rows,)),
            pltpu.SemaphoreType.DMA,
        ],
    )(live_lengths, in_hbm(kv_cache), in_hbm(gate_sums))
    message, tok, sums = kernel(
        k_attend,
        [((kv, rows // 2 + 1, 4, LANES), BF16), block, ((2, LANES), F32)],
        [VMEM] * 4,
        [pltpu.VMEM((4 * rows, LANES), F32)] * 4,
    )(recv, keys, values, gate_sums)
    (message,) = kernel(k_combine, [((tp, rows, width), BF16)], [VMEM] * 3)(
        exchanged(message, KV), sums, w_out
    )
    message, scaled = kernel(
        k_expand,
        [((kv, 8, LANES), BF16), block],
        [VMEM] * 6,
        [pltpu.VMEM((8 * kv, LANES), F32)],
    )(exchanged(message, "tp"), x, tok, gain, w_gate.T, w_up.T)
    message, mid = kernel(k_hidden, [((kv, 4, LANES), BF16), block], [VMEM] * 2)(
        exchanged(message, KV), scaled
    )
    (message,) = kernel(
        k_shrink, [((tp, rows, width), BF16)], [VMEM] * 2, [pltpu.VMEM((4 * kv, LANES), F32)]
    )(exchanged(message, KV), w_down)
    message, mix = kernel(
        k_sums,
        [((kv, 1, LANES), F32), ((own, rows), F32)],
        [VMEM] * 2,
        [pltpu.VMEM((width, rows), F32)],
    )(
        exchanged(message, "tp"), mid
    )
    (out,) = kernel(k_finish, [((own, rows), BF16)], [VMEM] * 3, last=True)(exchanged(message, KV), mix, second_gain[None])
    return out.T


def solution(mesh):
    split = Mesh(mesh.devices.reshape(8, 4, mesh.shape["tp"]), ("kv_0", "kv_1", "tp"))
    placed = (
        P(None, KV_TP),
        P(),
        P(None, KV, "tp"),
        P(None, "tp", KV),
        P(KV, "tp"),
        P(KV, "tp"),
        P(KV, "tp"),
        P(),
        P(),
        P("tp", KV),
        P(KV_TP),
        P(KV, "tp"),
        P(KV, "tp"),
        P("tp", KV),
        P(KV_TP),
    )
    return jax.shard_map(
        on_device, mesh=split, in_specs=placed, out_specs=P(None, KV_TP), check_vma=False
    )
```

```python
import functools

import jax
import jax.numpy as jnp
from jax import lax
from jax.experimental import pallas as pl
from jax.experimental.pallas import tpu as pltpu
from jax.sharding import Mesh
from jax.sharding import PartitionSpec as P

D = 4096
DH = 64
LANES = 128
KV = ("kv_0", "kv_1")
KV_TP = ("kv_0", "kv_1", "tp")
EPSILON = 1e-05
EMPTY_SCORE = -1e30
F32 = jnp.float32
BF16 = jnp.bfloat16

VMEM = pl.BlockSpec(memory_space=pltpu.VMEM)
SMEM = pl.BlockSpec(memory_space=pltpu.SMEM)
ANY = pl.BlockSpec(memory_space=pl.ANY)


def kernel(body, outs, specs, scratch=(), last=False, first=False, flops=None):
    return pl.pallas_call(
        body,
        out_shape=[
            jax.ShapeDtypeStruct(shape, dtype)
            if last or (first and n == 0)
            else pltpu.VMEM(shape, dtype)
            for n, (shape, dtype) in enumerate(outs)
        ],
        in_specs=specs,
        out_specs=[ANY if first and n == 0 else VMEM for n in range(len(outs))],
        scratch_shapes=scratch,
        cost_estimate=flops
        and pl.CostEstimate(flops=flops, bytes_accessed=flops // 100, transcendentals=0),
        compiler_params=pltpu.CompilerParams(vmem_limit_bytes=8 * 2**20),
    )


def exchanged(pieces, axis):
    return lax.all_to_all(pieces, axis, 0, 0, tiled=True)


def kv_index():
    return lax.axis_index("kv_0") * lax.axis_size("kv_1") + lax.axis_index("kv_1")


def iota(shape, dim):
    return lax.broadcasted_iota(jnp.int32, shape, dim)


def rounded(x):
    return x.astype(BF16).astype(F32)


def in_pieces(value, count):
    pieces = []
    for _ in range(count):
        piece = rounded(value)
        pieces.append(piece)
        value = value - piece
    return pieces


def diagonal(rows, turn):
    return iota((rows, LANES), 1) == iota((rows, LANES), 0) + rows * turn


def across(left, right, sides):
    return lax.dot_general(left, right, (sides, ((), ())), preferred_element_type=F32)


LAST = ((1,), (1,))
FIRST = ((0,), (0,))


def as_row(columns):
    rows = columns[0].shape[0]
    tile = jnp.zeros((rows, LANES), F32)
    for turn, column in enumerate(columns):
        tile = jnp.where(diagonal(rows, turn), column, tile)
    return jnp.sum(tile, axis=0, keepdims=True)


def as_column(row, rows, turns):
    mask = diagonal(rows, turns[0])
    for turn in turns[1:]:
        mask = mask | diagonal(rows, turn)
    return jnp.sum(jnp.where(mask, row, 0.0), axis=1, keepdims=True)


def summed(ref, start, size):
    total = ref[0, pl.ds(start, size)].astype(F32)
    for k in range(1, ref.shape[0]):
        total = total + ref[k, pl.ds(start, size)].astype(F32)
    return total


def tiles_of(block):
    return [block[4 * t : 4 * t + 4] for t in range(block.shape[0] // 4)]


def put(out, k, tiles):
    for t, tile in enumerate(tiles):
        out[k, t] = tile


def tiles_summed(ref, start, count):
    tiles = []
    for t in range(start, start + count):
        total = ref[0, t].astype(F32)
        for k in range(1, ref.shape[0]):
            total = total + ref[k, t].astype(F32)
        tiles.append(total)
    return tiles[0] if count == 1 else jnp.concatenate(tiles, axis=0)


def k_start(turned_hbm, gain_hbm, out, turned, gain, sem):
    pairs = ((turned_hbm, turned), (gain_hbm, gain))
    copies = [pltpu.make_async_copy(a, b, sem.at[k]) for k, (a, b) in enumerate(pairs)]
    for copy in copies:
        copy.start()
    for copy in copies:
        copy.wait()
    own, rows = turned.shape
    column = jnp.sum(jnp.where(diagonal(own, 0)[:, :own], gain[...], 0.0), axis=1, keepdims=True)
    pad = jnp.zeros((own, LANES - rows), F32)
    tile = jnp.concatenate([turned[...].astype(F32), pad], axis=1)
    for k, piece in enumerate(in_pieces(column, 3)):
        tile = jnp.where(iota(tile.shape, 1) == rows + k, piece, tile)
    tile = tile.astype(BF16)
    for k in range(out.shape[0]):
        out[k] = tile


def k_project(recv, w_query, w_key, w_value, w_forget, w_out, bias, out, x_out, gain_out, new_rows, staged, sem):
    width = recv.shape[0]
    same = jnp.where(iota((width, width), 0) == iota((width, width), 1), 1.0, 0.0).astype(BF16)
    rows = new_rows.shape[0]
    both = across(recv[:, : 2 * rows], same, FIRST)
    x = both[:rows]
    x_out[...] = x
    gain = both[rows : rows + 1] + both[rows + 1 : rows + 2] + both[rows + 2 : rows + 3]
    gain_out[...] = jnp.broadcast_to(gain, gain_out.shape)
    xb = x.astype(BF16)
    row = iota((8, LANES), 0)
    sums = across(jnp.ones((8, LANES), BF16), w_out[...], LAST)
    mine = iota(bias.shape, 1) == lax.axis_index("tp")
    once = jnp.where(kv_index() == 0, 1.0, 0.0)
    own_bias = jnp.sum(jnp.where(mine, bias[...], 0.0), axis=1, keepdims=True) * once
    query = jnp.dot(xb, w_query[...], preferred_element_type=F32)
    new_rows[:, :DH] = across(xb, w_key[...], LAST)
    new_rows[:, DH:] = across(xb, w_value[...], LAST)
    start = pl.multiple_of(kv_index() * width, width)
    forget = across(xb, w_forget[:, pl.ds(start, width)], LAST)
    token_col = jnp.sum(x, axis=1, keepdims=True)
    mine = iota(forget.shape, 1) == lax.axis_index("tp")
    forget_col = jnp.sum(jnp.where(mine, forget, 0.0), axis=1, keepdims=True)
    forget_col = forget_col + own_bias
    small = as_row([*in_pieces(forget_col, 2), *in_pieces(token_col, 2)])
    tail = jnp.where(row == 1, small, 0.0)
    tail = jnp.where(row == 2, sums[:, :LANES], tail)
    tail = jnp.where(row == 3, sums[:, LANES:], tail)
    tiles = tiles_of(query[:, :LANES].astype(BF16)) + tiles_of(query[:, LANES:].astype(BF16))
    devices = staged.shape[0]
    copies = []
    for b in range(rows):
        own_tail = jnp.where(row == 0, new_rows[pl.ds(b, 1), :], tail)[:4].astype(BF16)
        for k in range(b, devices, rows):
            put(staged, k, [*tiles, own_tail])
        if b % 4 == 3:
            for k in range(b - 3, devices, rows):
                at = pl.ds(k, 4)
                copies.append(pltpu.make_async_copy(staged.at[at], out.at[at], sem.at[k // 4]))
                copies[-1].start()
    for copy in copies:
        copy.wait()


def k_prepare(lengths, cache, gate, keys_o, values_o, gate_o, cache_v, gate_v, sem, gate_sem):
    rows, positions = cache.shape[:2]
    copies = [pltpu.make_async_copy(cache.at[b], cache_v.at[b], sem.at[b]) for b in range(rows)]
    gates = pltpu.make_async_copy(gate, gate_v, gate_sem)
    gates.start()
    for copy in copies:
        copy.start()
    gates.wait()
    place = kv_index() * positions + iota((8, positions), 1)
    first = iota((8, positions), 0) < 4
    for m in range(rows // 2):
        one = jnp.where(place < lengths[2 * m], gate_v[2 * m], EMPTY_SCORE)
        two = jnp.where(place < lengths[2 * m + 1], gate_v[2 * m + 1], EMPTY_SCORE)
        gate_o[m // 2, pl.ds(8 * (m % 2), 8), :] = jnp.where(first, one, two)
    for b in range(rows):
        copies[b].wait()
        keys_o[b // 4, pl.ds(DH * (b % 4), DH), :] = cache_v[b].T[:DH]
        if b % 2:
            values_o[b // 4, :, pl.ds(LANES * (b % 4 // 2), LANES)] = jnp.concatenate(
                [cache_v[b - 1][:, DH:], cache_v[b][:, DH:]], axis=1
            )


def k_attend(recv, keys, values, gate, out, tok_out, sums_out, qs, firsts, seconds, stats):
    rows = 4 * keys.shape[0]
    heads = 4
    scale = DH**-0.5
    left = rounded(tiles_summed(recv, 0, rows // 4))
    right = rounded(tiles_summed(recv, rows // 4, rows // 4))
    tail = tiles_summed(recv, rows // 2, 1)
    new_row = rounded(tail[0:1])
    small = tail[1:2]
    sums_out[...] = tail[2:4]
    tok_out[...] = jnp.broadcast_to(as_column(small, rows, (2, 3)), tok_out.shape)
    even = iota((rows, LANES), 0) % 2 == 0
    low = iota((rows, LANES), 1) < DH
    keep = even == low
    left_turned = pltpu.roll(left, DH, 1)
    right_turned = pltpu.roll(right, DH, 1)
    placed = (
        jnp.where(even, left, left_turned),
        jnp.where(even, left_turned, left),
        jnp.where(even, right, right_turned),
        jnp.where(even, right_turned, right),
    )
    for h, block in enumerate(placed):
        qs[pl.ds(h, rows, stride=heads), :] = jnp.where(keep, block, 0.0)
    all_rows = rows * heads
    owner = iota((all_rows, LANES), 0) // heads
    lane = iota((all_rows, LANES), 1)
    fetched = jnp.where((lane == owner) | (lane == owner + rows), small, 0.0)
    fetched = jnp.sum(fetched, axis=1, keepdims=True)
    new_gate = jnp.minimum(fetched, 0.0) - jnp.log(1.0 + jnp.exp(-jnp.abs(fetched)))
    lane = iota((1, LANES), 1)
    new_turned = pltpu.roll(jnp.broadcast_to(new_row, (8, LANES)), DH, 1)[0:1]
    new_key = jnp.where(lane < DH, new_row, new_turned)
    new_value = jnp.where(lane < DH, new_turned, new_row)
    own = jnp.sum(qs[...] * new_key, axis=1, keepdims=True) * scale
    mine = iota((all_rows, 1), 0) // heads == kv_index()
    own = jnp.where(mine, own, EMPTY_SCORE)
    lane = iota((16, LANES), 1)
    spot = jnp.where(iota((16, LANES), 0) % 8 < heads, DH, 0)
    upper = iota((16, LANES), 0) < 8
    straight = iota((16, LANES), 0) % 8 < heads
    packed = jnp.zeros((4, LANES), F32)
    for m in range(rows // 4):
        at = slice(16 * m, 16 * m + 16)
        query = qs[pl.ds(16 * m, 16), :] * scale
        query = [jnp.where(upper, query, 0.0), jnp.where(upper, 0.0, query)]
        query = jnp.concatenate(query, axis=1).astype(BF16)
        scores = jnp.dot(query, keys[m], preferred_element_type=F32)
        scores = scores + (gate[m] + new_gate[at])
        top = jnp.maximum(jnp.max(scores, axis=1, keepdims=True), own[at])
        top = jnp.maximum(top, 0.1 * EMPTY_SCORE)
        weights = jnp.exp(scores - top)
        own_weight = jnp.exp(own[at] - top)
        total = jnp.sum(weights, axis=1, keepdims=True) + own_weight
        value = jnp.dot(weights.astype(BF16), values[m], preferred_element_type=F32)
        value = jnp.where(upper, value[:, :LANES], value[:, LANES:])
        value = value + rounded(own_weight) * new_value
        spare = jnp.where(lane == spot, top, jnp.where(lane == spot + 1, total, value))
        turned = pltpu.roll(spare, DH, 1)
        firsts[pl.ds(16 * m, 16), :] = jnp.where(straight, spare, turned)
        second = jnp.where(straight, turned, spare)
        seconds[pl.ds(16 * m, 16), :] = second
        pieces = in_pieces(second, 3)
        stat = jnp.where(lane < 5, pltpu.roll(pieces[2], 4, 1), 0.0)
        stat = jnp.where(lane < 4, pltpu.roll(pieces[1], 2, 1), stat)
        stats[pl.ds(16 * m, 16), :] = jnp.where(lane < 2, pieces[0], stat)
        for h in range(heads):
            stat = stats[pl.ds(16 * m + h, 4, stride=heads), :]
            packed = packed + pltpu.roll(stat, 32 * m + 8 * h, 1)
        for side in range(2):
            at = 16 * m + 2 * side
            left = firsts[pl.ds(at, 4, stride=heads), :]
            right = seconds[pl.ds(at + 1, 4, stride=heads), :]
            tile = jnp.where(low[:4], left, right).astype(BF16)
            for k in range(out.shape[0]):
                out[k, rows // 4 * side + m] = tile
    packed = packed.astype(BF16)
    for k in range(out.shape[0]):
        out[k, rows // 2] = packed


def k_combine(recv, sums, w_out, out):
    devices = recv.shape[0]
    tiles = (recv.shape[1] - 1) // 2
    rows = 4 * tiles
    heads = 4 * DH
    source = iota((LANES, 2 * LANES), 0)
    column = iota((LANES, 2 * LANES), 1)
    place = source % 8
    is_top = column < LANES
    wanted = (place < 5) & (is_top == (place % 2 == 0))
    wanted = wanted & (source // 8 == column % LANES // 8)
    pick = jnp.where(wanted, 1.0, 0.0).astype(BF16)
    stats = recv[:, 2 * tiles].astype(F32)
    stats = jnp.concatenate([stats, stats], axis=1).astype(BF16).reshape(devices * 8, LANES)
    stats = jnp.dot(stats, pick, preferred_element_type=F32).reshape(devices, 8, 2 * LANES)
    tops = stats[:, :, :LANES]
    totals = stats[:, :, LANES:]
    scales = jnp.exp(tops - jnp.max(tops, axis=0, keepdims=True))
    joint = jnp.sum(totals * scales, axis=0, keepdims=True)
    shares = in_pieces(scales * (1.0 / joint), 2)
    source = iota((2 * LANES, heads), 0) % LANES
    column = iota((2 * LANES, heads), 1)
    wanted = (source % 8 == 0) & (source % 32 // 8 == column // DH)
    spread = jnp.where(wanted, 1.0, 0.0).astype(BF16)
    group = iota(tops.shape, 2) // 32 - iota(tops.shape, 1) // 4
    blocks = []
    for half in range(2):
        mine = [jnp.where(group == 2 * half, share, 0.0) for share in shares]
        mine = jnp.concatenate(mine, axis=2).astype(BF16).reshape(devices * 8, 2 * LANES)
        wide = jnp.dot(mine, spread, preferred_element_type=F32).reshape(devices, 8, heads)
        sides = []
        for side in range(2):
            at = tiles * side + 2 * half
            part = [recv[:, at + t].astype(F32) for t in range(2)]
            part = jnp.concatenate(part, axis=1)
            sides.append(jnp.sum(part * wide[:, :, side * LANES : (side + 1) * LANES], axis=0))
        blocks.append(jnp.concatenate(sides, axis=1))
    attended = jnp.concatenate(blocks, axis=0).astype(BF16)
    wide = attended.astype(F32)
    mean = wide[:, :LANES] * sums[0:1, :] + wide[:, LANES:] * sums[1:2, :]
    mean = jnp.sum(mean, axis=1, keepdims=True) / D
    attn_part = jnp.dot(attended, w_out[...], preferred_element_type=F32)
    attn_part = (attn_part - mean).astype(BF16)
    for k in range(out.shape[0]):
        out[k] = attn_part


def k_expand(recv, x, tok, gain, w_gate, w_up, out, scaled_out, tile):
    rows = x.shape[0]
    centred = x[...] - tok[:, 0:1] / D + summed(recv, 0, rows)
    scaled = centred * gain[0:1, :]
    scaled_out[...] = scaled
    squares = as_row(in_pieces(jnp.sum(centred * centred, axis=1, keepdims=True), 2))
    scaled = scaled.astype(BF16)
    pieces = tile.shape[0] // (8 * rows)
    tiles = 3 * pieces
    columns = w_gate.shape[0]
    for k, weight in enumerate((w_gate, w_up)):
        part = across(scaled, weight[...], LAST)
        pad = jnp.zeros((rows, tiles * LANES - columns), F32)
        part = jnp.concatenate([part, pad], axis=1)
        for t in range(tiles):
            at = 8 * (t // 3) + 3 * k + t % 3
            tile[pl.ds(at, rows, stride=8 * pieces), :] = part[:, t * LANES : (t + 1) * LANES]
    for h in range(pieces):
        tile[pl.ds(8 * h + 6, rows, stride=8 * pieces), :] = jnp.broadcast_to(
            squares, (rows, LANES)
        )
        tile[pl.ds(8 * h + 7, rows, stride=8 * pieces), :] = jnp.zeros((rows, LANES), F32)
    for k in range(out.shape[0]):
        out[k] = tile[pl.ds(8 * k, 8), :].astype(BF16)


def k_hidden(recv, scaled, out, mid_out):
    rows = scaled.shape[0]
    total = summed(recv, 0, 8)
    spread = as_column(total[6:7], rows, (0, 1)) / D
    shrink = lax.rsqrt(spread + EPSILON)
    mid_out[...] = rounded(scaled[...] * shrink)
    mine = iota((rows, 1), 0) == kv_index() // (out.shape[0] // rows)
    own = jnp.sum(jnp.where(mine, shrink, 0.0), axis=0, keepdims=True)
    total = total * own
    up = pltpu.roll(total, 5, 0)
    hidden = total / (1.0 + jnp.exp(-total)) * up
    hidden = jnp.where(iota((8, LANES), 0) < 3, hidden, 0.0)[:4].astype(BF16)
    for k in range(out.shape[0]):
        out[k] = hidden


def k_shrink(recv, w_down, out, tile):
    rows = out.shape[1]
    pieces = recv.shape[0] // rows
    for k in range(recv.shape[0]):
        tile[pl.ds(4 * k, 4), :] = recv[k].astype(F32)
    part = jnp.zeros((rows, LANES), F32)
    columns = w_down.shape[0]
    for t in range(3 * pieces):
        at = 4 * (t // 3) + t % 3
        size = min(LANES, columns - t * LANES)
        hidden = tile[pl.ds(at, rows, stride=4 * pieces), :][:, :size].astype(BF16)
        part = part + jnp.dot(
            hidden, w_down[pl.ds(t * LANES, size), :], preferred_element_type=F32
        )
    part = part.astype(BF16)
    for k in range(out.shape[0]):
        out[k] = part


def k_sums(recv, mid, out, own_out, turned):
    rows, width = mid.shape
    mixture = mid[...] + summed(recv, 0, rows)
    centre = jnp.sum(mixture, axis=1, keepdims=True) / width
    square = jnp.sum((mixture - centre) ** 2, axis=1, keepdims=True)
    message = as_row([centre, square])
    for k in range(out.shape[0]):
        out[k] = message
    turned[...] = mixture.T
    own = own_out.shape[0]
    start = pl.multiple_of(lax.axis_index("tp") * own, own)
    own_out[...] = turned[pl.ds(start, own), :]


def k_finish(recv, mix, gain, out):
    own, rows = mix.shape
    devices = recv.shape[0]
    total = recv[0]
    for k in range(1, devices):
        total = total + recv[k]
    middle = total / devices
    spread = (recv[0] - middle) ** 2
    for k in range(1, devices):
        spread = spread + (recv[k] - middle) ** 2
    spread = spread[:, :rows] * (D // devices) + total[:, rows : 2 * rows]
    shrink = lax.rsqrt(spread / D + EPSILON)
    column = jnp.sum(jnp.where(diagonal(own, 0)[:, :own], gain[...], 0.0), axis=1, keepdims=True)
    out[...] = ((mix[...] - middle[:, :rows]) * shrink * column).astype(BF16)


def on_device(
    tokens,
    live_lengths,
    kv_cache,
    gate_sums,
    w_query,
    w_key,
    w_value,
    w_forget,
    forget_bias,
    w_out,
    first_gain,
    w_gate,
    w_up,
    w_down,
    second_gain,
):
    rows, own = tokens.shape
    kv, tp = lax.axis_size(KV), lax.axis_size("tp")
    width = own * tp
    block = ((rows, LANES), F32)
    in_hbm = functools.partial(pltpu.with_memory_space_constraint, memory_space=pltpu.HBM)
    (message,) = kernel(
        k_start,
        [((tp, own, LANES), BF16)],
        [ANY] * 2,
        [
            pltpu.VMEM((own, rows), BF16),
            pltpu.VMEM((1, own), F32),
            pltpu.SemaphoreType.DMA((2,)),
        ],
        flops=10**11,
    )(in_hbm(tokens.T), in_hbm(first_gain[None]))
    recv = exchanged(message, "tp").reshape(width, LANES)
    message, x, gain = kernel(
        k_project,
        [((kv, rows // 2 + 1, 4, LANES), BF16), block, ((8, LANES), F32)],
        [VMEM] * 7,
        [
            pltpu.VMEM((rows, LANES), F32),
            pltpu.VMEM((kv, rows // 2 + 1, 4, LANES), BF16),
            pltpu.SemaphoreType.DMA((kv // 4,)),
        ],
        first=True,
    )(
        recv,
        w_query,
        w_key.T,
        w_value.T,
        w_forget.T,
        w_out,
        forget_bias[None],
    )
    recv = exchanged(message, KV)
    positions = kv_cache.shape[1]
    keys, values, gate_sums = kernel(
        k_prepare,
        [
            ((rows // 4, 4 * DH, positions), BF16),
            ((rows // 4, positions, 4 * DH), BF16),
            ((rows // 4, 16, positions), F32),
        ],
        [SMEM, ANY, ANY],
        [
            pltpu.VMEM(kv_cache.shape, BF16),
            pltpu.VMEM(gate_sums.shape, F32),
            pltpu.SemaphoreType.DMA((rows,)),
            pltpu.SemaphoreType.DMA,
        ],
    )(live_lengths, in_hbm(kv_cache), in_hbm(gate_sums))
    message, tok, sums = kernel(
        k_attend,
        [((kv, rows // 2 + 1, 4, LANES), BF16), block, ((2, LANES), F32)],
        [VMEM] * 4,
        [pltpu.VMEM((4 * rows, LANES), F32)] * 4,
    )(recv, keys, values, gate_sums)
    (message,) = kernel(k_combine, [((tp, rows, width), BF16)], [VMEM] * 3)(
        exchanged(message, KV), sums, w_out
    )
    message, scaled = kernel(
        k_expand,
        [((kv, 8, LANES), BF16), block],
        [VMEM] * 6,
        [pltpu.VMEM((8 * kv, LANES), F32)],
    )(exchanged(message, "tp"), x, tok, gain, w_gate.T, w_up.T)
    message, mid = kernel(k_hidden, [((kv, 4, LANES), BF16), block], [VMEM] * 2)(
        exchanged(message, KV), scaled
    )
    (message,) = kernel(
        k_shrink, [((tp, rows, width), BF16)], [VMEM] * 2, [pltpu.VMEM((4 * kv, LANES), F32)]
    )(exchanged(message, KV), w_down)
    message, mix = kernel(
        k_sums,
        [((kv, 1, LANES), F32), ((own, rows), F32)],
        [VMEM] * 2,
        [pltpu.VMEM((width, rows), F32)],
    )(
        exchanged(message, "tp"), mid
    )
    (out,) = kernel(k_finish, [((own, rows), BF16)], [VMEM] * 3, last=True)(exchanged(message, KV), mix, second_gain[None])
    return out.T


def solution(mesh):
    split = Mesh(mesh.devices.reshape(8, 4, mesh.shape["tp"]), ("kv_0", "kv_1", "tp"))
    placed = (
        P(None, KV_TP),
        P(),
        P(None, KV, "tp"),
        P(None, "tp", KV),
        P(KV, "tp"),
        P(KV, "tp"),
        P(KV, "tp"),
        P(),
        P(),
        P("tp", KV),
        P(KV_TP),
        P(KV, "tp"),
        P(KV, "tp"),
        P("tp", KV),
        P(KV_TP),
    )
    return jax.shard_map(
        on_device, mesh=split, in_specs=placed, out_specs=P(None, KV_TP), check_vma=False
    )
```

```python
import functools

import jax
import jax.numpy as jnp
from jax import lax
from jax.experimental import pallas as pl
from jax.experimental.pallas import tpu as pltpu
from jax.sharding import Mesh
from jax.sharding import PartitionSpec as P

D = 4096
DH = 64
LANES = 128
KV = ("kv_0", "kv_1")
KV_TP = ("kv_0", "kv_1", "tp")
EPSILON = 1e-05
EMPTY_SCORE = -1e30
F32 = jnp.float32
BF16 = jnp.bfloat16

VMEM = pl.BlockSpec(memory_space=pltpu.VMEM)
SMEM = pl.BlockSpec(memory_space=pltpu.SMEM)
ANY = pl.BlockSpec(memory_space=pl.ANY)


def kernel(body, outs, specs, scratch=(), last=False, flops=None):
    return pl.pallas_call(
        body,
        out_shape=[
            jax.ShapeDtypeStruct(shape, dtype) if last else pltpu.VMEM(shape, dtype)
            for shape, dtype in outs
        ],
        in_specs=specs,
        out_specs=[VMEM] * len(outs),
        scratch_shapes=scratch,
        cost_estimate=flops
        and pl.CostEstimate(flops=flops, bytes_accessed=flops // 100, transcendentals=0),
        compiler_params=pltpu.CompilerParams(vmem_limit_bytes=8 * 2**20),
    )


def exchanged(pieces, axis):
    return lax.all_to_all(pieces, axis, 0, 0, tiled=True)


def kv_index():
    return lax.axis_index("kv_0") * lax.axis_size("kv_1") + lax.axis_index("kv_1")


def iota(shape, dim):
    return lax.broadcasted_iota(jnp.int32, shape, dim)


def rounded(x):
    return x.astype(BF16).astype(F32)


def in_pieces(value, count):
    pieces = []
    for _ in range(count):
        piece = rounded(value)
        pieces.append(piece)
        value = value - piece
    return pieces


def diagonal(rows, turn):
    return iota((rows, LANES), 1) == iota((rows, LANES), 0) + rows * turn


def across(left, right, sides):
    return lax.dot_general(left, right, (sides, ((), ())), preferred_element_type=F32)


LAST = ((1,), (1,))
FIRST = ((0,), (0,))


def as_row(columns):
    rows = columns[0].shape[0]
    tile = jnp.zeros((rows, LANES), F32)
    for turn, column in enumerate(columns):
        tile = jnp.where(diagonal(rows, turn), column, tile)
    return jnp.sum(tile, axis=0, keepdims=True)


def as_column(row, rows, turns):
    mask = diagonal(rows, turns[0])
    for turn in turns[1:]:
        mask = mask | diagonal(rows, turn)
    return jnp.sum(jnp.where(mask, row, 0.0), axis=1, keepdims=True)


def summed(ref, start, size):
    total = ref[0, pl.ds(start, size)].astype(F32)
    for k in range(1, ref.shape[0]):
        total = total + ref[k, pl.ds(start, size)].astype(F32)
    return total


def tiles_of(block):
    return [block[4 * t : 4 * t + 4] for t in range(block.shape[0] // 4)]


def put(out, k, tiles):
    for t, tile in enumerate(tiles):
        out[k, t] = tile


def tiles_summed(ref, start, count):
    tiles = []
    for t in range(start, start + count):
        total = ref[0, t].astype(F32)
        for k in range(1, ref.shape[0]):
            total = total + ref[k, t].astype(F32)
        tiles.append(total)
    return tiles[0] if count == 1 else jnp.concatenate(tiles, axis=0)


def k_start(turned_hbm, gain_hbm, out, turned, gain, sem):
    pairs = ((turned_hbm, turned), (gain_hbm, gain))
    copies = [pltpu.make_async_copy(a, b, sem.at[k]) for k, (a, b) in enumerate(pairs)]
    for copy in copies:
        copy.start()
    for copy in copies:
        copy.wait()
    own, rows = turned.shape
    column = jnp.sum(jnp.where(diagonal(own, 0)[:, :own], gain[...], 0.0), axis=1, keepdims=True)
    pad = jnp.zeros((own, LANES - rows), F32)
    tile = jnp.concatenate([turned[...].astype(F32), pad], axis=1)
    for k, piece in enumerate(in_pieces(column, 3)):
        tile = jnp.where(iota(tile.shape, 1) == rows + k, piece, tile)
    tile = tile.astype(BF16)
    for k in range(out.shape[0]):
        out[k] = tile


def k_project(recv, w_query, w_key, w_value, w_forget, w_out, bias, out, x_out, gain_out, new_rows):
    width = recv.shape[0]
    same = jnp.where(iota((width, width), 0) == iota((width, width), 1), 1.0, 0.0).astype(BF16)
    rows = new_rows.shape[0]
    both = across(recv[:, : 2 * rows], same, FIRST)
    x = both[:rows]
    x_out[...] = x
    gain = both[rows : rows + 1] + both[rows + 1 : rows + 2] + both[rows + 2 : rows + 3]
    gain_out[...] = jnp.broadcast_to(gain, gain_out.shape)
    xb = x.astype(BF16)
    row = iota((8, LANES), 0)
    sums = across(jnp.ones((8, LANES), BF16), w_out[...], LAST)
    mine = iota(bias.shape, 1) == lax.axis_index("tp")
    once = jnp.where(kv_index() == 0, 1.0, 0.0)
    own_bias = jnp.sum(jnp.where(mine, bias[...], 0.0), axis=1, keepdims=True) * once
    query = jnp.dot(xb, w_query[...], preferred_element_type=F32)
    new_rows[:, :DH] = across(xb, w_key[...], LAST)
    new_rows[:, DH:] = across(xb, w_value[...], LAST)
    start = pl.multiple_of(kv_index() * width, width)
    forget = across(xb, w_forget[:, pl.ds(start, width)], LAST)
    token_col = jnp.sum(x, axis=1, keepdims=True)
    mine = iota(forget.shape, 1) == lax.axis_index("tp")
    forget_col = jnp.sum(jnp.where(mine, forget, 0.0), axis=1, keepdims=True)
    forget_col = forget_col + own_bias
    small = as_row([*in_pieces(forget_col, 2), *in_pieces(token_col, 2)])
    tail = jnp.where(row == 1, small, 0.0)
    tail = jnp.where(row == 2, sums[:, :LANES], tail)
    tail = jnp.where(row == 3, sums[:, LANES:], tail)
    tiles = tiles_of(query[:, :LANES].astype(BF16)) + tiles_of(query[:, LANES:].astype(BF16))
    for b in range(rows):
        own_tail = jnp.where(row == 0, new_rows[pl.ds(b, 1), :], tail)[:4].astype(BF16)
        for k in range(b, out.shape[0], rows):
            put(out, k, [*tiles, own_tail])


def k_prepare(
    lengths,
    cache,
    gate,
    keys_o,
    values_o,
    gate_o,
    pick_o,
    spread_o,
    cache_v,
    gate_v,
    sem,
    gate_sem,
):
    rows, positions = cache.shape[:2]
    copies = [pltpu.make_async_copy(cache.at[b], cache_v.at[b], sem.at[b]) for b in range(rows)]
    gates = pltpu.make_async_copy(gate, gate_v, gate_sem)
    gates.start()
    for copy in copies:
        copy.start()
    source = iota((LANES, 2 * LANES), 0)
    column = iota((LANES, 2 * LANES), 1)
    place = source % 8
    is_top = column < LANES
    wanted = (place < 5) & (is_top == (place % 2 == 0))
    wanted = wanted & (source // 8 == column % LANES // 8)
    pick_o[...] = jnp.where(wanted, 1.0, 0.0).astype(BF16)
    source = iota((2 * LANES, 4 * DH), 0) % LANES
    column = iota((2 * LANES, 4 * DH), 1)
    wanted = (source % 8 == 0) & (source % 32 // 8 == column // DH)
    spread_o[...] = jnp.where(wanted, 1.0, 0.0).astype(BF16)
    gates.wait()
    place = kv_index() * positions + iota((8, positions), 1)
    first = iota((8, positions), 0) < 4
    for m in range(rows // 2):
        one = jnp.where(place < lengths[2 * m], gate_v[2 * m], EMPTY_SCORE)
        two = jnp.where(place < lengths[2 * m + 1], gate_v[2 * m + 1], EMPTY_SCORE)
        gate_o[m // 2, pl.ds(8 * (m % 2), 8), :] = jnp.where(first, one, two)
    for b in range(rows):
        copies[b].wait()
        keys_o[b // 4, pl.ds(DH * (b % 4), DH), :] = cache_v[b].T[:DH]
        if b % 2:
            values_o[b // 4, :, pl.ds(LANES * (b % 4 // 2), LANES)] = jnp.concatenate(
                [cache_v[b - 1][:, DH:], cache_v[b][:, DH:]], axis=1
            )


def k_attend(recv, keys, values, gate, out, tok_out, sums_out, qs, firsts, seconds, stats):
    rows = 4 * keys.shape[0]
    heads = 4
    scale = DH**-0.5
    left = rounded(tiles_summed(recv, 0, rows // 4))
    right = rounded(tiles_summed(recv, rows // 4, rows // 4))
    tail = tiles_summed(recv, rows // 2, 1)
    new_row = rounded(tail[0:1])
    small = tail[1:2]
    sums_out[...] = tail[2:4]
    tok_out[...] = jnp.broadcast_to(as_column(small, rows, (2, 3)), tok_out.shape)
    even = iota((rows, LANES), 0) % 2 == 0
    low = iota((rows, LANES), 1) < DH
    keep = even == low
    left_turned = pltpu.roll(left, DH, 1)
    right_turned = pltpu.roll(right, DH, 1)
    placed = (
        jnp.where(even, left, left_turned),
        jnp.where(even, left_turned, left),
        jnp.where(even, right, right_turned),
        jnp.where(even, right_turned, right),
    )
    for h, block in enumerate(placed):
        qs[pl.ds(h, rows, stride=heads), :] = jnp.where(keep, block, 0.0)
    all_rows = rows * heads
    owner = iota((all_rows, LANES), 0) // heads
    lane = iota((all_rows, LANES), 1)
    fetched = jnp.where((lane == owner) | (lane == owner + rows), small, 0.0)
    fetched = jnp.sum(fetched, axis=1, keepdims=True)
    new_gate = jnp.minimum(fetched, 0.0) - jnp.log(1.0 + jnp.exp(-jnp.abs(fetched)))
    lane = iota((1, LANES), 1)
    new_turned = pltpu.roll(jnp.broadcast_to(new_row, (8, LANES)), DH, 1)[0:1]
    new_key = jnp.where(lane < DH, new_row, new_turned)
    new_value = jnp.where(lane < DH, new_turned, new_row)
    own = jnp.sum(qs[...] * new_key, axis=1, keepdims=True) * scale
    mine = iota((all_rows, 1), 0) // heads == kv_index()
    own = jnp.where(mine, own, EMPTY_SCORE)
    lane = iota((16, LANES), 1)
    spot = jnp.where(iota((16, LANES), 0) % 8 < heads, DH, 0)
    upper = iota((16, LANES), 0) < 8
    straight = iota((16, LANES), 0) % 8 < heads
    packed = jnp.zeros((4, LANES), F32)
    for m in range(rows // 4):
        at = slice(16 * m, 16 * m + 16)
        query = qs[pl.ds(16 * m, 16), :] * scale
        query = [jnp.where(upper, query, 0.0), jnp.where(upper, 0.0, query)]
        query = jnp.concatenate(query, axis=1).astype(BF16)
        scores = jnp.dot(query, keys[m], preferred_element_type=F32)
        scores = scores + (gate[m] + new_gate[at])
        top = jnp.maximum(jnp.max(scores, axis=1, keepdims=True), own[at])
        top = jnp.maximum(top, 0.1 * EMPTY_SCORE)
        weights = jnp.exp(scores - top)
        own_weight = jnp.exp(own[at] - top)
        total = jnp.sum(weights, axis=1, keepdims=True) + own_weight
        value = jnp.dot(weights.astype(BF16), values[m], preferred_element_type=F32)
        value = jnp.where(upper, value[:, :LANES], value[:, LANES:])
        value = value + rounded(own_weight) * new_value
        spare = jnp.where(lane == spot, top, jnp.where(lane == spot + 1, total, value))
        turned = pltpu.roll(spare, DH, 1)
        firsts[pl.ds(16 * m, 16), :] = jnp.where(straight, spare, turned)
        second = jnp.where(straight, turned, spare)
        seconds[pl.ds(16 * m, 16), :] = second
        pieces = in_pieces(second, 3)
        stat = jnp.where(lane < 5, pltpu.roll(pieces[2], 4, 1), 0.0)
        stat = jnp.where(lane < 4, pltpu.roll(pieces[1], 2, 1), stat)
        stats[pl.ds(16 * m, 16), :] = jnp.where(lane < 2, pieces[0], stat)
        for h in range(heads):
            stat = stats[pl.ds(16 * m + h, 4, stride=heads), :]
            packed = packed + pltpu.roll(stat, 32 * m + 8 * h, 1)
        for side in range(2):
            at = 16 * m + 2 * side
            left = firsts[pl.ds(at, 4, stride=heads), :]
            right = seconds[pl.ds(at + 1, 4, stride=heads), :]
            tile = jnp.where(low[:4], left, right).astype(BF16)
            for k in range(out.shape[0]):
                out[k, rows // 4 * side + m] = tile
    packed = packed.astype(BF16)
    for k in range(out.shape[0]):
        out[k, rows // 2] = packed


def k_combine(recv, sums, w_out, pick, spread, out):
    devices = recv.shape[0]
    tiles = (recv.shape[1] - 1) // 2
    rows = 4 * tiles
    heads = 4 * DH
    stats = recv[:, 2 * tiles].astype(F32)
    stats = jnp.concatenate([stats, stats], axis=1).astype(BF16).reshape(devices * 8, LANES)
    stats = jnp.dot(stats, pick[...], preferred_element_type=F32).reshape(devices, 8, 2 * LANES)
    tops = stats[:, :, :LANES]
    totals = stats[:, :, LANES:]
    scales = jnp.exp(tops - jnp.max(tops, axis=0, keepdims=True))
    joint = jnp.sum(totals * scales, axis=0, keepdims=True)
    shares = in_pieces(scales * (1.0 / joint), 2)
    group = iota(tops.shape, 2) // 32 - iota(tops.shape, 1) // 4
    blocks = []
    for half in range(2):
        mine = [jnp.where(group == 2 * half, share, 0.0) for share in shares]
        mine = jnp.concatenate(mine, axis=2).astype(BF16).reshape(devices * 8, 2 * LANES)
        wide = jnp.dot(mine, spread[...], preferred_element_type=F32).reshape(devices, 8, heads)
        sides = []
        for side in range(2):
            at = tiles * side + 2 * half
            part = [recv[:, at + t].astype(F32) for t in range(2)]
            part = jnp.concatenate(part, axis=1)
            sides.append(jnp.sum(part * wide[:, :, side * LANES : (side + 1) * LANES], axis=0))
        blocks.append(jnp.concatenate(sides, axis=1))
    attended = jnp.concatenate(blocks, axis=0).astype(BF16)
    wide = attended.astype(F32)
    mean = wide[:, :LANES] * sums[0:1, :] + wide[:, LANES:] * sums[1:2, :]
    mean = jnp.sum(mean, axis=1, keepdims=True) / D
    attn_part = jnp.dot(attended, w_out[...], preferred_element_type=F32)
    attn_part = (attn_part - mean).astype(BF16)
    for k in range(out.shape[0]):
        out[k] = attn_part


def k_expand(recv, x, tok, gain, w_gate, w_up, out, scaled_out, tile):
    rows = x.shape[0]
    centred = x[...] - tok[:, 0:1] / D + summed(recv, 0, rows)
    scaled = centred * gain[0:1, :]
    scaled_out[...] = scaled
    squares = as_row(in_pieces(jnp.sum(centred * centred, axis=1, keepdims=True), 2))
    scaled = scaled.astype(BF16)
    pieces = tile.shape[0] // (8 * rows)
    tiles = 3 * pieces
    columns = w_gate.shape[0]
    for k, weight in enumerate((w_gate, w_up)):
        part = across(scaled, weight[...], LAST)
        pad = jnp.zeros((rows, tiles * LANES - columns), F32)
        part = jnp.concatenate([part, pad], axis=1)
        for t in range(tiles):
            at = 8 * (t // 3) + 3 * k + t % 3
            tile[pl.ds(at, rows, stride=8 * pieces), :] = part[:, t * LANES : (t + 1) * LANES]
    for h in range(pieces):
        tile[pl.ds(8 * h + 6, rows, stride=8 * pieces), :] = jnp.broadcast_to(
            squares, (rows, LANES)
        )
        tile[pl.ds(8 * h + 7, rows, stride=8 * pieces), :] = jnp.zeros((rows, LANES), F32)
    for k in range(out.shape[0]):
        out[k] = tile[pl.ds(8 * k, 8), :].astype(BF16)


def k_hidden(recv, scaled, out, mid_out):
    rows = scaled.shape[0]
    total = summed(recv, 0, 8)
    spread = as_column(total[6:7], rows, (0, 1)) / D
    shrink = lax.rsqrt(spread + EPSILON)
    mid_out[...] = rounded(scaled[...] * shrink)
    mine = iota((rows, 1), 0) == kv_index() // (out.shape[0] // rows)
    own = jnp.sum(jnp.where(mine, shrink, 0.0), axis=0, keepdims=True)
    total = total * own
    up = pltpu.roll(total, 5, 0)
    hidden = total / (1.0 + jnp.exp(-total)) * up
    hidden = jnp.where(iota((8, LANES), 0) < 3, hidden, 0.0)[:4].astype(BF16)
    for k in range(out.shape[0]):
        out[k] = hidden


def k_shrink(recv, w_down, out, tile):
    rows = out.shape[1]
    pieces = recv.shape[0] // rows
    for k in range(recv.shape[0]):
        tile[pl.ds(4 * k, 4), :] = recv[k].astype(F32)
    part = jnp.zeros((rows, LANES), F32)
    columns = w_down.shape[0]
    for t in range(3 * pieces):
        at = 4 * (t // 3) + t % 3
        size = min(LANES, columns - t * LANES)
        hidden = tile[pl.ds(at, rows, stride=4 * pieces), :][:, :size].astype(BF16)
        part = part + jnp.dot(
            hidden, w_down[pl.ds(t * LANES, size), :], preferred_element_type=F32
        )
    part = part.astype(BF16)
    for k in range(out.shape[0]):
        out[k] = part


def k_sums(recv, mid, out, own_out, turned):
    rows, width = mid.shape
    mixture = mid[...] + summed(recv, 0, rows)
    centre = jnp.sum(mixture, axis=1, keepdims=True) / width
    square = jnp.sum((mixture - centre) ** 2, axis=1, keepdims=True)
    message = as_row([centre, square])
    for k in range(out.shape[0]):
        out[k] = message
    turned[...] = mixture.T
    own = own_out.shape[0]
    start = pl.multiple_of(lax.axis_index("tp") * own, own)
    own_out[...] = turned[pl.ds(start, own), :]


def k_finish(recv, mix, gain, out):
    own, rows = mix.shape
    devices = recv.shape[0]
    total = recv[0]
    for k in range(1, devices):
        total = total + recv[k]
    middle = total / devices
    spread = (recv[0] - middle) ** 2
    for k in range(1, devices):
        spread = spread + (recv[k] - middle) ** 2
    spread = spread[:, :rows] * (D // devices) + total[:, rows : 2 * rows]
    shrink = lax.rsqrt(spread / D + EPSILON)
    column = jnp.sum(jnp.where(diagonal(own, 0)[:, :own], gain[...], 0.0), axis=1, keepdims=True)
    out[...] = ((mix[...] - middle[:, :rows]) * shrink * column).astype(BF16)


def on_device(
    tokens,
    live_lengths,
    kv_cache,
    gate_sums,
    w_query,
    w_key,
    w_value,
    w_forget,
    forget_bias,
    w_out,
    first_gain,
    w_gate,
    w_up,
    w_down,
    second_gain,
):
    rows, own = tokens.shape
    kv, tp = lax.axis_size(KV), lax.axis_size("tp")
    width = own * tp
    block = ((rows, LANES), F32)
    in_hbm = functools.partial(pltpu.with_memory_space_constraint, memory_space=pltpu.HBM)
    (message,) = kernel(
        k_start,
        [((tp, own, LANES), BF16)],
        [ANY] * 2,
        [
            pltpu.VMEM((own, rows), BF16),
            pltpu.VMEM((1, own), F32),
            pltpu.SemaphoreType.DMA((2,)),
        ],
        flops=10**11,
    )(in_hbm(tokens.T), in_hbm(first_gain[None]))
    recv = exchanged(message, "tp").reshape(width, LANES)
    message, x, gain = kernel(
        k_project,
        [((kv, rows // 2 + 1, 4, LANES), BF16), block, ((8, LANES), F32)],
        [VMEM] * 7,
        [pltpu.VMEM((rows, LANES), F32)],
    )(
        recv,
        w_query,
        w_key.T,
        w_value.T,
        w_forget.T,
        w_out,
        forget_bias[None],
    )
    recv = exchanged(message, KV)
    positions = kv_cache.shape[1]
    keys, values, gate_sums, pick, spread = kernel(
        k_prepare,
        [
            ((rows // 4, 4 * DH, positions), BF16),
            ((rows // 4, positions, 4 * DH), BF16),
            ((rows // 4, 16, positions), F32),
            ((LANES, 2 * LANES), BF16),
            ((2 * LANES, 4 * DH), BF16),
        ],
        [SMEM, ANY, ANY],
        [
            pltpu.VMEM(kv_cache.shape, BF16),
            pltpu.VMEM(gate_sums.shape, F32),
            pltpu.SemaphoreType.DMA((rows,)),
            pltpu.SemaphoreType.DMA,
        ],
    )(live_lengths, in_hbm(kv_cache), in_hbm(gate_sums))
    message, tok, sums = kernel(
        k_attend,
        [((kv, rows // 2 + 1, 4, LANES), BF16), block, ((2, LANES), F32)],
        [VMEM] * 4,
        [pltpu.VMEM((4 * rows, LANES), F32)] * 4,
    )(recv, keys, values, gate_sums)
    (message,) = kernel(k_combine, [((tp, rows, width), BF16)], [VMEM] * 5)(
        exchanged(message, KV), sums, w_out, pick, spread
    )
    message, scaled = kernel(
        k_expand,
        [((kv, 8, LANES), BF16), block],
        [VMEM] * 6,
        [pltpu.VMEM((8 * kv, LANES), F32)],
    )(exchanged(message, "tp"), x, tok, gain, w_gate.T, w_up.T)
    message, mid = kernel(k_hidden, [((kv, 4, LANES), BF16), block], [VMEM] * 2)(
        exchanged(message, KV), scaled
    )
    (message,) = kernel(
        k_shrink, [((tp, rows, width), BF16)], [VMEM] * 2, [pltpu.VMEM((4 * kv, LANES), F32)]
    )(exchanged(message, KV), w_down)
    message, mix = kernel(
        k_sums,
        [((kv, 1, LANES), F32), ((own, rows), F32)],
        [VMEM] * 2,
        [pltpu.VMEM((width, rows), F32)],
    )(
        exchanged(message, "tp"), mid
    )
    (out,) = kernel(k_finish, [((own, rows), BF16)], [VMEM] * 3, last=True)(exchanged(message, KV), mix, second_gain[None])
    return out.T


def solution(mesh):
    split = Mesh(mesh.devices.reshape(8, 4, mesh.shape["tp"]), ("kv_0", "kv_1", "tp"))
    placed = (
        P(None, KV_TP),
        P(),
        P(None, KV, "tp"),
        P(None, "tp", KV),
        P(KV, "tp"),
        P(KV, "tp"),
        P(KV, "tp"),
        P(),
        P(),
        P("tp", KV),
        P(KV_TP),
        P(KV, "tp"),
        P(KV, "tp"),
        P("tp", KV),
        P(KV_TP),
    )
    return jax.shard_map(
        on_device, mesh=split, in_specs=placed, out_specs=P(None, KV_TP), check_vma=False
    )
```
